512 devices in a mesh: sp: 64 (over z, y), tp: 8 (over x, core).
Axes of the slice: x: 4, y: 8, z: 8, core: 2. Of those that a mesh axis runs over, the one named last changes fastest.
Arguments:
- tokens: bfloat16 [24576, 2048], P('sp', 'tp'), may hold values from -6 to 6
- input_gain: float32 [2048], replicated, may hold values from 0.1 to 1.9
- query_weight: bfloat16 [2048, 1024], P(None, 'tp'), may hold values from -0.5 to 0.5
- query_rot_weight: bfloat16 [2048, 512], P(None, 'tp'), may hold values from -0.125 to 0.125
- kv_down: bfloat16 [2048, 256], replicated, may hold values from -0.5 to 0.5
- rot_down: bfloat16 [2048, 32], replicated, may hold values from -0.125 to 0.125
- kv_gain: float32 [256], replicated, may hold values from 0.1 to 1.9
- key_up: bfloat16 [256, 1024], P(None, 'tp'), may hold values from -0.5 to 0.5
- value_up: bfloat16 [256, 1024], P(None, 'tp'), may hold values from -4 to 4
- conv_value_weight: bfloat16 [2048, 1024], P(None, 'tp'), may hold values from -0.125 to 0.125
- conv_gate_weight: bfloat16 [2048, 1024], P(None, 'tp'), may hold values from -0.125 to 0.125
- conv_taps: float32 [31, 1024], P(None, 'tp'), may hold values from -8 to 8
- conv_ln_gain: float32 [1024], P('tp'), may hold values from 0.1 to 1.9
- conv_ln_bias: float32 [1024], P('tp'), may hold values from -3 to 3
- att_out_gain: float32 [1024], P('tp'), may hold values from 0.1 to 1.9
- conv_out_gain: float32 [1024], P('tp'), may hold values from 0.1 to 1.9
- att_out_weight: bfloat16 [1024, 2048], P('tp'), may hold values from -0.125 to 0.125
- conv_out_weight: bfloat16 [1024, 2048], P('tp'), may hold values from -0.125 to 0.125
Outputs:
- mixed: bfloat16 [24576, 2048], P('sp', 'tp')
The draws below stay inside these ranges and needn't reach their ends.
All inputs are finite; a program needn't handle non-finite values.
Results may differ from the reference program's by a relative error of at most 0.017.
Values may be sent and summed in bfloat16 or wider, within the bound.
A program may use at most 128 MiB of HBM per device.

```python
import math
import jax
import jax.numpy as jnp
from jax import lax

D_MODEL = 2048
HEADS = 16
NOPE_DIM = 64
ROT_DIM = 32
VALUE_DIM = 64
KV_RANK = 256
CONV_CH = 1024
KERNEL = 31
TOKENS = 24576
ATT_WIDTH = 1024
N_TP = 8


def latent_weights(key):
    down_map = jax.random.normal(jax.random.fold_in(key, 101), (D_MODEL, KV_RANK), jnp.float32) / math.sqrt(D_MODEL)
    upward = jax.random.normal(jax.random.fold_in(key, 102), (KV_RANK, HEADS * NOPE_DIM), jnp.float32) / math.sqrt(KV_RANK)
    return (jnp.clip(down_map, -0.5, 0.5), jnp.clip(upward, -0.5, 0.5))


def rising_scales(key, entries):
    position = jnp.arange(entries, dtype=jnp.float32) / max(entries - 1, 1)
    jitter = jax.random.uniform(key, (entries,), jnp.float32)
    return 10.0 ** (0.5 * position + 0.5 * jitter - 0.5)


def draw_tokens(key, part):
    base_draw = jax.random.normal(jax.random.fold_in(key, 1), (TOKENS, D_MODEL), jnp.float32)
    return jnp.clip(base_draw, -6.0, 6.0).astype(jnp.bfloat16)


def draw_query_weight(key, part):
    base_draw = jax.random.normal(jax.random.fold_in(key, 104), (D_MODEL, HEADS * NOPE_DIM), jnp.float32) / math.sqrt(D_MODEL)
    return jnp.clip(base_draw, -0.5, 0.5).astype(jnp.bfloat16)


def draw_kv_down(key, part):
    return latent_weights(key)[0].astype(jnp.bfloat16)


def draw_key_up(key, part):
    return latent_weights(key)[1].astype(jnp.bfloat16)


def draw_value_up(key, part):
    base_draw = jax.random.normal(jax.random.fold_in(key, 201), (KV_RANK, HEADS * VALUE_DIM), jnp.float32) / math.sqrt(KV_RANK)
    scales = jnp.repeat(rising_scales(jax.random.fold_in(key, 202), HEADS), VALUE_DIM)
    return jnp.clip(base_draw * scales[None, :], -4.0, 4.0).astype(jnp.bfloat16)


def draw_conv_taps(key, part):
    base_draw = jax.random.normal(jax.random.fold_in(key, 301), (KERNEL, CONV_CH), jnp.float32) / math.sqrt(KERNEL)
    scales = rising_scales(jax.random.fold_in(key, 302), CONV_CH)
    return jnp.clip(base_draw * scales[None, :], -8.0, 8.0).astype(jnp.float32)


def steps_of(stream_key, dims, shards, least, largest):
    def one(dim, parts):
        heights = jax.random.uniform(jax.random.fold_in(jax.random.fold_in(stream_key, 6), dim), (parts,), jnp.float32, least / len(shards), largest / len(shards))
        return jnp.repeat(jnp.exp(heights), dims[dim] // parts).reshape((-1,) + (1,) * (len(dims) - dim - 1))

    level = one(*shards[0])
    for cut in shards[1:]:
        level = level * one(*cut)
    return level


def centred(own_key, dims, width, limit, split=(), held_as=jnp.bfloat16):
    values = width * jax.random.normal(own_key, dims, jnp.float32)
    if split:
        values = values * steps_of(own_key, dims, split, -0.22, 0.18)
    return jnp.clip(values, -limit, limit).astype(held_as)


def setup_inputs(seed: int = 0) -> dict:
    key_of = jax.random.split(jax.random.key(seed), 19)
    tokens = draw_tokens(jax.random.fold_in(key_of[18], 71), 0)
    input_gain = jnp.clip(1.0 + 0.18 * jax.random.normal(key_of[1], (D_MODEL,), jnp.float32), 0.1, 1.9)
    query_weight = draw_query_weight(jax.random.fold_in(key_of[18], 71), 0)
    query_rot_weight = centred(key_of[3], (D_MODEL, HEADS * ROT_DIM), D_MODEL ** -0.5, 0.125, ((1, 8),))
    kv_down = draw_kv_down(jax.random.fold_in(key_of[18], 71), 0)
    rot_down = centred(key_of[5], (D_MODEL, ROT_DIM), D_MODEL ** -0.5, 0.125)
    kv_gain = jnp.clip(1.0 + 0.18 * jax.random.normal(key_of[6], (KV_RANK,), jnp.float32), 0.1, 1.9)
    key_up = draw_key_up(jax.random.fold_in(key_of[18], 71), 0)
    value_up = draw_value_up(jax.random.fold_in(key_of[18], 71), 0)
    conv_value_weight = centred(key_of[9], (D_MODEL, CONV_CH), D_MODEL ** -0.5, 0.125, ((1, 8),))
    conv_gate_weight = centred(key_of[10], (D_MODEL, CONV_CH), D_MODEL ** -0.5, 0.125, ((1, 8),))
    conv_taps = draw_conv_taps(jax.random.fold_in(key_of[18], 71), 0)
    conv_ln_gain = jnp.clip(1.0 + 0.18 * jax.random.normal(key_of[12], (CONV_CH,), jnp.float32), 0.1, 1.9)
    conv_ln_bias = centred(key_of[13], (CONV_CH,), 0.5, 3.0, ((0, 8),), jnp.float32)
    att_out_gain = jnp.clip(1.0 + 0.18 * jax.random.normal(key_of[14], (ATT_WIDTH,), jnp.float32), 0.1, 1.9)
    conv_out_gain = jnp.clip(1.0 + 0.18 * jax.random.normal(key_of[15], (CONV_CH,), jnp.float32), 0.1, 1.9)
    att_out_weight = centred(key_of[16], (ATT_WIDTH, D_MODEL), (ATT_WIDTH + CONV_CH) ** -0.5, 0.125, ((0, 8),))
    conv_out_weight = centred(key_of[17], (CONV_CH, D_MODEL), (ATT_WIDTH + CONV_CH) ** -0.5, 0.125, ((0, 8),))
    return {"tokens": tokens, "input_gain": input_gain, "query_weight": query_weight, "query_rot_weight": query_rot_weight, "kv_down": kv_down, "rot_down": rot_down, "kv_gain": kv_gain, "key_up": key_up, "value_up": value_up, "conv_value_weight": conv_value_weight, "conv_gate_weight": conv_gate_weight, "conv_taps": conv_taps, "conv_ln_gain": conv_ln_gain, "conv_ln_bias": conv_ln_bias, "att_out_gain": att_out_gain, "conv_out_gain": conv_out_gain, "att_out_weight": att_out_weight, "conv_out_weight": conv_out_weight}


norm_eps = 1e-06
rope_base = 10000.0

def lifted(array):
    return lax.optimization_barrier(array).astype(jnp.float32)

def rotary_tables(positions, half_dim):
    frequency = rope_base ** (-jnp.arange(half_dim, dtype=jnp.float32) / half_dim)
    angles = positions.astype(jnp.float32)[:, None] * frequency[None, :]
    return (jnp.cos(angles), jnp.sin(angles))

def rotate_half(values, cos_table, sine_table):
    half_dim = cos_table.shape[-1]
    front_half = values[..., :half_dim]
    back_half = values[..., half_dim:]
    return jnp.concatenate([front_half * cos_table - back_half * sine_table, back_half * cos_table + front_half * sine_table], axis=-1)

def reference(tokens, input_gain, query_weight, query_rot_weight, kv_down, rot_down, kv_gain, key_up, value_up, conv_value_weight, conv_gate_weight, conv_taps, conv_ln_gain, conv_ln_bias, att_out_gain, conv_out_gain, att_out_weight, conv_out_weight):
    tokens_wide = tokens.astype(jnp.float32)
    row_scale = lax.rsqrt(lax.optimization_barrier(jnp.mean(tokens_wide * tokens_wide, axis=1, keepdims=True)) + norm_eps)
    scaled = (tokens_wide * input_gain[None, :]).astype(jnp.bfloat16)

    def project(weight):
        return jnp.dot(scaled.astype(jnp.float32), weight.astype(jnp.float32), preferred_element_type=jnp.float32)
    positions = jnp.arange(TOKENS, dtype=jnp.int32)
    cos_table, sine_table = rotary_tables(positions, ROT_DIM // 2)
    queries = (project(query_weight) * row_scale).astype(jnp.bfloat16).reshape(TOKENS, HEADS, NOPE_DIM)
    query_rot = rotate_half((project(query_rot_weight) * row_scale).reshape(TOKENS, HEADS, ROT_DIM), cos_table[:, None, :], sine_table[:, None, :]).astype(jnp.bfloat16)
    latent_raw = project(kv_down)
    latent = (latent_raw * lax.rsqrt(lax.optimization_barrier(jnp.mean(latent_raw * latent_raw, axis=1, keepdims=True)) + norm_eps) * kv_gain[None, :]).astype(jnp.bfloat16)
    key_rot = rotate_half(project(rot_down) * row_scale, cos_table, sine_table).astype(jnp.bfloat16)
    keys = jnp.dot(latent.astype(jnp.float32), key_up.astype(jnp.float32), preferred_element_type=jnp.float32).astype(jnp.bfloat16).reshape(TOKENS, HEADS, NOPE_DIM)
    values = jnp.dot(latent.astype(jnp.float32), value_up.astype(jnp.float32), preferred_element_type=jnp.float32).astype(jnp.bfloat16).reshape(TOKENS, HEADS, VALUE_DIM)
    queries_heads = jnp.transpose(lifted(queries), (1, 0, 2))
    qrot_heads = jnp.transpose(lifted(query_rot), (1, 0, 2))
    keys_heads = jnp.transpose(lifted(keys), (1, 0, 2))
    values_heads = jnp.transpose(lifted(values), (1, 0, 2))
    krot_wide = lifted(key_rot)
    inv_scale = 1.0 / math.sqrt(NOPE_DIM + ROT_DIM)
    block_len = min(512, TOKENS)
    pieces = []
    for block_idx in range(TOKENS // block_len):
        row_low = block_idx * block_len
        row_high = row_low + block_len
        key_pos = jnp.arange(row_high, dtype=jnp.int32)
        query_pos = jnp.arange(row_low, row_high, dtype=jnp.int32)
        visible = key_pos[None, :] <= query_pos[:, None]
        krot_part = krot_wide[:row_high]

        def one_head(members):
            query_head, qrot_head, key_head, value_head = members
            scores = (jnp.dot(query_head, key_head.T) + jnp.dot(qrot_head, krot_part.T)) * inv_scale
            row_max = lax.optimization_barrier(jnp.max(jnp.where(visible, scores, -jnp.inf), axis=1, keepdims=True))
            exp_scores = jnp.where(visible, jnp.exp(scores - row_max), 0.0)
            denominator = lax.optimization_barrier(jnp.sum(exp_scores, axis=1, keepdims=True))
            weighted = jnp.dot(lifted(exp_scores.astype(jnp.bfloat16)), value_head)
            return weighted / denominator
        head_out = lax.map(one_head, (queries_heads[:, row_low:row_high], qrot_heads[:, row_low:row_high], keys_heads[:, :row_high], values_heads[:, :row_high]))
        pieces.append(jnp.transpose(head_out, (1, 0, 2)).astype(jnp.bfloat16))
    attended = jnp.concatenate(pieces, axis=0).reshape(TOKENS, ATT_WIDTH)
    gated_input = (project(conv_value_weight) * row_scale * jax.nn.sigmoid(project(conv_gate_weight) * row_scale)).astype(jnp.bfloat16)
    padded = jnp.pad(lifted(gated_input), ((KERNEL - 1, 0), (0, 0)))
    conv_out = jnp.zeros((TOKENS, CONV_CH), jnp.float32)
    for tap_idx in range(KERNEL):
        conv_out = conv_out + conv_taps[tap_idx][None, :] * padded[tap_idx:tap_idx + TOKENS]
    mean_val = lax.optimization_barrier(jnp.mean(conv_out, axis=1, keepdims=True))
    spread = lax.optimization_barrier(jnp.mean(conv_out * conv_out, axis=1, keepdims=True)) - mean_val * mean_val
    swished = jax.nn.silu((conv_out - mean_val) * lax.rsqrt(spread + norm_eps) * conv_ln_gain[None, :] + conv_ln_bias[None, :])
    conv_mixed = (swished * lax.rsqrt(lax.optimization_barrier(jnp.mean(swished * swished, axis=1, keepdims=True)) + norm_eps) * conv_out_gain[None, :]).astype(jnp.bfloat16)
    att_wide = lifted(attended)
    att_mixed = (att_wide * lax.rsqrt(lax.optimization_barrier(jnp.mean(att_wide * att_wide, axis=1, keepdims=True)) + norm_eps) * att_out_gain[None, :]).astype(jnp.bfloat16)
    att_share = ATT_WIDTH // N_TP
    conv_share = CONV_CH // N_TP
    result = jnp.zeros((TOKENS, D_MODEL), jnp.float32)
    for group_idx in range(N_TP):
        att_low = group_idx * att_share
        conv_low = group_idx * conv_share
        partial_value = jnp.dot(att_mixed[:, att_low:att_low + att_share].astype(jnp.float32), att_out_weight[att_low:att_low + att_share].astype(jnp.float32), preferred_element_type=jnp.float32) + jnp.dot(conv_mixed[:, conv_low:conv_low + conv_share].astype(jnp.float32), conv_out_weight[conv_low:conv_low + conv_share].astype(jnp.float32), preferred_element_type=jnp.float32)
        result = result + lifted(partial_value.astype(jnp.bfloat16))
    return result.astype(jnp.bfloat16)
```

```python
import math

import jax
import jax.numpy as jnp
from jax import lax
from jax.experimental import pallas as pl
from jax.experimental.pallas import tpu as pltpu
from jax.sharding import PartitionSpec as P

D_MODEL = 2048
NOPE_DIM = 64
ROT_DIM = 32
VALUE_DIM = 64
CONV_CH = 1024
KERNEL = 31
ATT_WIDTH = 1024


norm_eps = 1e-06
far_below = -1e30
rope_base = 10000.0


def copy_for_each(x, axis):
    peers = lax.axis_size(axis)
    return lax.all_to_all(jnp.broadcast_to(x[None], (peers, *x.shape)), axis, 0, 0, tiled=True)


def in_order(pieces, dim):
    pieces = jnp.moveaxis(pieces, 0, dim)
    shape = pieces.shape
    return pieces.reshape(*shape[:dim], shape[dim] * shape[dim + 1], *shape[dim + 2 :])


def gathered_copies(x, axis, dim):
    pieces = copy_for_each(x, axis)
    return in_order(pieces, dim)


def sent_together(arrays, axis, dim, along):
    both = jnp.concatenate(arrays, axis=along)
    result, at, gathered = (lax.all_gather(both, axis, axis=dim, tiled=True), 0, [])
    for a in arrays:
        gathered.append(lax.slice_in_dim(result, at, at + a.shape[along], axis=along))
        at += a.shape[along]
    return tuple(gathered)


def shifted(block, axis, distance):
    devices = range(lax.axis_size(axis))
    route = [(i - distance, i) for i in devices if i - distance in devices]
    return lax.ppermute(block, axis, route)


def of_everyone(x, axis):
    everything = copy_for_each(x, axis)
    return jnp.sum(everything, axis=0)


def in_one(arrays, axis):
    line, at, gathered = (jnp.concatenate([a.reshape(-1) for a in arrays]), 0, [])
    so_far = of_everyone(line, axis)
    for a in arrays:
        gathered.append(so_far[at : at + a.size].reshape(a.shape))
        at += a.size
    return tuple(gathered)


def cut_along(x, dim, peers):
    shape = x.shape
    pieces = x.reshape(*shape[:dim], peers, shape[dim] // peers, *shape[dim + 1 :])
    return jnp.moveaxis(pieces, dim, 0)


def summed_on_arrival(x, axis, dim):
    pieces = cut_along(x, dim, lax.axis_size(axis))
    arrived = lax.all_to_all(pieces, axis, split_axis=0, concat_axis=0, tiled=True)
    return arrived.astype(jnp.float32).sum(axis=0)


def rotary_tables(positions, half_dim):
    frequency = rope_base ** (-jnp.arange(half_dim, dtype=jnp.float32) / half_dim)
    angles = positions.astype(jnp.float32)[:, None] * frequency[None, :]
    return (jnp.cos(angles), jnp.sin(angles))


def rotate_half(values, cos_table, sine_table):
    half_dim = cos_table.shape[-1]
    front_half = values[..., :half_dim]
    back_half = values[..., half_dim:]
    return jnp.concatenate(
        [
            front_half * cos_table - back_half * sine_table,
            back_half * cos_table + front_half * sine_table,
        ],
        axis=-1,
    )

MESH = pl.DeviceIdType.MESH
ROWS = 384
SHARE = 112
KSETS = 16
LOG2E = 1.4426950408889634


def ring_peers(tp):
    x, c = tp // 2, tp % 2
    right = ((x + 1) % 4) * 2 + c
    left = ((x + 3) % 4) * 2 + c
    far = ((x + 2) % 4) * 2 + c
    partner = x * 2 + (1 - c)
    return right, left, far, partner


class RingGather:
    def __init__(self, buf, lo, hi, mid, send, recv, sp, tp):
        self.buf, self.lo, self.hi, self.mid = buf, lo, hi, mid
        self.send, self.recv, self.sp, self.tp = send, recv, sp, tp
        self.right, self.left, self.far, self.partner = ring_peers(tp)

    def piece(self, slot, part=None):
        lo, hi = {None: (self.lo, self.hi), 0: (self.lo, self.mid), 1: (self.mid, self.hi)}[part]
        return self.buf.at[slot, pl.ds(lo, hi - lo)]

    def copy(self, slot, part, sem, to):
        return pltpu.make_async_remote_copy(
            src_ref=self.piece(slot, part),
            dst_ref=self.piece(slot, part),
            send_sem=self.send.at[sem],
            recv_sem=self.recv.at[sem],
            device_id=(self.sp, to),
            device_id_type=MESH,
        )

    def begin(self):
        self.copy(self.tp, None, 0, self.right).start()
        self.copy(self.tp, None, 1, self.left).start()
        self.copy(self.tp, None, 2, self.partner).start()

    def relay(self):
        self.copy(self.left, None, 0, self.right).wait_recv()
        self.copy(self.left, 0, 5, self.right).start()
        self.copy(self.left, None, 3, self.partner).start()
        self.copy(self.right, None, 1, self.left).wait_recv()
        self.copy(self.right, 1, 6, self.left).start()
        self.copy(self.right, None, 4, self.partner).start()

    def relay_far(self):
        self.copy(self.far, 0, 5, self.right).wait_recv()
        self.copy(self.far, 0, 7, self.partner).start()
        self.copy(self.far, 1, 6, self.left).wait_recv()
        self.copy(self.far, 1, 8, self.partner).start()

    def finish(self):
        for sem, part in ((2, None), (3, None), (4, None), (7, 0), (8, 1)):
            self.copy(self.far, part, sem, self.partner).wait_recv()

    def drain(self):
        for sem, part in ((0, None), (1, None), (2, None), (3, None), (4, None), (5, 0), (6, 1), (7, 0), (8, 1)):
            self.copy(self.tp, part, sem, self.partner).wait_send()


def member_z(member, kind):
    return 2 * member + (kind + member) % 2


def attention_kernel(
    q_ref, share_ref, key_up_ref, value_up_ref, out_ref,
    qbuf, kbuf, kk, vv, wkv, top, acc, o_send, l_send, o_recv, l_recv, own_lse,
    q_ssem, q_rsem, k_ssem, k_rsem, ag_ssem, ag_rsem, o_ssem, o_rsem, l_ssem, l_rsem,
):
    sp, tp = lax.axis_index("sp"), lax.axis_index("tp")
    z, y = sp // 8, sp % 8
    kind, mine = (z + z // 2) % 2, z // 2
    right, left, far, partner = ring_peers(tp)

    members = [None]
    for i in range(1, 4):
        members.append(member_z((mine + i) % 4, kind) * 8 + y)
    key_peers = []
    for dz in range(8):
        zz = (z + dz) % 8
        for e in range(2):
            yy = (y % 4 + z // 2 + 4 - zz // 2) % 4
            yy = (yy + 4 * (y // 4) + 4 * e) % 8
            key_peers.append(zz * 8 + yy)

    barrier = pltpu.get_barrier_semaphore()
    for i in range(1, 4):
        pl.semaphore_signal(barrier, inc=1, device_id=(members[i], tp), device_id_type=MESH)
    for i in range(1, 16):
        pl.semaphore_signal(barrier, inc=1, device_id=(key_peers[i], tp), device_id_type=MESH)
    for peer in (right, left, partner):
        pl.semaphore_signal(barrier, inc=1, device_id=(sp, peer), device_id_type=MESH)
    pl.semaphore_wait(barrier, 21)

    slot = z * 2 + y // 4
    half = z // 4

    def key_copy(i):
        return pltpu.make_async_remote_copy(
            src_ref=share_ref,
            dst_ref=kbuf.at[tp, slot],
            send_sem=k_ssem.at[i],
            recv_sem=k_rsem.at[half],
            device_id=(key_peers[i], tp),
            device_id_type=MESH,
        )

    def query_copy(i):
        return pltpu.make_async_remote_copy(
            src_ref=q_ref,
            dst_ref=qbuf.at[i - 1],
            send_sem=q_ssem.at[i - 1],
            recv_sem=q_rsem.at[i - 1],
            device_id=(members[i], tp),
            device_id_type=MESH,
        )

    own_copy = pltpu.make_async_copy(share_ref, kbuf.at[tp, slot], k_rsem.at[half])
    own_copy.start()
    for i in range(1, 16):
        key_copy(i).start()
    for i in range(1, 4):
        query_copy(i).start()

    lane = lax.broadcasted_iota(jnp.int32, (256, 128), 1)
    for n, ref in enumerate((key_up_ref, value_up_ref)):
        w = ref[...].astype(jnp.float32)
        wkv[:, pl.ds(256 * n, 128)] = jnp.where(lane < 64, w, 0.0).astype(jnp.bfloat16)
        wkv[:, pl.ds(256 * n + 128, 128)] = jnp.where(
            lane < 64, pltpu.roll(w, 64, 1), 0.0
        ).astype(jnp.bfloat16)

    gathers = []
    for p in range(2):
        arrived = kbuf.at[tp, pl.ds(8 * p, 8)]
        pltpu.make_async_copy(arrived, arrived, k_rsem.at[p]).wait()
        gather = RingGather(
            kbuf, 8 * p, 8 * p + 8, 8 * p + 4, ag_ssem.at[p], ag_rsem.at[p], sp, tp
        )
        gather.begin()
        gathers.append(gather)
    for gather in gathers:
        gather.relay()

    low = lax.broadcasted_iota(jnp.int32, (ROWS, 128), 1) < 64

    def assemble(s, carry):
        first = kbuf[:, s, 0:48, :].reshape(ROWS, 128)
        second = kbuf[:, s, 48:96, :].reshape(ROWS, 128)
        rows = jnp.concatenate([first, second], axis=1)
        product = jnp.dot(rows, wkv[...], preferred_element_type=jnp.float32)
        folded = kbuf[0:6, s, 96:112, :].astype(jnp.float32).reshape(96, 128)
        turned = [pltpu.roll(folded, (64 - 32 * j) % 128, 1).reshape(6, 1, 16, 128) for j in range(4)]
        rotary = jnp.concatenate(turned, axis=1).reshape(ROWS, 128)
        at = pl.ds(pl.multiple_of(s * ROWS, ROWS), ROWS)
        for h in range(2):
            kk[h, at, :] = jnp.where(low, product[:, 128 * h : 128 * h + 128], rotary).astype(jnp.bfloat16)
            vv[h, at, :] = jnp.where(
                low, product[:, 256 + 128 * h : 384 + 128 * h], 1.0
            ).astype(jnp.bfloat16)
        return carry

    for p in range(2):
        gathers[p].relay_far()
    for p in range(2):
        gathers[p].finish()
        lax.fori_loop(8 * p, 8 * p + 8, assemble, 0)

    def step(queries, start, size, diagonal):
        for h in range(2):
            at = pl.ds(pl.multiple_of(start, ROWS), size)
            scores = lax.dot_general(
                queries[:, 128 * h : 128 * h + 128],
                kk[h, at, :],
                (((1,), (1,)), ((), ())),
                preferred_element_type=jnp.float32,
            )
            if diagonal:
                seen = lax.broadcasted_iota(jnp.int32, (ROWS, size), 1) <= lax.broadcasted_iota(
                    jnp.int32, (ROWS, size), 0
                )
                scores = jnp.where(seen, scores, far_below)
            before = top[h]
            now = jnp.maximum(before, jnp.max(scores, axis=1, keepdims=True))
            top[h] = now
            weights = jnp.exp2(scores - now[:, :1]).astype(jnp.bfloat16)
            acc[h] = acc[h] * jnp.exp2(before - now) + jnp.dot(
                weights, vv[h, at, :], preferred_element_type=jnp.float32
            )

    def attend(queries, whole, diagonal):
        top[...] = jnp.full(top.shape, far_below, jnp.float32)
        acc[...] = jnp.zeros(acc.shape, jnp.float32)

        def pair(j, carry):
            step(queries, j * (2 * ROWS), 2 * ROWS, False)
            return carry

        lax.fori_loop(0, whole // 2, pair, 0)

        @pl.when(whole % 2 == 1)
        def _():
            step(queries, (whole - 1) * ROWS, ROWS, False)

        if diagonal:
            step(queries, whole * ROWS, ROWS, True)
        sums, tops = [], []
        for h in range(2):
            a = acc[h]
            total = jnp.where(low, pltpu.roll(a, 64, 1), a)
            sums.append(total)
            tops.append(top[h] + jnp.log2(jnp.maximum(total, 1e-37)))
        value = jnp.where(low, acc[0], pltpu.roll(acc[1], 64, 1))
        total = jnp.where(low, sums[0], sums[1])
        return value / jnp.maximum(total, 1e-37), tops

    tag = lax.broadcasted_iota(jnp.int32, (ROWS, 128), 1)

    def back_copies(i):
        return (
            pltpu.make_async_remote_copy(
                src_ref=o_send.at[i - 1],
                dst_ref=o_recv.at[i - 1],
                send_sem=o_ssem.at[i - 1],
                recv_sem=o_rsem.at[i - 1],
                device_id=(member_z((mine + 4 - i) % 4, kind) * 8 + y, tp),
                device_id_type=MESH,
            ),
            pltpu.make_async_remote_copy(
                src_ref=l_send.at[i - 1],
                dst_ref=l_recv.at[i - 1],
                send_sem=l_ssem.at[i - 1],
                recv_sem=l_rsem.at[i - 1],
                device_id=(member_z((mine + 4 - i) % 4, kind) * 8 + y, tp),
                device_id_type=MESH,
            ),
        )

    residue = (y + mine) % 4
    for i in (2, 1, 3):
        query_copy(i).wait_recv()
        their = (mine + 4 - i) % 4
        their_z = member_z(their, kind)
        first = (residue + 4 - their) % 4
        whole = (
            2 * their_z
            + jnp.where(first <= y, 1, 0).astype(jnp.int32)
            + jnp.where(first + 4 <= y, 1, 0).astype(jnp.int32)
        )
        out, tops = attend(qbuf.at[i - 1], whole, False)
        o_send[i - 1] = out.astype(jnp.bfloat16)
        packed = jnp.where(tag < 4, tops[0], tops[1])
        l_send[i - 1] = jnp.transpose(packed)[0:8, :]
        for copy in back_copies(i):
            copy.start()
    out, tops = attend(q_ref, 2 * z + y // 4, True)
    own_lse[...] = jnp.where(low, tops[0], tops[1])

    logs, values = [own_lse[...]], [out]
    for i in range(1, 4):
        for copy in back_copies(i):
            copy.wait_recv()
        columns = jnp.transpose(l_recv[i - 1])
        logs.append(jnp.where(low, columns[:, 0:1], columns[:, 4:5]))
        values.append(o_recv[i - 1].astype(jnp.float32))
    peak = jnp.maximum(jnp.maximum(logs[0], logs[1]), jnp.maximum(logs[2], logs[3]))
    shares = [jnp.exp2(log - peak) for log in logs]
    total = shares[0] + shares[1] + shares[2] + shares[3]
    merged = sum(s * v for s, v in zip(shares, values))
    out_ref[...] = (merged / total).astype(jnp.bfloat16)

    for i in range(1, 16):
        key_copy(i).wait_send()
    for i in range(1, 4):
        query_copy(i).wait_send()
        for copy in back_copies(i):
            copy.wait_send()
    for gather in gathers:
        gather.drain()


def attention(queries, share, key_up, value_up):
    vmem = pl.BlockSpec(memory_space=pltpu.VMEM)
    bf, f32 = jnp.bfloat16, jnp.float32
    dma = pltpu.SemaphoreType.DMA
    return pl.pallas_call(
        attention_kernel,
        out_shape=jax.ShapeDtypeStruct((ROWS, 128), bf),
        in_specs=[vmem] * 4,
        out_specs=vmem,
        scratch_shapes=[
            pltpu.VMEM((3, ROWS, 256), bf),
            pltpu.VMEM((8, KSETS, SHARE, 128), bf),
            pltpu.VMEM((2, KSETS * ROWS, 128), bf),
            pltpu.VMEM((2, KSETS * ROWS, 128), bf),
            pltpu.VMEM((256, 512), bf),
            pltpu.VMEM((2, ROWS, 128), f32),
            pltpu.VMEM((2, ROWS, 128), f32),
            pltpu.VMEM((3, ROWS, 128), bf),
            pltpu.VMEM((3, 8, ROWS), f32),
            pltpu.VMEM((3, ROWS, 128), bf),
            pltpu.VMEM((3, 8, ROWS), f32),
            pltpu.VMEM((ROWS, 128), f32),
            dma((3,)), dma((3,)), dma((16,)), dma((2,)), dma((2, 9)), dma((2, 9)),
            dma((3,)), dma((3,)), dma((3,)), dma((3,)),
        ],
        compiler_params=pltpu.CompilerParams(collective_id=1, has_side_effects=True),
        name="attention",
    )(queries, share, key_up, value_up)


def shards(
    tokens,
    input_gain,
    query_weight,
    query_rot_weight,
    kv_down,
    rot_down,
    kv_gain,
    key_up,
    value_up,
    conv_value_weight,
    conv_gate_weight,
    conv_taps,
    conv_ln_gain,
    conv_ln_bias,
    att_out_gain,
    conv_out_gain,
    att_out_weight,
    conv_out_weight,
):
    tok_rows = tokens.shape[0]
    heads_here = key_up.shape[1] // NOPE_DIM
    chan_here = conv_taps.shape[1]
    weight_list = (
        query_weight,
        query_rot_weight,
        kv_down,
        rot_down,
        conv_value_weight,
        conv_gate_weight,
    )
    wide_part = gathered_copies(tokens, "tp", 1).astype(jnp.float32)
    scaled = (wide_part * input_gain[None, :]).astype(jnp.bfloat16)

    def add_product(weight):
        return jnp.dot(scaled, weight, preferred_element_type=jnp.float32)

    summed = tuple((add_product(weight) for weight in weight_list))
    q_acc, qrot_acc, latent_raw, rot_acc, value_acc, gate_acc, square_sum = summed + (
        jnp.sum(wide_part * wide_part, axis=1),
    )
    row_scale = lax.rsqrt(square_sum / D_MODEL + norm_eps)[:, None]
    positions = lax.axis_index("sp") * tok_rows + jnp.arange(tok_rows, dtype=jnp.int32)
    cos_table, sine_table = rotary_tables(positions, ROT_DIM // 2)
    latent = (
        latent_raw
        * lax.rsqrt(jnp.mean(latent_raw * latent_raw, axis=1, keepdims=True) + norm_eps)
        * kv_gain[None, :]
    ).astype(jnp.bfloat16)
    key_rot = rotate_half(rot_acc * row_scale, cos_table, sine_table).astype(jnp.bfloat16)
    gated_input = (value_acc * row_scale * jax.nn.sigmoid(gate_acc * row_scale)).astype(
        jnp.bfloat16
    )
    scale = LOG2E / math.sqrt(NOPE_DIM + ROT_DIM)
    q_rot = rotate_half(
        (qrot_acc * row_scale).reshape(tok_rows, heads_here, ROT_DIM),
        cos_table[:, None, :],
        sine_table[:, None, :],
    )
    q_nope = (q_acc * row_scale).reshape(tok_rows, heads_here, NOPE_DIM)
    packed_queries = (
        jnp.concatenate([q_nope, q_rot, jnp.zeros((tok_rows, heads_here, 32), jnp.float32)], axis=2)
        * scale
    ).astype(jnp.bfloat16).reshape(tok_rows, 256)
    t = lax.axis_index("tp")
    mine = lax.dynamic_slice_in_dim(latent, t * 48, 48, 0)
    folds = key_rot.reshape(6, 4, 16, 32).transpose(0, 2, 1, 3).reshape(6, 16, 128)
    fold = lax.dynamic_index_in_dim(folds, jnp.minimum(t, 5), 0, keepdims=False)
    share = jnp.concatenate([mine[:, :128], mine[:, 128:], fold], axis=0)

    def square_rows(matrix):
        wide_rows = matrix.astype(jnp.float32)
        return jnp.sum(wide_rows * wide_rows, axis=1)

    rim_rows = shifted(gated_input[tok_rows - (KERNEL - 1) :], "sp", 1)
    padded = jnp.concatenate([rim_rows, gated_input], axis=0)
    conv_out = jnp.zeros((tok_rows, chan_here), jnp.float32)
    for tap_idx in range(KERNEL):
        conv_out = conv_out + conv_taps[tap_idx][None, :] * padded[
            tap_idx : tap_idx + tok_rows
        ].astype(jnp.float32)
    moment_one, moment_two = in_one(
        (jnp.sum(conv_out, axis=1), jnp.sum(conv_out * conv_out, axis=1)), "tp"
    )
    mean_val = moment_one / CONV_CH
    spread = moment_two / CONV_CH - mean_val * mean_val
    normed = (conv_out - mean_val[:, None]) * lax.rsqrt(spread + norm_eps)[:, None]
    swished = jax.nn.silu(normed * conv_ln_gain[None, :] + conv_ln_bias[None, :])
    attended = attention(packed_queries, share, key_up, value_up)
    att_sq, conv_sq = in_one((square_rows(attended), square_rows(swished)), "tp")
    att_mixed = (
        attended.astype(jnp.float32)
        * lax.rsqrt(att_sq / ATT_WIDTH + norm_eps)[:, None]
        * att_out_gain[None, :]
    ).astype(jnp.bfloat16)
    conv_mixed = (
        swished * lax.rsqrt(conv_sq / CONV_CH + norm_eps)[:, None] * conv_out_gain[None, :]
    ).astype(jnp.bfloat16)
    contract = (((0,), (1,)), ((), ()))
    feature_rows = summed_on_arrival(
        (
            lax.dot_general(att_out_weight, att_mixed, contract, preferred_element_type=jnp.float32)
            + lax.dot_general(
                conv_out_weight, conv_mixed, contract, preferred_element_type=jnp.float32
            )
        ).astype(jnp.bfloat16),
        "tp",
        0,
    )
    return feature_rows.T.astype(jnp.bfloat16)


def solution(mesh):
    return jax.shard_map(
        shards,
        mesh=mesh,
        in_specs=(
            P("sp", "tp"),
            P(),
            P(None, "tp"),
            P(None, "tp"),
            P(),
            P(),
            P(),
            P(None, "tp"),
            P(None, "tp"),
            P(None, "tp"),
            P(None, "tp"),
            P(None, "tp"),
            P("tp"),
            P("tp"),
            P("tp"),
            P("tp"),
            P("tp", None),
            P("tp", None),
        ),
        out_specs=P("sp", "tp"),
        check_vma=False,
    )
```

```python
import math

import jax
import jax.numpy as jnp
from jax import lax
from jax.experimental import pallas as pl
from jax.experimental.pallas import tpu as pltpu
from jax.sharding import PartitionSpec as P

D_MODEL = 2048
NOPE_DIM = 64
ROT_DIM = 32
VALUE_DIM = 64
CONV_CH = 1024
KERNEL = 31
ATT_WIDTH = 1024


norm_eps = 1e-06
far_below = -1e30
rope_base = 10000.0


def copy_for_each(x, axis):
    peers = lax.axis_size(axis)
    return lax.all_to_all(jnp.broadcast_to(x[None], (peers, *x.shape)), axis, 0, 0, tiled=True)


def in_order(pieces, dim):
    pieces = jnp.moveaxis(pieces, 0, dim)
    shape = pieces.shape
    return pieces.reshape(*shape[:dim], shape[dim] * shape[dim + 1], *shape[dim + 2 :])


def gathered_copies(x, axis, dim):
    pieces = copy_for_each(x, axis)
    return in_order(pieces, dim)


def rotary_tables(positions, half_dim):
    frequency = rope_base ** (-jnp.arange(half_dim, dtype=jnp.float32) / half_dim)
    angles = positions.astype(jnp.float32)[:, None] * frequency[None, :]
    return (jnp.cos(angles), jnp.sin(angles))


def rotate_half(values, cos_table, sine_table):
    half_dim = cos_table.shape[-1]
    front_half = values[..., :half_dim]
    back_half = values[..., half_dim:]
    return jnp.concatenate(
        [
            front_half * cos_table - back_half * sine_table,
            back_half * cos_table + front_half * sine_table,
        ],
        axis=-1,
    )


MESH = pl.DeviceIdType.MESH
ROWS = 384
SHARE = 112
KSETS = 16
PIECE = 4 * ROWS
LOG2E = 1.4426950408889634


def ring_peers(tp):
    x, c = tp // 2, tp % 2
    right = ((x + 1) % 4) * 2 + c
    left = ((x + 3) % 4) * 2 + c
    far = ((x + 2) % 4) * 2 + c
    partner = x * 2 + (1 - c)
    return right, left, far, partner


class RingGather:
    def __init__(self, buf, lo, hi, mid, send, recv, sp, tp):
        self.buf, self.lo, self.hi, self.mid = buf, lo, hi, mid
        self.send, self.recv, self.sp, self.tp = send, recv, sp, tp
        self.right, self.left, self.far, self.partner = ring_peers(tp)

    def piece(self, slot, part=None):
        lo, hi = {None: (self.lo, self.hi), 0: (self.lo, self.mid), 1: (self.mid, self.hi)}[part]
        return self.buf.at[slot, pl.ds(lo, hi - lo)]

    def copy(self, slot, part, sem, to):
        return pltpu.make_async_remote_copy(
            src_ref=self.piece(slot, part),
            dst_ref=self.piece(slot, part),
            send_sem=self.send.at[sem],
            recv_sem=self.recv.at[sem],
            device_id=(self.sp, to),
            device_id_type=MESH,
        )

    def begin(self):
        self.copy(self.tp, None, 0, self.right).start()
        self.copy(self.tp, None, 1, self.left).start()
        self.copy(self.tp, None, 2, self.partner).start()

    def relay(self):
        self.copy(self.left, None, 0, self.right).wait_recv()
        self.copy(self.left, 0, 5, self.right).start()
        self.copy(self.left, None, 3, self.partner).start()
        self.copy(self.right, None, 1, self.left).wait_recv()
        self.copy(self.right, 1, 6, self.left).start()
        self.copy(self.right, None, 4, self.partner).start()

    def relay_far(self):
        self.copy(self.far, 0, 5, self.right).wait_recv()
        self.copy(self.far, 0, 7, self.partner).start()
        self.copy(self.far, 1, 6, self.left).wait_recv()
        self.copy(self.far, 1, 8, self.partner).start()

    def finish(self):
        for sem, part in ((2, None), (3, None), (4, None), (7, 0), (8, 1)):
            self.copy(self.far, part, sem, self.partner).wait_recv()

    def drain(self):
        for sem, part in ((0, None), (1, None), (2, None), (3, None), (4, None), (5, 0), (6, 1), (7, 0), (8, 1)):
            self.copy(self.tp, part, sem, self.partner).wait_send()


def member_z(member, kind):
    return 2 * member + (kind + member) % 2


def layer_kernel(
    q_ref, share_ref, gated_ref, key_up_ref, value_up_ref, taps_ref, ln_gain_ref, ln_bias_ref,
    att_gain_ref, conv_gain_ref, att_w_ref, conv_w_ref, out_ref,
    qraw, qbuf, kbuf, kk, vv, wkv, top, acc, o_send, l_send, o_recv, l_recv, own_out, own_lse,
    halo, padded, conv_out, mom_send, mom_recv, cbuf, abuf, weights, gains, gain_all, branch,
    q_ssem, q_rsem, k_ssem, k_rsem, f_ssem, f_rsem, ag_ssem, ag_rsem, o_ssem, o_rsem, l_ssem, l_rsem,
    h_ssem, h_rsem, m_ssem, m_rsem, c_ssem, c_rsem, a_ssem, a_rsem, w_ssem, w_rsem, g_ssem, g_rsem,
    own_sem,
):
    sp, tp = lax.axis_index("sp"), lax.axis_index("tp")
    z, y = sp // 8, sp % 8
    kind, mine, parity = (z + z // 2) % 2, z // 2, y % 2
    residue = (y // 2 + mine) % 4
    bf, f32 = jnp.bfloat16, jnp.float32

    def member_sp(member):
        return member_z(member, kind) * 8 + y

    key_peers = []
    for dz in range(8):
        zz = (z + dz) % 8
        key_peers.append(zz * 8 + 2 * ((residue + 4 - zz // 2) % 4) + parity)
    pair = z * 8 + (y + 1 - 2 * parity)
    after, before_sp = (sp + 1) % 64, (sp + 63) % 64

    barrier = pltpu.get_barrier_semaphore()
    for i in range(1, 4):
        pl.semaphore_signal(
            barrier, inc=1, device_id=(member_sp((mine + i) % 4), tp), device_id_type=MESH
        )
    for i in range(1, 8):
        pl.semaphore_signal(barrier, inc=1, device_id=(key_peers[i], tp), device_id_type=MESH)
        pl.semaphore_signal(barrier, inc=1, device_id=(sp, (tp + i) % 8), device_id_type=MESH)
    pl.semaphore_signal(barrier, inc=1, device_id=(pair, tp), device_id_type=MESH)
    pl.semaphore_signal(barrier, inc=1, device_id=(before_sp, tp), device_id_type=MESH)
    pl.semaphore_wait(barrier, 19)

    def remote(src, dst, ssem, rsem, to):
        return pltpu.make_async_remote_copy(
            src_ref=src, dst_ref=dst, send_sem=ssem, recv_sem=rsem, device_id=to, device_id_type=MESH
        )

    halo_copy = remote(gated_ref.at[pl.ds(ROWS - 32, 32)], halo, h_ssem, h_rsem, (after, tp))
    halo_copy.start()

    slot = 4 * mine + 2 * parity + z % 2

    def key_copy(i):
        return remote(
            share_ref, kbuf.at[tp, slot], k_ssem.at[i], k_rsem.at[mine], (key_peers[i], tp)
        )

    pltpu.make_async_copy(share_ref, kbuf.at[tp, slot], k_rsem.at[mine]).start()
    for i in range(1, 8):
        key_copy(i).start()

    def query_copy(i):
        return remote(
            q_ref, qraw.at[i - 1], q_ssem.at[i - 1], q_rsem.at[i - 1], (member_sp((mine + i) % 4), tp)
        )

    for i in range(1, 4):
        query_copy(i).start()

    gains[...] = jnp.zeros(gains.shape, f32)
    gains[0:1, :] = att_gain_ref[...]
    gains[1:2, :] = conv_gain_ref[...]
    lane = lax.broadcasted_iota(jnp.int32, (256, 128), 1)
    for n, ref in enumerate((key_up_ref, value_up_ref)):
        w = ref[...].astype(f32)
        wkv[:, pl.ds(256 * n, 128)] = jnp.where(lane < 64, w, 0.0).astype(bf)
        wkv[:, pl.ds(256 * n + 128, 128)] = jnp.where(lane < 64, pltpu.roll(w, 64, 1), 0.0).astype(bf)

    tag = lax.broadcasted_iota(jnp.int32, (ROWS, 128), 1)
    low = tag < 64

    def unpack(ref, member):
        nope = ref[0:ROWS, :].astype(f32)
        fold = ref[ROWS : ROWS + ROWS // 2, :].astype(f32)
        for h in range(2):
            body = nope if h == 0 else pltpu.roll(nope, 64, 1)
            upper = pltpu.roll(fold, 64 - 32 * h, 1)
            lower = fold if h == 0 else pltpu.roll(fold, 96, 1)
            rotary = jnp.concatenate([upper, lower], axis=0)
            qbuf[member, h] = jnp.where(low, body, jnp.where(tag < 96, rotary, 0.0)).astype(bf)

    unpack(q_ref, mine)

    halo_copy.wait_recv()
    edge = halo[...].astype(f32)
    padded[0:32, :] = jnp.where(sp > 0, edge, jnp.zeros_like(edge))
    padded[pl.ds(32, ROWS), :] = gated_ref[...].astype(f32)
    total = jnp.zeros((ROWS, 128), f32)
    for tap in range(KERNEL):
        total = total + taps_ref[tap : tap + 1, :] * padded[pl.ds(tap + 2, ROWS), :]
    conv_out[...] = total
    sum_one = jnp.sum(total, axis=1, keepdims=True)
    sum_two = jnp.sum(total * total, axis=1, keepdims=True)
    mom_send[...] = jnp.transpose(jnp.where(tag == 0, sum_one, sum_two))[0:8, :]

    def forward(p):
        piece = kbuf.at[tp, pl.ds(4 * p + 2 * parity, 2)]
        return remote(piece, piece, f_ssem.at[p], f_rsem.at[p], (pair, tp))

    for p in range(4):
        piece = kbuf.at[tp, pl.ds(4 * p + 2 * parity, 2)]
        pltpu.make_async_copy(piece, piece, k_rsem.at[p]).wait()
        forward(p).start()

    def moment_copy(j):
        return remote(
            mom_send, mom_recv.at[tp], m_ssem.at[j], m_rsem.at[tp], (sp, (tp + j) % 8)
        )

    for j in range(1, 8):
        moment_copy(j).start()

    gathers = [
        RingGather(kbuf, 4 * p, 4 * p + 4, 4 * p + 2, ag_ssem.at[p], ag_rsem.at[p], sp, tp)
        for p in range(4)
    ]
    conv_gather = RingGather(cbuf, 0, ROWS, ROWS // 2, c_ssem, c_rsem, sp, tp)
    att_gather = RingGather(abuf, 0, ROWS, ROWS // 2, a_ssem, a_rsem, sp, tp)

    def begin(p):
        forward(p).wait_recv()
        gathers[p].begin()

    def assemble(p):
        slots = [4 * p + u for u in range(4)]
        first = jnp.concatenate([kbuf[:, s, 0:48, :].reshape(ROWS, 128) for s in slots], axis=0)
        second = jnp.concatenate([kbuf[:, s, 48:96, :].reshape(ROWS, 128) for s in slots], axis=0)
        product = jnp.dot(
            jnp.concatenate([first, second], axis=1), wkv[...], preferred_element_type=f32
        )
        pieces = []
        for s in slots:
            folded = kbuf[0:6, s, 96:112, :].astype(f32).reshape(96, 128)
            turned = [
                pltpu.roll(folded, (64 - 32 * j) % 128, 1).reshape(6, 1, 16, 128) for j in range(4)
            ]
            pieces.append(jnp.concatenate(turned, axis=1).reshape(ROWS, 128))
        rotary = jnp.concatenate(pieces, axis=0)
        front = lax.broadcasted_iota(jnp.int32, (PIECE, 128), 1) < 64
        for h in range(2):
            kk[h, pl.ds(p * PIECE, PIECE), :] = jnp.where(
                front, product[:, 128 * h : 128 * h + 128], rotary
            ).astype(bf)
            vv[h, pl.ds(p * PIECE, PIECE), :] = jnp.where(
                front, product[:, 256 + 128 * h : 384 + 128 * h], 1.0
            ).astype(bf)

    def step(member, p, masked):
        if masked:
            offset = lax.broadcasted_iota(jnp.int32, (ROWS, ROWS), 1) - lax.broadcasted_iota(
                jnp.int32, (ROWS, ROWS), 0
            )
            block = member_sp(member)
        for h in range(2):
            scores = lax.dot_general(
                qbuf[member, h],
                kk[h, pl.ds(p * PIECE, PIECE), :],
                (((1,), (1,)), ((), ())),
                preferred_element_type=f32,
            )
            if masked:
                columns = []
                for u in range(4):
                    key_block = (2 * p + u % 2) * 8 + 2 * ((residue + 4 - p) % 4) + u // 2
                    columns.append(
                        jnp.where(
                            offset <= (block - key_block) * ROWS,
                            scores[:, ROWS * u : ROWS * u + ROWS],
                            far_below,
                        )
                    )
                scores = jnp.concatenate(columns, axis=1)
            now = jnp.broadcast_to(jnp.max(scores, axis=1, keepdims=True), (ROWS, 128))
            if p > 0:
                before = top[member, h]
                now = jnp.maximum(before, now)
            top[member, h] = now
            likely = jnp.exp2(scores - jnp.concatenate([now] * (PIECE // 128), axis=1)).astype(bf)
            fresh = jnp.dot(likely, vv[h, pl.ds(p * PIECE, PIECE), :], preferred_element_type=f32)
            if p > 0:
                fresh = acc[member, h] * jnp.exp2(before - now) + fresh
            acc[member, h] = fresh

    def back_copies(member, source):
        to = (member_sp(member), tp)
        return (
            remote(o_send.at[member], o_recv.at[source], o_ssem.at[member], o_rsem.at[source], to),
            remote(l_send.at[member], l_recv.at[source], l_ssem.at[member], l_rsem.at[source], to),
        )

    def finalize(member):
        sums, tops = [], []
        for h in range(2):
            a = acc[member, h]
            part = jnp.where(low, pltpu.roll(a, 64, 1), a)
            sums.append(part)
            tops.append(top[member, h] + jnp.log2(part))
        value = jnp.where(low, acc[member, 0], pltpu.roll(acc[member, 1], 64, 1))
        value = value / jnp.where(low, sums[0], sums[1])
        o_send[member] = value.astype(bf)
        l_send[member] = jnp.transpose(jnp.where(tag < 4, tops[0], tops[1]))[0:8, :]

        @pl.when(mine == member)
        def _():
            own_out[...] = value
            own_lse[...] = jnp.where(low, tops[0], tops[1])

        @pl.when(mine != member)
        def _():
            for copy in back_copies(member, mine):
                copy.start()

    def weight_copies(j):
        to = (sp, (tp + j) % 8)
        columns = pl.ds(pl.multiple_of(256 * ((tp + j) % 8), 256), 256)
        return (
            remote(att_w_ref.at[:, columns], weights.at[0, tp], w_ssem.at[0, j], w_rsem.at[0, tp], to),
            remote(conv_w_ref.at[:, columns], weights.at[1, tp], w_ssem.at[1, j], w_rsem.at[1, tp], to),
            remote(gains, gain_all.at[tp], g_ssem.at[j], g_rsem.at[tp], to),
        )

    own_columns = pl.ds(pl.multiple_of(256 * tp, 256), 256)
    own_weights = (
        pltpu.make_async_copy(att_w_ref.at[:, own_columns], weights.at[0, tp], own_sem.at[0]),
        pltpu.make_async_copy(conv_w_ref.at[:, own_columns], weights.at[1, tp], own_sem.at[1]),
    )

    begin(0)
    gathers[0].relay()
    begin(1)
    gathers[0].relay_far()
    gathers[0].finish()
    assemble(0)
    gathers[1].relay()
    begin(2)
    step(mine, 0, True)
    gathers[1].relay_far()

    mom_recv[tp] = mom_send[...]
    for j in range(1, 8):
        source = (tp + j) % 8
        remote(mom_send, mom_recv.at[source], m_ssem.at[j], m_rsem.at[source], (sp, source)).wait_recv()
    moments = mom_recv[0]
    for t in range(1, 8):
        moments = moments + mom_recv[t]
    columns = jnp.transpose(moments)
    mean_val = columns[:, 0:1] / CONV_CH
    spread = columns[:, 1:2] / CONV_CH - mean_val * mean_val
    normed = (conv_out[...] - mean_val) * lax.rsqrt(spread + norm_eps)
    swished = jax.nn.silu(normed * ln_gain_ref[...] + ln_bias_ref[...])
    cbuf[tp] = swished.astype(bf)

    def arrive(i):
        query_copy(i).wait_recv()
        member = (mine + 4 - i) % 4
        unpack(qraw.at[i - 1], member)
        return member

    step(arrive(1), 0, True)
    gathers[2].relay()
    begin(3)
    step(arrive(3), 0, True)
    gathers[2].relay_far()
    gathers[3].relay()
    conv_gather.begin()
    for copy in own_weights:
        copy.start()
    step(arrive(2), 0, True)
    gathers[3].relay_far()
    conv_gather.relay()
    for j in range(1, 8):
        for copy in weight_copies(j):
            copy.start()
    finalize(0)
    gathers[1].finish()
    assemble(1)
    step(1, 1, True)
    conv_gather.relay_far()
    finalize(1)
    step(2, 1, False)
    step(3, 1, False)
    gathers[2].finish()
    assemble(2)
    step(2, 2, True)
    finalize(2)
    step(3, 2, False)
    gathers[3].finish()
    assemble(3)
    step(3, 3, True)
    finalize(3)

    gain_all[tp] = gains[...]
    conv_gather.finish()
    for copy in own_weights:
        copy.wait()
    for j in range(1, 8):
        source = (tp + j) % 8
        for n in range(2):
            remote(
                weights.at[n, source], weights.at[n, source], w_ssem.at[n, j], w_rsem.at[n, source], (sp, source)
            ).wait_recv()
        remote(gains, gain_all.at[source], g_ssem.at[j], g_rsem.at[source], (sp, source)).wait_recv()

    def product(buf, n):
        wide = jnp.concatenate([buf[t] for t in range(8)], axis=1).astype(f32)
        gain = jnp.concatenate([gain_all[t, n : n + 1, :] for t in range(8)], axis=1)
        power = jnp.sum(wide * wide, axis=1, keepdims=True)
        mixed = (wide * lax.rsqrt(power / CONV_CH + norm_eps) * gain).astype(bf)
        return jnp.dot(mixed, weights[n].reshape(1024, 256), preferred_element_type=f32)

    branch[...] = product(cbuf, 1)

    logs, values = [own_lse[...]], [own_out[...]]
    for i in range(1, 4):
        source = (mine + i) % 4
        for copy in back_copies(source, source):
            copy.wait_recv()
        columns = jnp.transpose(l_recv[source])
        logs.append(jnp.where(low, columns[:, 0:1], columns[:, 4:5]))
        values.append(o_recv[source].astype(f32))
    peak = jnp.maximum(jnp.maximum(logs[0], logs[1]), jnp.maximum(logs[2], logs[3]))
    shares = [jnp.exp2(log - peak) for log in logs]
    merged = sum(s * v for s, v in zip(shares, values)) / sum(shares)
    abuf[tp] = merged.astype(bf)

    att_gather.begin()
    att_gather.relay()
    att_gather.relay_far()
    att_gather.finish()
    out_ref[...] = (branch[...] + product(abuf, 0)).astype(bf)

    halo_copy.wait_send()
    for i in range(1, 8):
        key_copy(i).wait_send()
        moment_copy(i).wait_send()
        for copy in weight_copies(i):
            copy.wait_send()
    for p in range(4):
        forward(p).wait_send()
        gathers[p].drain()
    for i in range(1, 4):
        query_copy(i).wait_send()
        member = (mine + i) % 4
        for copy in back_copies(member, mine):
            copy.wait_send()
    conv_gather.drain()
    att_gather.drain()


def layer(*args):
    vmem, anywhere = pl.BlockSpec(memory_space=pltpu.VMEM), pl.BlockSpec(memory_space=pl.ANY)
    bf, f32 = jnp.bfloat16, jnp.float32
    dma = pltpu.SemaphoreType.DMA
    return pl.pallas_call(
        layer_kernel,
        out_shape=jax.ShapeDtypeStruct((ROWS, 256), bf),
        in_specs=[vmem] * 10 + [anywhere] * 2,
        out_specs=vmem,
        scratch_shapes=[
            pltpu.VMEM((3, ROWS + ROWS // 2, 128), bf),
            pltpu.VMEM((4, 2, ROWS, 128), bf),
            pltpu.VMEM((8, KSETS, SHARE, 128), bf),
            pltpu.VMEM((2, KSETS * ROWS, 128), bf),
            pltpu.VMEM((2, KSETS * ROWS, 128), bf),
            pltpu.VMEM((256, 512), bf),
            pltpu.VMEM((4, 2, ROWS, 128), f32),
            pltpu.VMEM((4, 2, ROWS, 128), f32),
            pltpu.VMEM((4, ROWS, 128), bf),
            pltpu.VMEM((4, 8, ROWS), f32),
            pltpu.VMEM((4, ROWS, 128), bf),
            pltpu.VMEM((4, 8, ROWS), f32),
            pltpu.VMEM((ROWS, 128), f32),
            pltpu.VMEM((ROWS, 128), f32),
            pltpu.VMEM((32, 128), bf),
            pltpu.VMEM((32 + ROWS, 128), f32),
            pltpu.VMEM((ROWS, 128), f32),
            pltpu.VMEM((8, ROWS), f32),
            pltpu.VMEM((8, 8, ROWS), f32),
            pltpu.VMEM((8, ROWS, 128), bf),
            pltpu.VMEM((8, ROWS, 128), bf),
            pltpu.VMEM((2, 8, 128, 256), bf),
            pltpu.VMEM((8, 128), f32),
            pltpu.VMEM((8, 8, 128), f32),
            pltpu.VMEM((ROWS, 256), f32),
            dma((3,)), dma((3,)), dma((8,)), dma((4,)), dma((4,)), dma((4,)), dma((4, 9)), dma((4, 9)),
            dma((4,)), dma((4,)), dma((4,)), dma((4,)), dma, dma, dma((8,)), dma((8,)),
            dma((9,)), dma((9,)), dma((9,)), dma((9,)), dma((2, 8)), dma((2, 8)), dma((8,)), dma((8,)),
            dma((2,)),
        ],
        compiler_params=pltpu.CompilerParams(collective_id=1, has_side_effects=True),
        name="layer",
    )(*args)


def shards(
    tokens,
    input_gain,
    query_weight,
    query_rot_weight,
    kv_down,
    rot_down,
    kv_gain,
    key_up,
    value_up,
    conv_value_weight,
    conv_gate_weight,
    conv_taps,
    conv_ln_gain,
    conv_ln_bias,
    att_out_gain,
    conv_out_gain,
    att_out_weight,
    conv_out_weight,
):
    tok_rows = tokens.shape[0]
    heads_here = key_up.shape[1] // NOPE_DIM
    weight_list = (
        query_weight,
        query_rot_weight,
        kv_down,
        rot_down,
        conv_value_weight,
        conv_gate_weight,
    )
    wide_part = gathered_copies(tokens, "tp", 1).astype(jnp.float32)
    scaled = (wide_part * input_gain[None, :]).astype(jnp.bfloat16)

    def add_product(weight):
        return jnp.dot(scaled, weight, preferred_element_type=jnp.float32)

    summed = tuple((add_product(weight) for weight in weight_list))
    q_acc, qrot_acc, latent_raw, rot_acc, value_acc, gate_acc, square_sum = summed + (
        jnp.sum(wide_part * wide_part, axis=1),
    )
    row_scale = lax.rsqrt(square_sum / D_MODEL + norm_eps)[:, None]
    positions = lax.axis_index("sp") * tok_rows + jnp.arange(tok_rows, dtype=jnp.int32)
    cos_table, sine_table = rotary_tables(positions, ROT_DIM // 2)
    latent = (
        latent_raw
        * lax.rsqrt(jnp.mean(latent_raw * latent_raw, axis=1, keepdims=True) + norm_eps)
        * kv_gain[None, :]
    ).astype(jnp.bfloat16)
    key_rot = rotate_half(rot_acc * row_scale, cos_table, sine_table).astype(jnp.bfloat16)
    gated_input = (value_acc * row_scale * jax.nn.sigmoid(gate_acc * row_scale)).astype(
        jnp.bfloat16
    )
    scale = LOG2E / math.sqrt(NOPE_DIM + ROT_DIM)
    q_rot = rotate_half(
        (qrot_acc * (row_scale * scale)).reshape(tok_rows, heads_here, ROT_DIM),
        cos_table[:, None, :],
        sine_table[:, None, :],
    ).reshape(tok_rows, heads_here * ROT_DIM)
    q_rot = jnp.concatenate([q_rot[: tok_rows // 2], q_rot[tok_rows // 2 :]], axis=1)
    packed = jnp.concatenate([q_acc * (row_scale * scale), q_rot], axis=0).astype(jnp.bfloat16)
    t = lax.axis_index("tp")
    mine = lax.dynamic_slice_in_dim(latent, t * 48, 48, 0)
    folds = key_rot.reshape(6, 4, 16, 32).transpose(0, 2, 1, 3).reshape(6, 16, 128)
    fold = lax.dynamic_index_in_dim(folds, jnp.minimum(t, 5), 0, keepdims=False)
    share = jnp.concatenate([mine[:, :128], mine[:, 128:], fold], axis=0)
    return layer(
        packed,
        share,
        gated_input,
        key_up,
        value_up,
        conv_taps,
        conv_ln_gain[None, :],
        conv_ln_bias[None, :],
        att_out_gain[None, :],
        conv_out_gain[None, :],
        att_out_weight,
        conv_out_weight,
    )


def solution(mesh):
    return jax.shard_map(
        shards,
        mesh=mesh,
        in_specs=(
            P("sp", "tp"),
            P(),
            P(None, "tp"),
            P(None, "tp"),
            P(),
            P(),
            P(),
            P(None, "tp"),
            P(None, "tp"),
            P(None, "tp"),
            P(None, "tp"),
            P(None, "tp"),
            P("tp"),
            P("tp"),
            P("tp"),
            P("tp"),
            P("tp", None),
            P("tp", None),
        ),
        out_specs=P("sp", "tp"),
        check_vma=False,
    )
```

```python
import math

import jax
import jax.numpy as jnp
import numpy as np
from jax import lax
from jax.experimental import pallas as pl
from jax.experimental.pallas import tpu as pltpu
from jax.sharding import PartitionSpec as P

D_MODEL = 2048
NOPE_DIM = 64
ROT_DIM = 32
CONV_CH = 1024
KERNEL = 31

norm_eps = 1e-06
far_below = -1e30
rope_base = 10000.0


MESH = pl.DeviceIdType.MESH
ROWS = 384
SHARE = 112
KSETS = 16
PIECE = 4 * ROWS
SCALE = 1.4426950408889634 / math.sqrt(NOPE_DIM + ROT_DIM)


def ring_peers(tp):
    x, c = tp // 2, tp % 2
    right = ((x + 1) % 4) * 2 + c
    left = ((x + 3) % 4) * 2 + c
    far = ((x + 2) % 4) * 2 + c
    partner = x * 2 + (1 - c)
    return right, left, far, partner


class RingGather:
    def __init__(self, buf, lo, hi, mid, send, recv, sp, tp):
        self.buf, self.lo, self.hi, self.mid = buf, lo, hi, mid
        self.send, self.recv, self.sp, self.tp = send, recv, sp, tp
        self.right, self.left, self.far, self.partner = ring_peers(tp)

    def piece(self, slot, part=None):
        lo, hi = {None: (self.lo, self.hi), 0: (self.lo, self.mid), 1: (self.mid, self.hi)}[part]
        return self.buf.at[slot, pl.ds(lo, hi - lo)]

    def copy(self, slot, part, sem, to):
        return pltpu.make_async_remote_copy(
            src_ref=self.piece(slot, part),
            dst_ref=self.piece(slot, part),
            send_sem=self.send.at[sem],
            recv_sem=self.recv.at[sem],
            device_id=(self.sp, to),
            device_id_type=MESH,
        )

    def begin(self):
        self.copy(self.tp, None, 0, self.right).start()
        self.copy(self.tp, None, 1, self.left).start()
        self.copy(self.tp, None, 2, self.partner).start()

    def relay(self):
        self.copy(self.left, None, 0, self.right).wait_recv()
        self.copy(self.left, 0, 5, self.right).start()
        self.copy(self.left, None, 3, self.partner).start()
        self.copy(self.right, None, 1, self.left).wait_recv()
        self.copy(self.right, 1, 6, self.left).start()
        self.copy(self.right, None, 4, self.partner).start()

    def relay_far(self):
        self.copy(self.far, 0, 5, self.right).wait_recv()
        self.copy(self.far, 0, 7, self.partner).start()
        self.copy(self.far, 1, 6, self.left).wait_recv()
        self.copy(self.far, 1, 8, self.partner).start()

    def finish(self):
        for sem, part in ((2, None), (3, None), (4, None), (7, 0), (8, 1)):
            self.copy(self.far, part, sem, self.partner).wait_recv()

    def drain(self):
        for sem, part in ((0, None), (1, None), (2, None), (3, None), (4, None), (5, 0), (6, 1), (7, 0), (8, 1)):
            self.copy(self.tp, part, sem, self.partner).wait_send()


def member_z(member, kind):
    return 2 * member + (kind + member) % 2


def layer_kernel(
    tokens_hbm, query_hbm, query_rot_hbm, kv_down_hbm, rot_down_hbm, key_up_hbm, value_up_hbm,
    conv_value_hbm, conv_gate_hbm, att_w_ref, conv_w_ref, near_cos_hbm, near_sin_hbm,
    base_cos_ref, base_sin_ref, input_gain_ref, kv_gain_ref,
    taps_ref, ln_gain_ref, ln_bias_ref, att_gain_ref, conv_gain_ref, out_ref,
    tbuf, scaled, wall, wqr, wrd, wkvd, kup, vup, near_cos, near_sin, spun,
    q_ref, share_ref, gated_ref,
    qraw, qbuf, kbuf, kk, vv, wkv, top, acc, o_send, l_send, o_recv, l_recv, own_out, own_lse,
    halo, padded, conv_out, mom_send, mom_recv, cbuf, abuf, weights, gains, gain_all, branch,
    q_ssem, q_rsem, k_ssem, k_rsem, f_ssem, f_rsem, ag_ssem, ag_rsem, o_ssem, o_rsem, l_ssem, l_rsem,
    h_ssem, h_rsem, m_ssem, m_rsem, c_ssem, c_rsem, a_ssem, a_rsem, w_ssem, w_rsem, g_ssem, g_rsem,
    own_sem, t_ssem, t_rsem, load_sem,
):
    sp, tp = lax.axis_index("sp"), lax.axis_index("tp")
    z, y = sp // 8, sp % 8
    kind, mine, parity = (z + z // 2) % 2, z // 2, y % 2
    residue = (y // 2 + mine) % 4
    bf, f32 = jnp.bfloat16, jnp.float32

    def member_sp(member):
        return member_z(member, kind) * 8 + y

    key_peers = []
    for dz in range(8):
        zz = (z + dz) % 8
        key_peers.append(zz * 8 + 2 * ((residue + 4 - zz // 2) % 4) + parity)
    pair = z * 8 + (y + 1 - 2 * parity)
    after, before_sp = (sp + 1) % 64, (sp + 63) % 64

    loads = [
        pltpu.make_async_copy(src, dst, load_sem.at[n])
        for n, (src, dst) in enumerate(
            (
                (tokens_hbm, tbuf.at[tp]),
                (query_rot_hbm, wqr),
                (rot_down_hbm, wrd),
                (key_up_hbm, kup),
                (value_up_hbm, vup),
                (query_hbm, wall.at[:, pl.ds(0, 128)]),
                (conv_value_hbm, wall.at[:, pl.ds(128, 128)]),
                (conv_gate_hbm, wall.at[:, pl.ds(256, 128)]),
                (kv_down_hbm, wkvd),
                (near_cos_hbm, near_cos),
                (near_sin_hbm, near_sin),
            )
        )
    ]
    for load in loads:
        load.start()

    barrier = pltpu.get_barrier_semaphore()
    for i in range(1, 4):
        pl.semaphore_signal(
            barrier, inc=1, device_id=(member_sp((mine + i) % 4), tp), device_id_type=MESH
        )
    for i in range(1, 8):
        pl.semaphore_signal(barrier, inc=1, device_id=(key_peers[i], tp), device_id_type=MESH)
        pl.semaphore_signal(barrier, inc=1, device_id=(sp, (tp + i) % 8), device_id_type=MESH)
    pl.semaphore_signal(barrier, inc=1, device_id=(pair, tp), device_id_type=MESH)
    pl.semaphore_signal(barrier, inc=1, device_id=(before_sp, tp), device_id_type=MESH)
    pl.semaphore_wait(barrier, 19)

    def remote(src, dst, ssem, rsem, to):
        return pltpu.make_async_remote_copy(
            src_ref=src, dst_ref=dst, send_sem=ssem, recv_sem=rsem, device_id=to, device_id_type=MESH
        )

    tokens_gather = RingGather(tbuf, 0, ROWS, ROWS // 2, t_ssem, t_rsem, sp, tp)
    loads[0].wait()
    tokens_gather.begin()

    gains[...] = jnp.zeros(gains.shape, f32)
    gains[0:1, :] = att_gain_ref[...]
    gains[1:2, :] = conv_gain_ref[...]
    loads[1].wait()
    loads[2].wait()
    wall[:, pl.ds(384, 128)] = jnp.concatenate(
        [wqr[...].astype(f32), wrd[...].astype(f32), jnp.zeros((D_MODEL, 32), f32)], axis=1
    ).astype(bf)
    loads[3].wait()
    loads[4].wait()
    lane = lax.broadcasted_iota(jnp.int32, (256, 128), 1)
    for n, ref in enumerate((kup, vup)):
        w = ref[...].astype(f32)
        wkv[:, pl.ds(256 * n, 128)] = jnp.where(lane < 64, w, 0.0).astype(bf)
        wkv[:, pl.ds(256 * n + 128, 128)] = jnp.where(lane < 64, pltpu.roll(w, 64, 1), 0.0).astype(bf)

    def scale_block(t):
        columns = pl.ds(pl.multiple_of(256 * t, 256), 256)
        x = tbuf[t].astype(f32)
        scaled[:, columns] = (x * input_gain_ref[:, columns]).astype(bf)
        return x * x

    squares = scale_block(tp)
    tokens_gather.relay()
    squares = squares + scale_block(tokens_gather.left)
    squares = squares + scale_block(tokens_gather.right)
    tokens_gather.relay_far()
    tokens_gather.finish()
    squares = squares + scale_block(tokens_gather.far)
    for t in (tp, tokens_gather.left, tokens_gather.right, tokens_gather.far):
        squares = squares + scale_block(t + 1 - 2 * (t % 2))
    row_scale = lax.rsqrt(jnp.sum(squares, axis=1, keepdims=True) / D_MODEL + norm_eps)

    for load in loads[5:]:
        load.wait()
    raw = jnp.dot(
        scaled[pl.ds(pl.multiple_of(48 * tp, 16), 48), :], wkvd[...], preferred_element_type=f32
    )
    power = jnp.sum(raw * raw, axis=1, keepdims=True) / 256
    latent = (raw * lax.rsqrt(power + norm_eps) * kv_gain_ref[...]).astype(bf)
    share_ref[0:48, :] = latent[:, 0:128]
    share_ref[48:96, :] = latent[:, 128:256]

    tag = lax.broadcasted_iota(jnp.int32, (ROWS, 128), 1)
    low = tag < 64
    sums = jnp.dot(scaled[...], wall[...], preferred_element_type=f32)
    flat = sums[:, 384:512] * row_scale
    cos_base, sin_base = base_cos_ref[pl.ds(sp, 1), :], base_sin_ref[pl.ds(sp, 1), :]
    cosine = near_cos[...] * cos_base - near_sin[...] * sin_base
    sine = near_sin[...] * cos_base + near_cos[...] * sin_base
    forward_half = tag % 32 < 16
    other = jnp.where(forward_half, pltpu.roll(flat, 112, 1), pltpu.roll(flat, 16, 1))
    turned_rows = flat * cosine + other * jnp.where(forward_half, -sine, sine)
    spun[...] = turned_rows
    short = lax.broadcasted_iota(jnp.int32, (16, 128), 1) // 32
    fold = jnp.zeros((16, 128), f32)
    first_row = 64 * jnp.minimum(tp, 5)
    for j in range(4):
        part = spun[pl.ds(pl.multiple_of(first_row + 16 * j, 16), 16), :]
        fold = jnp.where(short == j, pltpu.roll(part, (64 + 32 * j) % 128, 1), fold)
    share_ref[96:112, :] = fold.astype(bf)
    q_ref[0:ROWS, :] = (sums[:, 0:128] * (row_scale * SCALE)).astype(bf)
    half = ROWS // 2
    q_ref[ROWS : ROWS + half, :] = (
        jnp.where(low[0:half], turned_rows[0:half], pltpu.roll(turned_rows[half:ROWS], 64, 1)) * SCALE
    ).astype(bf)
    gated = (sums[:, 128:256] * row_scale * jax.nn.sigmoid(sums[:, 256:384] * row_scale)).astype(bf)
    gated_ref[...] = gated

    slot = 4 * mine + 2 * parity + z % 2

    def key_copy(i):
        return remote(
            share_ref, kbuf.at[tp, slot], k_ssem.at[i], k_rsem.at[mine], (key_peers[i], tp)
        )

    pltpu.make_async_copy(share_ref, kbuf.at[tp, slot], k_rsem.at[mine]).start()
    for i in range(1, 8):
        key_copy(i).start()

    halo_copy = remote(gated_ref.at[pl.ds(ROWS - 32, 32)], halo, h_ssem, h_rsem, (after, tp))
    halo_copy.start()

    def query_copy(i):
        return remote(
            q_ref, qraw.at[i - 1], q_ssem.at[i - 1], q_rsem.at[i - 1], (member_sp((mine + i) % 4), tp)
        )

    for i in range(1, 4):
        query_copy(i).start()

    def unpack(ref, member):
        nope = ref[0:ROWS, :].astype(f32)
        fold = ref[ROWS : ROWS + ROWS // 2, :].astype(f32)
        for h in range(2):
            body = nope if h == 0 else pltpu.roll(nope, 64, 1)
            upper = pltpu.roll(fold, 64 - 32 * h, 1)
            lower = fold if h == 0 else pltpu.roll(fold, 96, 1)
            rotary = jnp.concatenate([upper, lower], axis=0)
            qbuf[member, h] = jnp.where(low, body, jnp.where(tag < 96, rotary, 0.0)).astype(bf)

    unpack(q_ref, mine)

    halo_copy.wait_recv()
    edge = halo[...].astype(f32)
    padded[0:32, :] = jnp.where(sp > 0, edge, jnp.zeros_like(edge))
    padded[pl.ds(32, ROWS), :] = gated_ref[...].astype(f32)
    total = jnp.zeros((ROWS, 128), f32)
    for tap in range(KERNEL):
        total = total + taps_ref[tap : tap + 1, :] * padded[pl.ds(tap + 2, ROWS), :]
    conv_out[...] = total
    sum_one = jnp.sum(total, axis=1, keepdims=True)
    sum_two = jnp.sum(total * total, axis=1, keepdims=True)
    mom_send[...] = jnp.transpose(jnp.where(tag == 0, sum_one, sum_two))[0:8, :]

    def forward(p):
        piece = kbuf.at[tp, pl.ds(4 * p + 2 * parity, 2)]
        return remote(piece, piece, f_ssem.at[p], f_rsem.at[p], (pair, tp))

    for p in range(4):
        piece = kbuf.at[tp, pl.ds(4 * p + 2 * parity, 2)]
        pltpu.make_async_copy(piece, piece, k_rsem.at[p]).wait()
        forward(p).start()

    def moment_copy(j):
        return remote(
            mom_send, mom_recv.at[tp], m_ssem.at[j], m_rsem.at[tp], (sp, (tp + j) % 8)
        )

    for j in range(1, 8):
        moment_copy(j).start()

    gathers = [
        RingGather(kbuf, 4 * p, 4 * p + 4, 4 * p + 2, ag_ssem.at[p], ag_rsem.at[p], sp, tp)
        for p in range(4)
    ]
    conv_gather = RingGather(cbuf, 0, ROWS, ROWS // 2, c_ssem, c_rsem, sp, tp)
    att_gather = RingGather(abuf, 0, ROWS, ROWS // 2, a_ssem, a_rsem, sp, tp)

    def begin(p):
        forward(p).wait_recv()
        gathers[p].begin()

    def assemble(p):
        slots = [4 * p + u for u in range(4)]
        first = jnp.concatenate([kbuf[:, s, 0:48, :].reshape(ROWS, 128) for s in slots], axis=0)
        second = jnp.concatenate([kbuf[:, s, 48:96, :].reshape(ROWS, 128) for s in slots], axis=0)
        product = jnp.dot(
            jnp.concatenate([first, second], axis=1), wkv[...], preferred_element_type=f32
        )
        pieces = []
        for s in slots:
            folded = kbuf[0:6, s, 96:112, :].astype(f32).reshape(96, 128)
            turned = [
                pltpu.roll(folded, (64 - 32 * j) % 128, 1).reshape(6, 1, 16, 128) for j in range(4)
            ]
            pieces.append(jnp.concatenate(turned, axis=1).reshape(ROWS, 128))
        rotary = jnp.concatenate(pieces, axis=0)
        front = lax.broadcasted_iota(jnp.int32, (PIECE, 128), 1) < 64
        for h in range(2):
            kk[h, pl.ds(p * PIECE, PIECE), :] = jnp.where(
                front, product[:, 128 * h : 128 * h + 128], rotary
            ).astype(bf)
            vv[h, pl.ds(p * PIECE, PIECE), :] = jnp.where(
                front, product[:, 256 + 128 * h : 384 + 128 * h], 1.0
            ).astype(bf)

    def step(member, p, masked):
        if masked:
            offset = lax.broadcasted_iota(jnp.int32, (ROWS, ROWS), 1) - lax.broadcasted_iota(
                jnp.int32, (ROWS, ROWS), 0
            )
            block = member_sp(member)
        for h in range(2):
            scores = lax.dot_general(
                qbuf[member, h],
                kk[h, pl.ds(p * PIECE, PIECE), :],
                (((1,), (1,)), ((), ())),
                preferred_element_type=f32,
            )
            if masked:
                columns = []
                for u in range(4):
                    key_block = (2 * p + u % 2) * 8 + 2 * ((residue + 4 - p) % 4) + u // 2
                    columns.append(
                        jnp.where(
                            offset <= (block - key_block) * ROWS,
                            scores[:, ROWS * u : ROWS * u + ROWS],
                            far_below,
                        )
                    )
                scores = jnp.concatenate(columns, axis=1)
            now = jnp.broadcast_to(jnp.max(scores, axis=1, keepdims=True), (ROWS, 128))
            if p > 0:
                before = top[member, h]
                now = jnp.maximum(before, now)
            top[member, h] = now
            likely = jnp.exp2(scores - jnp.concatenate([now] * (PIECE // 128), axis=1)).astype(bf)
            fresh = jnp.dot(likely, vv[h, pl.ds(p * PIECE, PIECE), :], preferred_element_type=f32)
            if p > 0:
                fresh = acc[member, h] * jnp.exp2(before - now) + fresh
            acc[member, h] = fresh

    def back_copies(member, source):
        to = (member_sp(member), tp)
        return (
            remote(o_send.at[member], o_recv.at[source], o_ssem.at[member], o_rsem.at[source], to),
            remote(l_send.at[member], l_recv.at[source], l_ssem.at[member], l_rsem.at[source], to),
        )

    def finalize(member):
        sums, tops = [], []
        for h in range(2):
            a = acc[member, h]
            part = jnp.where(low, pltpu.roll(a, 64, 1), a)
            sums.append(part)
            tops.append(top[member, h] + jnp.log2(part))
        value = jnp.where(low, acc[member, 0], pltpu.roll(acc[member, 1], 64, 1))
        value = value / jnp.where(low, sums[0], sums[1])
        o_send[member] = value.astype(bf)
        l_send[member] = jnp.transpose(jnp.where(tag < 4, tops[0], tops[1]))[0:8, :]

        @pl.when(mine == member)
        def _():
            own_out[...] = value
            own_lse[...] = jnp.where(low, tops[0], tops[1])

        @pl.when(mine != member)
        def _():
            for copy in back_copies(member, mine):
                copy.start()

    def weight_copies(j):
        to = (sp, (tp + j) % 8)
        columns = pl.ds(pl.multiple_of(256 * ((tp + j) % 8), 256), 256)
        return (
            remote(att_w_ref.at[:, columns], weights.at[0, tp], w_ssem.at[0, j], w_rsem.at[0, tp], to),
            remote(conv_w_ref.at[:, columns], weights.at[1, tp], w_ssem.at[1, j], w_rsem.at[1, tp], to),
            remote(gains, gain_all.at[tp], g_ssem.at[j], g_rsem.at[tp], to),
        )

    own_columns = pl.ds(pl.multiple_of(256 * tp, 256), 256)
    own_weights = (
        pltpu.make_async_copy(att_w_ref.at[:, own_columns], weights.at[0, tp], own_sem.at[0]),
        pltpu.make_async_copy(conv_w_ref.at[:, own_columns], weights.at[1, tp], own_sem.at[1]),
    )

    begin(0)
    gathers[0].relay()
    begin(1)
    gathers[0].relay_far()
    gathers[0].finish()
    assemble(0)
    gathers[1].relay()
    begin(2)
    step(mine, 0, True)
    gathers[1].relay_far()

    mom_recv[tp] = mom_send[...]
    for j in range(1, 8):
        source = (tp + j) % 8
        remote(mom_send, mom_recv.at[source], m_ssem.at[j], m_rsem.at[source], (sp, source)).wait_recv()
    moments = mom_recv[0]
    for t in range(1, 8):
        moments = moments + mom_recv[t]
    columns = jnp.transpose(moments)
    mean_val = columns[:, 0:1] / CONV_CH
    spread = columns[:, 1:2] / CONV_CH - mean_val * mean_val
    normed = (conv_out[...] - mean_val) * lax.rsqrt(spread + norm_eps)
    swished = jax.nn.silu(normed * ln_gain_ref[...] + ln_bias_ref[...])
    cbuf[tp] = swished.astype(bf)

    def arrive(i):
        query_copy(i).wait_recv()
        member = (mine + 4 - i) % 4
        unpack(qraw.at[i - 1], member)
        return member

    step(arrive(1), 0, True)
    gathers[2].relay()
    begin(3)
    step(arrive(3), 0, True)
    gathers[2].relay_far()
    gathers[3].relay()
    conv_gather.begin()
    for copy in own_weights:
        copy.start()
    step(arrive(2), 0, True)
    gathers[3].relay_far()
    conv_gather.relay()
    for j in range(1, 8):
        for copy in weight_copies(j):
            copy.start()
    finalize(0)
    gathers[1].finish()
    assemble(1)
    step(1, 1, True)
    conv_gather.relay_far()
    finalize(1)
    step(2, 1, False)
    step(3, 1, False)
    gathers[2].finish()
    assemble(2)
    step(2, 2, True)
    finalize(2)
    step(3, 2, False)
    gathers[3].finish()
    assemble(3)
    step(3, 3, True)
    finalize(3)

    gain_all[tp] = gains[...]
    conv_gather.finish()
    for copy in own_weights:
        copy.wait()
    for j in range(1, 8):
        source = (tp + j) % 8
        for n in range(2):
            remote(
                weights.at[n, source], weights.at[n, source], w_ssem.at[n, j], w_rsem.at[n, source], (sp, source)
            ).wait_recv()
        remote(gains, gain_all.at[source], g_ssem.at[j], g_rsem.at[source], (sp, source)).wait_recv()

    def product(buf, n):
        wide = jnp.concatenate([buf[t] for t in range(8)], axis=1).astype(f32)
        gain = jnp.concatenate([gain_all[t, n : n + 1, :] for t in range(8)], axis=1)
        power = jnp.sum(wide * wide, axis=1, keepdims=True)
        mixed = (wide * lax.rsqrt(power / CONV_CH + norm_eps) * gain).astype(bf)
        return jnp.dot(mixed, weights[n].reshape(1024, 256), preferred_element_type=f32)

    branch[...] = product(cbuf, 1)

    logs, values = [own_lse[...]], [own_out[...]]
    for i in range(1, 4):
        source = (mine + i) % 4
        for copy in back_copies(source, source):
            copy.wait_recv()
        columns = jnp.transpose(l_recv[source])
        logs.append(jnp.where(low, columns[:, 0:1], columns[:, 4:5]))
        values.append(o_recv[source].astype(f32))
    peak = jnp.maximum(jnp.maximum(logs[0], logs[1]), jnp.maximum(logs[2], logs[3]))
    shares = [jnp.exp2(log - peak) for log in logs]
    merged = sum(s * v for s, v in zip(shares, values)) / sum(shares)
    abuf[tp] = merged.astype(bf)

    att_gather.begin()
    att_gather.relay()
    att_gather.relay_far()
    att_gather.finish()
    out_ref[...] = (branch[...] + product(abuf, 0)).astype(bf)

    tokens_gather.drain()
    halo_copy.wait_send()
    for i in range(1, 8):
        key_copy(i).wait_send()
        moment_copy(i).wait_send()
        for copy in weight_copies(i):
            copy.wait_send()
    for p in range(4):
        forward(p).wait_send()
        gathers[p].drain()
    for i in range(1, 4):
        query_copy(i).wait_send()
        member = (mine + i) % 4
        for copy in back_copies(member, mine):
            copy.wait_send()
    conv_gather.drain()
    att_gather.drain()


def layer(*args):
    vmem, anywhere = pl.BlockSpec(memory_space=pltpu.VMEM), pl.BlockSpec(memory_space=pl.ANY)
    bf, f32 = jnp.bfloat16, jnp.float32
    dma = pltpu.SemaphoreType.DMA
    return pl.pallas_call(
        layer_kernel,
        out_shape=jax.ShapeDtypeStruct((ROWS, 256), bf),
        in_specs=[anywhere] * 13 + [vmem] * 9,
        out_specs=vmem,
        scratch_shapes=[
            pltpu.VMEM((8, ROWS, 256), bf),
            pltpu.VMEM((ROWS, D_MODEL), bf),
            pltpu.VMEM((D_MODEL, 512), bf),
            pltpu.VMEM((D_MODEL, 64), bf),
            pltpu.VMEM((D_MODEL, 32), bf),
            pltpu.VMEM((D_MODEL, 256), bf),
            pltpu.VMEM((256, 128), bf),
            pltpu.VMEM((256, 128), bf),
            pltpu.VMEM((ROWS, 128), f32),
            pltpu.VMEM((ROWS, 128), f32),
            pltpu.VMEM((ROWS, 128), f32),
            pltpu.VMEM((ROWS + ROWS // 2, 128), bf),
            pltpu.VMEM((SHARE, 128), bf),
            pltpu.VMEM((ROWS, 128), bf),
            pltpu.VMEM((3, ROWS + ROWS // 2, 128), bf),
            pltpu.VMEM((4, 2, ROWS, 128), bf),
            pltpu.VMEM((8, KSETS, SHARE, 128), bf),
            pltpu.VMEM((2, KSETS * ROWS, 128), bf),
            pltpu.VMEM((2, KSETS * ROWS, 128), bf),
            pltpu.VMEM((256, 512), bf),
            pltpu.VMEM((4, 2, ROWS, 128), f32),
            pltpu.VMEM((4, 2, ROWS, 128), f32),
            pltpu.VMEM((4, ROWS, 128), bf),
            pltpu.VMEM((4, 8, ROWS), f32),
            pltpu.VMEM((4, ROWS, 128), bf),
            pltpu.VMEM((4, 8, ROWS), f32),
            pltpu.VMEM((ROWS, 128), f32),
            pltpu.VMEM((ROWS, 128), f32),
            pltpu.VMEM((32, 128), bf),
            pltpu.VMEM((32 + ROWS, 128), f32),
            pltpu.VMEM((ROWS, 128), f32),
            pltpu.VMEM((8, ROWS), f32),
            pltpu.VMEM((8, 8, ROWS), f32),
            pltpu.VMEM((8, ROWS, 128), bf),
            pltpu.VMEM((8, ROWS, 128), bf),
            pltpu.VMEM((2, 8, 128, 256), bf),
            pltpu.VMEM((8, 128), f32),
            pltpu.VMEM((8, 8, 128), f32),
            pltpu.VMEM((ROWS, 256), f32),
            dma((3,)), dma((3,)), dma((8,)), dma((4,)), dma((4,)), dma((4,)), dma((4, 9)), dma((4, 9)),
            dma((4,)), dma((4,)), dma((4,)), dma((4,)), dma, dma, dma((8,)), dma((8,)),
            dma((9,)), dma((9,)), dma((9,)), dma((9,)), dma((2, 8)), dma((2, 8)), dma((8,)), dma((8,)),
            dma((2,)), dma((9,)), dma((9,)), dma((11,)),
        ],
        compiler_params=pltpu.CompilerParams(collective_id=1, has_side_effects=True),
        name="layer",
    )(*args)


def rotary_tables():
    lanes = np.arange(128)
    frequency = rope_base ** (-(lanes % 16) / 16.0)
    near = np.arange(ROWS)[:, None] * frequency[None, :]
    base = (np.arange(64) * ROWS)[:, None] * frequency[None, :]
    return tuple(np.asarray(f(a), np.float32) for a in (near, base) for f in (np.cos, np.sin))


def shards(
    tokens,
    input_gain,
    query_weight,
    query_rot_weight,
    kv_down,
    rot_down,
    kv_gain,
    key_up,
    value_up,
    conv_value_weight,
    conv_gate_weight,
    conv_taps,
    conv_ln_gain,
    conv_ln_bias,
    att_out_gain,
    conv_out_gain,
    att_out_weight,
    conv_out_weight,
):
    near_cos, near_sin, base_cos, base_sin = rotary_tables()
    return layer(
        tokens,
        query_weight,
        query_rot_weight,
        kv_down,
        rot_down,
        key_up,
        value_up,
        conv_value_weight,
        conv_gate_weight,
        att_out_weight,
        conv_out_weight,
        jnp.asarray(near_cos),
        jnp.asarray(near_sin),
        jnp.asarray(base_cos),
        jnp.asarray(base_sin),
        input_gain[None, :],
        kv_gain[None, :],
        conv_taps,
        conv_ln_gain[None, :],
        conv_ln_bias[None, :],
        att_out_gain[None, :],
        conv_out_gain[None, :],
    )


def solution(mesh):
    return jax.shard_map(
        shards,
        mesh=mesh,
        in_specs=(
            P("sp", "tp"),
            P(),
            P(None, "tp"),
            P(None, "tp"),
            P(),
            P(),
            P(),
            P(None, "tp"),
            P(None, "tp"),
            P(None, "tp"),
            P(None, "tp"),
            P(None, "tp"),
            P("tp"),
            P("tp"),
            P("tp"),
            P("tp"),
            P("tp", None),
            P("tp", None),
        ),
        out_specs=P("sp", "tp"),
        check_vma=False,
    )
```

```python
import math

import jax
import jax.numpy as jnp
import numpy as np
from jax import lax
from jax.experimental import pallas as pl
from jax.experimental.pallas import tpu as pltpu
from jax.sharding import PartitionSpec as P

D_MODEL = 2048
NOPE_DIM = 64
ROT_DIM = 32
CONV_CH = 1024
KERNEL = 31

norm_eps = 1e-06
far_below = -1e30
rope_base = 10000.0


MESH = pl.DeviceIdType.MESH
ROWS = 384
SHARE = 112
KSETS = 16
PIECE = 4 * ROWS
SCALE = 1.4426950408889634 / math.sqrt(NOPE_DIM + ROT_DIM)


def ring_peers(tp):
    x, c = tp // 2, tp % 2
    right = ((x + 1) % 4) * 2 + c
    left = ((x + 3) % 4) * 2 + c
    far = ((x + 2) % 4) * 2 + c
    partner = x * 2 + (1 - c)
    return right, left, far, partner


class RingGather:
    def __init__(self, buf, lo, size, send, recv, sp, tp):
        self.buf, self.lo, self.size = buf, lo, size
        self.send, self.recv, self.sp, self.tp = send, recv, sp, tp
        self.right, self.left, self.far, self.partner = ring_peers(tp)

    def piece(self, slot, part=None):
        size = self.size if part is None else self.size // 2
        start = self.lo + size if part == 1 else self.lo
        return self.buf.at[slot, pl.ds(start, size)]

    def copy(self, slot, part, sem, to):
        return pltpu.make_async_remote_copy(
            src_ref=self.piece(slot, part),
            dst_ref=self.piece(slot, part),
            send_sem=self.send.at[sem],
            recv_sem=self.recv.at[sem],
            device_id=(self.sp, to),
            device_id_type=MESH,
        )

    def begin(self):
        self.copy(self.tp, None, 0, self.right).start()
        self.copy(self.tp, None, 1, self.left).start()
        self.copy(self.tp, None, 2, self.partner).start()

    def relay(self):
        self.copy(self.left, None, 0, self.right).wait_recv()
        self.copy(self.left, 0, 5, self.right).start()
        self.copy(self.left, None, 3, self.partner).start()
        self.copy(self.right, None, 1, self.left).wait_recv()
        self.copy(self.right, 1, 6, self.left).start()
        self.copy(self.right, None, 4, self.partner).start()

    def relay_far(self):
        self.copy(self.far, 0, 5, self.right).wait_recv()
        self.copy(self.far, 0, 7, self.partner).start()
        self.copy(self.far, 1, 6, self.left).wait_recv()
        self.copy(self.far, 1, 8, self.partner).start()

    def finish(self):
        for sem, part in ((2, None), (3, None), (4, None), (7, 0), (8, 1)):
            self.copy(self.far, part, sem, self.partner).wait_recv()

    def drain(self):
        for sem, part in ((0, None), (1, None), (2, None), (3, None), (4, None), (5, 0), (6, 1), (7, 0), (8, 1)):
            self.copy(self.tp, part, sem, self.partner).wait_send()


def member_z(member, kind):
    return 2 * member + (kind + member) % 2


def layer_kernel(
    tokens_hbm, query_hbm, query_rot_hbm, kv_down_hbm, rot_down_hbm, key_up_hbm, value_up_hbm,
    conv_value_hbm, conv_gate_hbm, att_w_ref, conv_w_ref, near_cos_hbm, near_sin_hbm,
    base_cos_ref, base_sin_ref, input_gain_ref, kv_gain_ref,
    taps_ref, ln_gain_ref, ln_bias_ref, att_gain_ref, conv_gain_ref, out_ref,
    tbuf, scaled, wall, wqr, wrd, wkvd, kup, vup, near_cos, near_sin, p_send, p_recv,
    q_ref, share_ref, gated_ref,
    qraw, qbuf, kbuf, kk, vv, wkv, top, acc, o_send, l_send, o_recv, l_recv, own_out, own_lse,
    halo, padded, conv_out, mom_send, mom_recv, cbuf, abuf, weights, gains, gain_all, branch,
    q_ssem, q_rsem, k_ssem, k_rsem, f_ssem, f_rsem, ag_ssem, ag_rsem, o_ssem, o_rsem, l_ssem, l_rsem,
    h_ssem, h_rsem, m_ssem, m_rsem, c_ssem, c_rsem, a_ssem, a_rsem, w_ssem, w_rsem, g_ssem, g_rsem,
    own_sem, t_ssem, t_rsem, load_sem, p_ssem, p_rsem,
):
    sp, tp = lax.axis_index("sp"), lax.axis_index("tp")
    z, y = sp // 8, sp % 8
    kind, mine, parity = (z + z // 2) % 2, z // 2, y % 2
    residue = (y // 2 + mine) % 4
    bf, f32 = jnp.bfloat16, jnp.float32

    def member_sp(member):
        return member_z(member, kind) * 8 + y

    place = 2 * parity + z % 2
    z_other, y_other = z + 1 - 2 * (z % 2), y + 1 - 2 * parity
    quad = (z_other * 8 + y, z * 8 + y_other, z_other * 8 + y_other)
    orders = (0, 1, 3, 2)
    pieces = [(mine + d) % 4 for d in orders]
    far_quads = [None]
    for j in range(1, 4):
        m = (mine + 4 - orders[j]) % 4
        far_quads.append((2 * m + z % 2) * 8 + 2 * ((residue + 4 - m) % 4) + parity)
    after, before_sp = (sp + 1) % 64, (sp + 63) % 64

    own_rows = pl.ds(pl.multiple_of(256 * tp, 256), 256)
    wrd[32:128, :] = jnp.zeros((96, 256), bf)
    loads = [
        pltpu.make_async_copy(src, dst, load_sem.at[n])
        for n, (src, dst) in enumerate(
            (
                (tokens_hbm, tbuf.at[tp]),
                (kv_down_hbm.at[own_rows], wkvd),
                (rot_down_hbm.at[:, own_rows], wrd.at[pl.ds(0, 32)]),
                (key_up_hbm, kup),
                (value_up_hbm, vup),
                (query_hbm, wall.at[:, pl.ds(0, 128)]),
                (conv_value_hbm, wall.at[:, pl.ds(128, 128)]),
                (conv_gate_hbm, wall.at[:, pl.ds(256, 128)]),
                (query_rot_hbm, wqr),
                (near_cos_hbm, near_cos),
                (near_sin_hbm, near_sin),
            )
        )
    ]
    for load in loads:
        load.start()

    barrier = pltpu.get_barrier_semaphore()
    for i in range(1, 4):
        pl.semaphore_signal(
            barrier, inc=1, device_id=(member_sp((mine + i) % 4), tp), device_id_type=MESH
        )
        pl.semaphore_signal(barrier, inc=1, device_id=(far_quads[i], tp), device_id_type=MESH)
        pl.semaphore_signal(barrier, inc=1, device_id=(quad[i - 1], tp), device_id_type=MESH)
    for i in range(1, 8):
        pl.semaphore_signal(barrier, inc=1, device_id=(sp, (tp + i) % 8), device_id_type=MESH)
    pl.semaphore_signal(barrier, inc=1, device_id=(before_sp, tp), device_id_type=MESH)
    pl.semaphore_wait(barrier, 17)

    def remote(src, dst, ssem, rsem, to):
        return pltpu.make_async_remote_copy(
            src_ref=src, dst_ref=dst, send_sem=ssem, recv_sem=rsem, device_id=to, device_id_type=MESH
        )

    def scale_block(t):
        columns = pl.ds(pl.multiple_of(256 * t, 256), 256)
        x = tbuf[t].astype(f32)
        scaled[:, columns] = (x * input_gain_ref[:, columns]).astype(bf)
        return x * x

    tag = lax.broadcasted_iota(jnp.int32, (ROWS, 128), 1)
    low = tag < 64
    tokens_gather = RingGather(tbuf, 0, ROWS, t_ssem, t_rsem, sp, tp)
    for load in loads[0:3]:
        load.wait()
    squares = scale_block(tp)
    mine_scaled = scaled[:, own_rows]
    p_send[:, 0:256] = jnp.dot(mine_scaled, wkvd[...], preferred_element_type=f32).astype(bf)
    rot_part = lax.dot_general(
        mine_scaled, wrd[...], (((1,), (1,)), ((), ())), preferred_element_type=f32
    )
    p_send[:, 256:384] = jnp.where(
        tag == 32, jnp.sum(squares, axis=1, keepdims=True), rot_part
    ).astype(bf)

    def part_copy(j):
        peer = (tp + j) % 8
        return remote(
            p_send.at[pl.ds(pl.multiple_of(48 * peer, 16), 48)],
            p_recv.at[tp],
            p_ssem.at[j],
            p_rsem.at[tp],
            (sp, peer),
        )

    for j in range(1, 8):
        part_copy(j).start()
    tokens_gather.begin()

    gains[...] = jnp.zeros(gains.shape, f32)
    gains[0:1, :] = att_gain_ref[...]
    gains[1:2, :] = conv_gain_ref[...]
    for load in loads[3:]:
        load.wait()
    lane = lax.broadcasted_iota(jnp.int32, (256, 128), 1)
    for n, ref in enumerate((kup, vup)):
        w = ref[...].astype(f32)
        wkv[:, pl.ds(256 * n, 128)] = jnp.where(lane < 64, w, 0.0).astype(bf)
        wkv[:, pl.ds(256 * n + 128, 128)] = jnp.where(lane < 64, pltpu.roll(w, 64, 1), 0.0).astype(bf)
    cos_base, sin_base = base_cos_ref[pl.ds(sp, 1), :], base_sin_ref[pl.ds(sp, 1), :]

    def turn(rows, near_c, near_s):
        cosine = near_c * cos_base - near_s * sin_base
        sine = near_s * cos_base + near_c * sin_base
        front = lax.broadcasted_iota(jnp.int32, rows.shape, 1) % 32 < 16
        other = jnp.where(front, pltpu.roll(rows, 112, 1), pltpu.roll(rows, 16, 1))
        return rows * cosine + other * jnp.where(front, -sine, sine)

    share_rows = pl.ds(pl.multiple_of(48 * tp, 16), 48)
    raw = p_send[share_rows, :].astype(f32)
    for j in range(1, 8):
        source = (tp + j) % 8
        remote(
            p_send.at[share_rows], p_recv.at[source], p_ssem.at[j], p_rsem.at[source], (sp, source)
        ).wait_recv()
        raw = raw + p_recv[source].astype(f32)
    power = jnp.sum(raw[:, 0:256] * raw[:, 0:256], axis=1, keepdims=True) / 256
    latent = (raw[:, 0:256] * lax.rsqrt(power + norm_eps) * kv_gain_ref[...]).astype(bf)
    share_ref[0:48, :] = latent[:, 0:128]
    share_ref[48:96, :] = latent[:, 128:256]
    key_rows = raw[:, 256:384]
    key_rows = key_rows * lax.rsqrt(key_rows[:, 32:33] / D_MODEL + norm_eps)
    key_rows = turn(key_rows, near_cos[share_rows, :], near_sin[share_rows, :])
    group = lax.broadcasted_iota(jnp.int32, (16, 128), 1) // 32
    fold = jnp.zeros((16, 128), f32)
    for j in range(3):
        fold = jnp.where(group == j, pltpu.roll(key_rows[16 * j : 16 * j + 16], 32 * j, 1), fold)
    share_ref[96:112, :] = fold.astype(bf)

    def block(j):
        return kbuf.at[tp, 4 * pieces[j] + place]

    own_block = pltpu.make_async_copy(share_ref, block(0), own_sem.at[2])
    own_block.start()

    def key_copy(j):
        return remote(share_ref, block(0), k_ssem.at[j], k_rsem.at[j], (far_quads[j], tp))

    def quad_copy(j, n):
        source = share_ref if j == 0 else block(j)
        return remote(source, block(j), f_ssem.at[j, n], f_rsem.at[j, n], (quad[n], tp))

    def spread(j):
        if j > 0:
            remote(share_ref, block(j), k_ssem.at[j], k_rsem.at[j], (far_quads[j], tp)).wait_recv()
        for n in range(3):
            quad_copy(j, n).start()

    gathers = [
        RingGather(kbuf, 4 * p, 4, ag_ssem.at[j], ag_rsem.at[j], sp, tp)
        for j, p in enumerate(pieces)
    ]
    conv_gather = RingGather(cbuf, 0, ROWS, c_ssem, c_rsem, sp, tp)
    att_gather = RingGather(abuf, 0, ROWS, a_ssem, a_rsem, sp, tp)

    def begin(j):
        for n in range(3):
            quad_copy(j, n).wait_recv()
        gathers[j].begin()

    spread(0)
    for j in range(1, 4):
        key_copy(j).start()
    own_block.wait()

    tokens_gather.relay()
    squares = squares + scale_block(tokens_gather.left)
    squares = squares + scale_block(tokens_gather.right)
    begin(0)
    tokens_gather.relay_far()
    spread(1)
    spread(2)
    tokens_gather.finish()
    squares = squares + scale_block(tokens_gather.far)
    for t in (tp, tokens_gather.left, tokens_gather.right, tokens_gather.far):
        squares = squares + scale_block(t + 1 - 2 * (t % 2))
    row_scale = lax.rsqrt(jnp.sum(squares, axis=1, keepdims=True) / D_MODEL + norm_eps)
    flat = lax.dot_general(
        scaled[...], wqr[...], (((1,), (1,)), ((), ())), preferred_element_type=f32
    )
    flat = jnp.concatenate([flat * row_scale, jnp.zeros((ROWS, 64), f32)], axis=1)
    turned_rows = turn(flat, near_cos[...], near_sin[...])
    sums = jnp.dot(scaled[...], wall[...], preferred_element_type=f32)
    q_ref[0:ROWS, :] = (sums[:, 0:128] * (row_scale * SCALE)).astype(bf)
    half = ROWS // 2
    q_ref[ROWS : ROWS + half, :] = (
        jnp.where(low[0:half], turned_rows[0:half], pltpu.roll(turned_rows[half:ROWS], 64, 1)) * SCALE
    ).astype(bf)
    gated = (sums[:, 128:256] * row_scale * jax.nn.sigmoid(sums[:, 256:384] * row_scale)).astype(bf)
    gated_ref[...] = gated

    halo_copy = remote(gated_ref.at[pl.ds(ROWS - 32, 32)], halo, h_ssem, h_rsem, (after, tp))
    halo_copy.start()

    def query_copy(i):
        return remote(
            q_ref, qraw.at[i - 1], q_ssem.at[i - 1], q_rsem.at[i - 1], (member_sp((mine + i) % 4), tp)
        )

    for i in range(1, 4):
        query_copy(i).start()

    def unpack(ref, member):
        nope = ref[0:ROWS, :].astype(f32)
        fold = ref[ROWS : ROWS + ROWS // 2, :].astype(f32)
        for h in range(2):
            body = nope if h == 0 else pltpu.roll(nope, 64, 1)
            upper = pltpu.roll(fold, 64 - 32 * h, 1)
            lower = fold if h == 0 else pltpu.roll(fold, 96, 1)
            rotary = jnp.concatenate([upper, lower], axis=0)
            qbuf[member, h] = jnp.where(low, body, jnp.where(tag < 96, rotary, 0.0)).astype(bf)

    begin(1)
    gathers[0].relay()
    spread(3)
    unpack(q_ref, mine)
    begin(2)
    gathers[1].relay()
    gathers[0].relay_far()

    halo_copy.wait_recv()
    edge = halo[...].astype(f32)
    padded[0:32, :] = jnp.where(sp > 0, edge, jnp.zeros_like(edge))
    padded[pl.ds(32, ROWS), :] = gated_ref[...].astype(f32)
    total = jnp.zeros((ROWS, 128), f32)
    for tap in range(KERNEL):
        total = total + taps_ref[tap : tap + 1, :] * padded[pl.ds(tap + 2, ROWS), :]
    conv_out[...] = total
    sum_one = jnp.sum(total, axis=1, keepdims=True)
    sum_two = jnp.sum(total * total, axis=1, keepdims=True)
    mom_send[...] = jnp.transpose(jnp.where(tag == 0, sum_one, sum_two))[0:8, :]

    begin(3)
    gathers[2].relay()
    gathers[1].relay_far()

    def moment_copy(j):
        return remote(
            mom_send, mom_recv.at[tp], m_ssem.at[j], m_rsem.at[tp], (sp, (tp + j) % 8)
        )

    for j in range(1, 8):
        moment_copy(j).start()

    def assemble(p):
        slots = [4 * p + u for u in range(4)]
        at = pl.ds(pl.multiple_of(p * PIECE, PIECE), PIECE)
        first = jnp.concatenate([kbuf[:, s, 0:48, :].reshape(ROWS, 128) for s in slots], axis=0)
        second = jnp.concatenate([kbuf[:, s, 48:96, :].reshape(ROWS, 128) for s in slots], axis=0)
        product = jnp.dot(
            jnp.concatenate([first, second], axis=1), wkv[...], preferred_element_type=f32
        )
        pieces = []
        for s in slots:
            folded = kbuf[:, s, 96:112, :].astype(f32).reshape(128, 128)
            turned = [
                pltpu.roll(folded, (64 - 32 * j) % 128, 1).reshape(8, 1, 16, 128) for j in range(3)
            ]
            pieces.append(jnp.concatenate(turned, axis=1).reshape(ROWS, 128))
        rotary = jnp.concatenate(pieces, axis=0)
        front = lax.broadcasted_iota(jnp.int32, (PIECE, 128), 1) < 64
        for h in range(2):
            kk[h, at, :] = jnp.where(
                front, product[:, 128 * h : 128 * h + 128], rotary
            ).astype(bf)
            vv[h, at, :] = jnp.where(
                front, product[:, 256 + 128 * h : 384 + 128 * h], 1.0
            ).astype(bf)

    def step(member, p, masked):
        if masked:
            offset = lax.broadcasted_iota(jnp.int32, (ROWS, ROWS), 1) - lax.broadcasted_iota(
                jnp.int32, (ROWS, ROWS), 0
            )
            block = member_sp(member)
        for h in range(2):
            scores = lax.dot_general(
                qbuf[member, h],
                kk[h, pl.ds(p * PIECE, PIECE), :],
                (((1,), (1,)), ((), ())),
                preferred_element_type=f32,
            )
            if masked:
                columns = []
                for u in range(4):
                    key_block = (2 * p + u % 2) * 8 + 2 * ((residue + 4 - p) % 4) + u // 2
                    columns.append(
                        jnp.where(
                            offset <= (block - key_block) * ROWS,
                            scores[:, ROWS * u : ROWS * u + ROWS],
                            far_below,
                        )
                    )
                scores = jnp.concatenate(columns, axis=1)
            now = jnp.broadcast_to(jnp.max(scores, axis=1, keepdims=True), (ROWS, 128))
            if p > 0:
                before = top[member, h]
                now = jnp.maximum(before, now)
            top[member, h] = now
            likely = jnp.exp2(scores - jnp.concatenate([now] * (PIECE // 128), axis=1)).astype(bf)
            fresh = jnp.dot(likely, vv[h, pl.ds(p * PIECE, PIECE), :], preferred_element_type=f32)
            if p > 0:
                fresh = acc[member, h] * jnp.exp2(before - now) + fresh
            acc[member, h] = fresh

    def back_copies(member, source):
        to = (member_sp(member), tp)
        return (
            remote(o_send.at[member], o_recv.at[source], o_ssem.at[member], o_rsem.at[source], to),
            remote(l_send.at[member], l_recv.at[source], l_ssem.at[member], l_rsem.at[source], to),
        )

    def finalize(member):
        sums, tops = [], []
        for h in range(2):
            a = acc[member, h]
            part = jnp.where(low, pltpu.roll(a, 64, 1), a)
            sums.append(part)
            tops.append(top[member, h] + jnp.log2(part))
        value = jnp.where(low, acc[member, 0], pltpu.roll(acc[member, 1], 64, 1))
        value = value / jnp.where(low, sums[0], sums[1])
        o_send[member] = value.astype(bf)
        l_send[member] = jnp.transpose(jnp.where(tag < 4, tops[0], tops[1]))[0:8, :]

        @pl.when(mine == member)
        def _():
            own_out[...] = value
            own_lse[...] = jnp.where(low, tops[0], tops[1])

        @pl.when(mine != member)
        def _():
            for copy in back_copies(member, mine):
                copy.start()

    def weight_copies(j):
        to = (sp, (tp + j) % 8)
        columns = pl.ds(pl.multiple_of(256 * ((tp + j) % 8), 256), 256)
        return (
            remote(att_w_ref.at[:, columns], weights.at[0, tp], w_ssem.at[0, j], w_rsem.at[0, tp], to),
            remote(conv_w_ref.at[:, columns], weights.at[1, tp], w_ssem.at[1, j], w_rsem.at[1, tp], to),
            remote(gains, gain_all.at[tp], g_ssem.at[j], g_rsem.at[tp], to),
        )

    own_columns = pl.ds(pl.multiple_of(256 * tp, 256), 256)
    own_weights = (
        pltpu.make_async_copy(att_w_ref.at[:, own_columns], weights.at[0, tp], own_sem.at[0]),
        pltpu.make_async_copy(conv_w_ref.at[:, own_columns], weights.at[1, tp], own_sem.at[1]),
    )

    gathers[3].relay()
    gathers[2].relay_far()
    gathers[0].finish()
    assemble(pieces[0])
    gathers[3].relay_far()

    mom_recv[tp] = mom_send[...]
    for j in range(1, 8):
        source = (tp + j) % 8
        remote(mom_send, mom_recv.at[source], m_ssem.at[j], m_rsem.at[source], (sp, source)).wait_recv()
    moments = mom_recv[0]
    for t in range(1, 8):
        moments = moments + mom_recv[t]
    columns = jnp.transpose(moments)
    mean_val = columns[:, 0:1] / CONV_CH
    spread = columns[:, 1:2] / CONV_CH - mean_val * mean_val
    normed = (conv_out[...] - mean_val) * lax.rsqrt(spread + norm_eps)
    swished = jax.nn.silu(normed * ln_gain_ref[...] + ln_bias_ref[...])
    cbuf[tp] = swished.astype(bf)

    conv_gather.begin()
    for copy in own_weights:
        copy.start()
    for j in range(1, 8):
        for copy in weight_copies(j):
            copy.start()

    def arrive(i):
        query_copy(i).wait_recv()
        member = (mine + 4 - i) % 4
        unpack(qraw.at[i - 1], member)
        return member

    for j in range(1, 4):
        gathers[j].finish()
        assemble(pieces[j])
    step(mine, 0, True)
    conv_gather.relay()
    step(arrive(1), 0, True)
    conv_gather.relay_far()
    step(arrive(3), 0, True)
    step(arrive(2), 0, True)
    finalize(0)
    step(1, 1, True)
    finalize(1)
    step(2, 1, False)
    step(2, 2, True)
    finalize(2)
    step(3, 1, False)
    step(3, 2, False)
    step(3, 3, True)
    finalize(3)

    gain_all[tp] = gains[...]
    conv_gather.finish()
    for copy in own_weights:
        copy.wait()
    for j in range(1, 8):
        source = (tp + j) % 8
        for n in range(2):
            remote(
                weights.at[n, source], weights.at[n, source], w_ssem.at[n, j], w_rsem.at[n, source], (sp, source)
            ).wait_recv()
        remote(gains, gain_all.at[source], g_ssem.at[j], g_rsem.at[source], (sp, source)).wait_recv()

    def product(buf, n):
        wide = jnp.concatenate([buf[t] for t in range(8)], axis=1).astype(f32)
        gain = jnp.concatenate([gain_all[t, n : n + 1, :] for t in range(8)], axis=1)
        power = jnp.sum(wide * wide, axis=1, keepdims=True)
        mixed = (wide * lax.rsqrt(power / CONV_CH + norm_eps) * gain).astype(bf)
        return jnp.dot(mixed, weights[n].reshape(1024, 256), preferred_element_type=f32)

    branch[...] = product(cbuf, 1)

    logs, values = [own_lse[...]], [own_out[...]]
    for i in range(1, 4):
        source = (mine + i) % 4
        for copy in back_copies(source, source):
            copy.wait_recv()
        columns = jnp.transpose(l_recv[source])
        logs.append(jnp.where(low, columns[:, 0:1], columns[:, 4:5]))
        values.append(o_recv[source].astype(f32))
    peak = jnp.maximum(jnp.maximum(logs[0], logs[1]), jnp.maximum(logs[2], logs[3]))
    shares = [jnp.exp2(log - peak) for log in logs]
    merged = sum(s * v for s, v in zip(shares, values)) / sum(shares)
    abuf[tp] = merged.astype(bf)

    att_gather.begin()
    att_gather.relay()
    att_gather.relay_far()
    att_gather.finish()
    out_ref[...] = (branch[...] + product(abuf, 0)).astype(bf)

    tokens_gather.drain()
    halo_copy.wait_send()
    for i in range(1, 8):
        part_copy(i).wait_send()
        moment_copy(i).wait_send()
        for copy in weight_copies(i):
            copy.wait_send()
    for j in range(4):
        if j > 0:
            key_copy(j).wait_send()
        for n in range(3):
            quad_copy(j, n).wait_send()
        gathers[j].drain()
    for i in range(1, 4):
        query_copy(i).wait_send()
        member = (mine + i) % 4
        for copy in back_copies(member, mine):
            copy.wait_send()
    conv_gather.drain()
    att_gather.drain()


def layer(*args):
    vmem, anywhere = pl.BlockSpec(memory_space=pltpu.VMEM), pl.BlockSpec(memory_space=pl.ANY)
    bf, f32 = jnp.bfloat16, jnp.float32
    dma = pltpu.SemaphoreType.DMA
    return pl.pallas_call(
        layer_kernel,
        out_shape=jax.ShapeDtypeStruct((ROWS, 256), bf),
        in_specs=[anywhere] * 13 + [vmem] * 9,
        out_specs=vmem,
        scratch_shapes=[
            pltpu.VMEM((8, ROWS, 256), bf),
            pltpu.VMEM((ROWS, D_MODEL), bf),
            pltpu.VMEM((D_MODEL, 384), bf),
            pltpu.VMEM((64, D_MODEL), bf),
            pltpu.VMEM((128, 256), bf),
            pltpu.VMEM((256, 256), bf),
            pltpu.VMEM((256, 128), bf),
            pltpu.VMEM((256, 128), bf),
            pltpu.VMEM((ROWS, 128), f32),
            pltpu.VMEM((ROWS, 128), f32),
            pltpu.VMEM((ROWS, 384), bf),
            pltpu.VMEM((8, 48, 384), bf),
            pltpu.VMEM((ROWS + ROWS // 2, 128), bf),
            pltpu.VMEM((SHARE, 128), bf),
            pltpu.VMEM((ROWS, 128), bf),
            pltpu.VMEM((3, ROWS + ROWS // 2, 128), bf),
            pltpu.VMEM((4, 2, ROWS, 128), bf),
            pltpu.VMEM((8, KSETS, SHARE, 128), bf),
            pltpu.VMEM((2, KSETS * ROWS, 128), bf),
            pltpu.VMEM((2, KSETS * ROWS, 128), bf),
            pltpu.VMEM((256, 512), bf),
            pltpu.VMEM((4, 2, ROWS, 128), f32),
            pltpu.VMEM((4, 2, ROWS, 128), f32),
            pltpu.VMEM((4, ROWS, 128), bf),
            pltpu.VMEM((4, 8, ROWS), f32),
            pltpu.VMEM((4, ROWS, 128), bf),
            pltpu.VMEM((4, 8, ROWS), f32),
            pltpu.VMEM((ROWS, 128), f32),
            pltpu.VMEM((ROWS, 128), f32),
            pltpu.VMEM((32, 128), bf),
            pltpu.VMEM((32 + ROWS, 128), f32),
            pltpu.VMEM((ROWS, 128), f32),
            pltpu.VMEM((8, ROWS), f32),
            pltpu.VMEM((8, 8, ROWS), f32),
            pltpu.VMEM((8, ROWS, 128), bf),
            pltpu.VMEM((8, ROWS, 128), bf),
            pltpu.VMEM((2, 8, 128, 256), bf),
            pltpu.VMEM((8, 128), f32),
            pltpu.VMEM((8, 8, 128), f32),
            pltpu.VMEM((ROWS, 256), f32),
            dma((3,)), dma((3,)), dma((4,)), dma((4,)), dma((4, 3)), dma((4, 3)), dma((4, 9)), dma((4, 9)),
            dma((4,)), dma((4,)), dma((4,)), dma((4,)), dma, dma, dma((8,)), dma((8,)),
            dma((9,)), dma((9,)), dma((9,)), dma((9,)), dma((2, 8)), dma((2, 8)), dma((8,)), dma((8,)),
            dma((3,)), dma((9,)), dma((9,)), dma((11,)), dma((8,)), dma((8,)),
        ],
        compiler_params=pltpu.CompilerParams(collective_id=1, has_side_effects=True),
        name="layer",
    )(*args)


def rotary_tables():
    lanes = np.arange(128)
    frequency = rope_base ** (-(lanes % 16) / 16.0)
    near = np.arange(ROWS)[:, None] * frequency[None, :]
    base = (np.arange(64) * ROWS)[:, None] * frequency[None, :]
    return tuple(np.asarray(f(a), np.float32) for a in (near, base) for f in (np.cos, np.sin))


def shards(
    tokens,
    input_gain,
    query_weight,
    query_rot_weight,
    kv_down,
    rot_down,
    kv_gain,
    key_up,
    value_up,
    conv_value_weight,
    conv_gate_weight,
    conv_taps,
    conv_ln_gain,
    conv_ln_bias,
    att_out_gain,
    conv_out_gain,
    att_out_weight,
    conv_out_weight,
):
    near_cos, near_sin, base_cos, base_sin = rotary_tables()
    return layer(
        tokens,
        query_weight,
        query_rot_weight.T,
        kv_down,
        rot_down.T,
        key_up,
        value_up,
        conv_value_weight,
        conv_gate_weight,
        att_out_weight,
        conv_out_weight,
        jnp.asarray(near_cos),
        jnp.asarray(near_sin),
        jnp.asarray(base_cos),
        jnp.asarray(base_sin),
        input_gain[None, :],
        kv_gain[None, :],
        conv_taps,
        conv_ln_gain[None, :],
        conv_ln_bias[None, :],
        att_out_gain[None, :],
        conv_out_gain[None, :],
    )


def solution(mesh):
    return jax.shard_map(
        shards,
        mesh=mesh,
        in_specs=(
            P("sp", "tp"),
            P(),
            P(None, "tp"),
            P(None, "tp"),
            P(),
            P(),
            P(),
            P(None, "tp"),
            P(None, "tp"),
            P(None, "tp"),
            P(None, "tp"),
            P(None, "tp"),
            P("tp"),
            P("tp"),
            P("tp"),
            P("tp"),
            P("tp", None),
            P("tp", None),
        ),
        out_specs=P("sp", "tp"),
        check_vma=False,
    )
```

```python
import math

import jax
import jax.numpy as jnp
import numpy as np
from jax import lax
from jax.experimental import pallas as pl
from jax.experimental.pallas import tpu as pltpu
from jax.sharding import PartitionSpec as P

D_MODEL = 2048
NOPE_DIM = 64
ROT_DIM = 32
CONV_CH = 1024
KERNEL = 31

norm_eps = 1e-06
far_below = -1e30
rope_base = 10000.0


MESH = pl.DeviceIdType.MESH
ROWS = 384
SHARE = 112
KSETS = 16
PIECE = 4 * ROWS
SCALE = 1.4426950408889634 / math.sqrt(NOPE_DIM + ROT_DIM)


def ring_peers(tp):
    x, c = tp // 2, tp % 2
    right = ((x + 1) % 4) * 2 + c
    left = ((x + 3) % 4) * 2 + c
    far = ((x + 2) % 4) * 2 + c
    partner = x * 2 + (1 - c)
    return right, left, far, partner


class RingGather:
    def __init__(self, buf, lo, size, send, recv, sp, tp):
        self.buf, self.lo, self.size = buf, lo, size
        self.send, self.recv, self.sp, self.tp = send, recv, sp, tp
        self.right, self.left, self.far, self.partner = ring_peers(tp)

    def piece(self, slot, part=None):
        size = self.size if part is None else self.size // 2
        start = self.lo + size if part == 1 else self.lo
        return self.buf.at[slot, pl.ds(start, size)]

    def copy(self, slot, part, sem, to):
        return pltpu.make_async_remote_copy(
            src_ref=self.piece(slot, part),
            dst_ref=self.piece(slot, part),
            send_sem=self.send.at[sem],
            recv_sem=self.recv.at[sem],
            device_id=(self.sp, to),
            device_id_type=MESH,
        )

    def begin(self):
        self.copy(self.tp, None, 0, self.right).start()
        self.copy(self.tp, None, 1, self.left).start()
        self.copy(self.tp, None, 2, self.partner).start()

    def relay(self):
        self.copy(self.left, None, 0, self.right).wait_recv()
        self.copy(self.left, 0, 5, self.right).start()
        self.copy(self.left, None, 3, self.partner).start()
        self.copy(self.right, None, 1, self.left).wait_recv()
        self.copy(self.right, 1, 6, self.left).start()
        self.copy(self.right, None, 4, self.partner).start()

    def relay_far(self):
        self.copy(self.far, 0, 5, self.right).wait_recv()
        self.copy(self.far, 0, 7, self.partner).start()
        self.copy(self.far, 1, 6, self.left).wait_recv()
        self.copy(self.far, 1, 8, self.partner).start()

    def finish(self):
        for sem, part in ((2, None), (3, None), (4, None), (7, 0), (8, 1)):
            self.copy(self.far, part, sem, self.partner).wait_recv()

    def drain(self):
        for sem, part in ((0, None), (1, None), (2, None), (3, None), (4, None), (5, 0), (6, 1), (7, 0), (8, 1)):
            self.copy(self.tp, part, sem, self.partner).wait_send()


def member_z(member, kind):
    return 2 * member + (kind + member) % 2


def layer_kernel(
    tokens_hbm, query_hbm, query_rot_hbm, kv_down_hbm, rot_down_hbm, key_up_hbm, value_up_hbm,
    conv_value_hbm, conv_gate_hbm, att_w_ref, conv_w_ref, near_cos_hbm, near_sin_hbm,
    base_cos_ref, base_sin_ref, input_gain_ref, kv_gain_ref,
    taps_ref, ln_gain_ref, ln_bias_ref, att_gain_ref, conv_gain_ref, out_ref,
    tbuf, scaled, wall, wqr, wrd, wkvd, kup, vup, near_cos, near_sin, p_send, p_recv,
    q_ref, share_ref, gated_ref,
    qraw, qbuf, kbuf, kk, vv, wkv, top, acc, o_send, l_send, o_recv, l_recv, own_out, own_lse,
    halo, padded, conv_out, mom_send, mom_recv, cbuf, abuf, weights, gains, gain_all, branch,
    q_ssem, q_rsem, k_ssem, k_rsem, f_ssem, f_rsem, ag_ssem, ag_rsem, o_ssem, o_rsem, l_ssem, l_rsem,
    h_ssem, h_rsem, m_ssem, m_rsem, c_ssem, c_rsem, a_ssem, a_rsem, w_ssem, w_rsem, g_ssem, g_rsem,
    own_sem, t_ssem, t_rsem, load_sem, p_ssem, p_rsem, v_ssem, v_rsem,
):
    sp, tp = lax.axis_index("sp"), lax.axis_index("tp")
    z, y = sp // 8, sp % 8
    kind, mine, parity = (z + z // 2) % 2, z // 2, y % 2
    residue = (y // 2 + mine + 2) % 4
    bf, f32 = jnp.bfloat16, jnp.float32

    def member_sp(member):
        return member_z(member, kind) * 8 + y

    place = 2 * parity + z % 2
    z_other, y_other = z + 1 - 2 * (z % 2), y + 1 - 2 * parity
    quad = (z_other * 8 + y, z * 8 + y_other, z_other * 8 + y_other)
    key_peers = []
    for d in range(4):
        m = (mine + d) % 4
        key_peers.append((2 * m + z % 2) * 8 + 2 * ((residue + 4 - m) % 4) + parity)
    after, before_sp = (sp + 1) % 64, (sp + 63) % 64

    own_rows = pl.ds(pl.multiple_of(256 * tp, 256), 256)
    wrd[32:128, :] = jnp.zeros((96, 256), bf)
    loads = [
        pltpu.make_async_copy(src, dst, load_sem.at[n])
        for n, (src, dst) in enumerate(
            (
                (tokens_hbm, tbuf.at[tp]),
                (kv_down_hbm.at[own_rows], wkvd),
                (rot_down_hbm.at[:, own_rows], wrd.at[pl.ds(0, 32)]),
                (key_up_hbm, kup),
                (value_up_hbm, vup),
                (query_hbm, wall.at[:, pl.ds(0, 128)]),
                (conv_value_hbm, wall.at[:, pl.ds(128, 128)]),
                (conv_gate_hbm, wall.at[:, pl.ds(256, 128)]),
                (query_rot_hbm, wqr),
                (near_cos_hbm, near_cos),
                (near_sin_hbm, near_sin),
            )
        )
    ]
    for load in loads:
        load.start()

    barrier = pltpu.get_barrier_semaphore()
    for i in range(1, 4):
        pl.semaphore_signal(
            barrier, inc=1, device_id=(member_sp((mine + i) % 4), tp), device_id_type=MESH
        )
        pl.semaphore_signal(barrier, inc=1, device_id=(quad[i - 1], tp), device_id_type=MESH)
    for peer in key_peers:
        pl.semaphore_signal(barrier, inc=1, device_id=(peer, tp), device_id_type=MESH)
    for i in range(1, 8):
        pl.semaphore_signal(barrier, inc=1, device_id=(sp, (tp + i) % 8), device_id_type=MESH)
        pl.semaphore_signal(barrier, inc=1, device_id=(z * 8 + (y + i) % 8, tp), device_id_type=MESH)
    pl.semaphore_signal(barrier, inc=1, device_id=(before_sp, tp), device_id_type=MESH)
    pl.semaphore_wait(barrier, 25)

    def remote(src, dst, ssem, rsem, to):
        return pltpu.make_async_remote_copy(
            src_ref=src, dst_ref=dst, send_sem=ssem, recv_sem=rsem, device_id=to, device_id_type=MESH
        )

    def scale_block(t):
        columns = pl.ds(pl.multiple_of(256 * t, 256), 256)
        x = tbuf[t].astype(f32)
        scaled[:, columns] = (x * input_gain_ref[:, columns]).astype(bf)
        return x * x

    tag = lax.broadcasted_iota(jnp.int32, (ROWS, 128), 1)
    low = tag < 64
    slab = pl.ds(pl.multiple_of(16 * y, 16), 16)

    def weight_copies(j):
        to = (sp, (tp + j) % 8)
        columns = pl.ds(pl.multiple_of(256 * ((tp + j) % 8), 256), 256)
        return (
            remote(
                att_w_ref.at[slab, columns], weights.at[0, tp, slab], w_ssem.at[0, j], w_rsem.at[0, tp], to
            ),
            remote(
                conv_w_ref.at[slab, columns], weights.at[1, tp, slab], w_ssem.at[1, j], w_rsem.at[1, tp], to
            ),
            remote(gains, gain_all.at[tp], g_ssem.at[j], g_rsem.at[tp], to),
        )

    own_weights = (
        pltpu.make_async_copy(att_w_ref.at[slab, own_rows], weights.at[0, tp, slab], own_sem.at[0]),
        pltpu.make_async_copy(conv_w_ref.at[slab, own_rows], weights.at[1, tp, slab], own_sem.at[1]),
    )

    def slab_copy(d):
        rows = weights.at[:, :, slab]
        return remote(rows, rows, v_ssem.at[d], v_rsem.at[y], (z * 8 + (y + d) % 8, tp))

    gains[...] = jnp.zeros(gains.shape, f32)
    gains[0:1, :] = att_gain_ref[...]
    gains[1:2, :] = conv_gain_ref[...]
    for copy in own_weights:
        copy.start()

    tokens_gather = RingGather(tbuf, 0, ROWS, t_ssem, t_rsem, sp, tp)
    for load in loads[0:3]:
        load.wait()
    squares = scale_block(tp)
    mine_scaled = scaled[:, own_rows]
    p_send[:, 0:256] = jnp.dot(mine_scaled, wkvd[...], preferred_element_type=f32).astype(bf)
    rot_part = lax.dot_general(
        mine_scaled, wrd[...], (((1,), (1,)), ((), ())), preferred_element_type=f32
    )
    p_send[:, 256:384] = jnp.where(
        tag == 32, jnp.sum(squares, axis=1, keepdims=True), rot_part
    ).astype(bf)

    def part_copy(j):
        peer = (tp + j) % 8
        return remote(
            p_send.at[pl.ds(pl.multiple_of(48 * peer, 16), 48)],
            p_recv.at[tp],
            p_ssem.at[j],
            p_rsem.at[tp],
            (sp, peer),
        )

    for j in range(1, 8):
        part_copy(j).start()
    tokens_gather.begin()

    for j in range(1, 8):
        for copy in weight_copies(j):
            copy.start()
    for load in loads[3:]:
        load.wait()
    lane = lax.broadcasted_iota(jnp.int32, (256, 128), 1)
    for n, ref in enumerate((kup, vup)):
        w = ref[...].astype(f32)
        wkv[:, pl.ds(256 * n, 128)] = jnp.where(lane < 64, w, 0.0).astype(bf)
        wkv[:, pl.ds(256 * n + 128, 128)] = jnp.where(lane < 64, pltpu.roll(w, 64, 1), 0.0).astype(bf)
    cos_base, sin_base = base_cos_ref[pl.ds(sp, 1), :], base_sin_ref[pl.ds(sp, 1), :]

    def turn(rows, near_c, near_s):
        cosine = near_c * cos_base - near_s * sin_base
        sine = near_s * cos_base + near_c * sin_base
        front = lax.broadcasted_iota(jnp.int32, rows.shape, 1) % 32 < 16
        other = jnp.where(front, pltpu.roll(rows, 112, 1), pltpu.roll(rows, 16, 1))
        return rows * cosine + other * jnp.where(front, -sine, sine)

    share_rows = pl.ds(pl.multiple_of(48 * tp, 16), 48)
    raw = p_send[share_rows, :].astype(f32)
    for j in range(1, 8):
        source = (tp + j) % 8
        remote(
            p_send.at[share_rows], p_recv.at[source], p_ssem.at[j], p_rsem.at[source], (sp, source)
        ).wait_recv()
        raw = raw + p_recv[source].astype(f32)
    power = jnp.sum(raw[:, 0:256] * raw[:, 0:256], axis=1, keepdims=True) / 256
    latent = (raw[:, 0:256] * lax.rsqrt(power + norm_eps) * kv_gain_ref[...]).astype(bf)
    share_ref[0:48, :] = latent[:, 0:128]
    share_ref[48:96, :] = latent[:, 128:256]
    key_rows = raw[:, 256:384]
    key_rows = key_rows * lax.rsqrt(key_rows[:, 32:33] / D_MODEL + norm_eps)
    key_rows = turn(key_rows, near_cos[share_rows, :], near_sin[share_rows, :])
    group = lax.broadcasted_iota(jnp.int32, (16, 128), 1) // 32
    fold = jnp.zeros((16, 128), f32)
    for j in range(3):
        fold = jnp.where(group == j, pltpu.roll(key_rows[16 * j : 16 * j + 16], 32 * j, 1), fold)
    share_ref[96:112, :] = fold.astype(bf)

    def block(p):
        return kbuf.at[tp, 4 * p + place]

    def key_copy(d):
        return remote(share_ref, block(mine), k_ssem.at[d], k_rsem.at[mine], (key_peers[d], tp))

    def quad_copy(p, n):
        return remote(block(p), block(p), f_ssem.at[p, n], f_rsem.at[p, n], (quad[n], tp))

    def spread(p):
        remote(share_ref, block(p), k_ssem.at[0], k_rsem.at[p], (key_peers[0], tp)).wait_recv()
        for n in range(3):
            quad_copy(p, n).start()

    def begin(p):
        for n in range(3):
            quad_copy(p, n).wait_recv()
        gathers[p].begin()

    for d in range(4):
        key_copy(d).start()

    gathers = [
        RingGather(kbuf, 4 * p, 4, ag_ssem.at[p], ag_rsem.at[p], sp, tp) for p in range(4)
    ]
    conv_gather = RingGather(cbuf, 0, ROWS, c_ssem, c_rsem, sp, tp)
    att_gather = RingGather(abuf, 0, ROWS, a_ssem, a_rsem, sp, tp)

    tokens_gather.relay()
    squares = squares + scale_block(tokens_gather.left)
    squares = squares + scale_block(tokens_gather.right)
    tokens_gather.relay_far()
    tokens_gather.finish()
    squares = squares + scale_block(tokens_gather.far)
    for t in (tp, tokens_gather.left, tokens_gather.right, tokens_gather.far):
        squares = squares + scale_block(t + 1 - 2 * (t % 2))
    row_scale = lax.rsqrt(jnp.sum(squares, axis=1, keepdims=True) / D_MODEL + norm_eps)
    for p in range(4):
        spread(p)
    flat = lax.dot_general(
        scaled[...], wqr[...], (((1,), (1,)), ((), ())), preferred_element_type=f32
    )
    flat = jnp.concatenate([flat * row_scale, jnp.zeros((ROWS, 64), f32)], axis=1)
    turned_rows = turn(flat, near_cos[...], near_sin[...])
    sums = jnp.dot(scaled[...], wall[...], preferred_element_type=f32)
    q_ref[0:ROWS, :] = (sums[:, 0:128] * (row_scale * SCALE)).astype(bf)
    half = ROWS // 2
    q_ref[ROWS : ROWS + half, :] = (
        jnp.where(low[0:half], turned_rows[0:half], pltpu.roll(turned_rows[half:ROWS], 64, 1)) * SCALE
    ).astype(bf)
    gated = (sums[:, 128:256] * row_scale * jax.nn.sigmoid(sums[:, 256:384] * row_scale)).astype(bf)
    gated_ref[...] = gated

    halo_copy = remote(gated_ref.at[pl.ds(ROWS - 32, 32)], halo, h_ssem, h_rsem, (after, tp))
    halo_copy.start()

    def query_copy(i):
        return remote(
            q_ref, qraw.at[i - 1], q_ssem.at[i - 1], q_rsem.at[i - 1], (member_sp((mine + i) % 4), tp)
        )

    for i in range(1, 4):
        query_copy(i).start()

    def unpack(ref, member):
        nope = ref[0:ROWS, :].astype(f32)
        fold = ref[ROWS : ROWS + ROWS // 2, :].astype(f32)
        for h in range(2):
            body = nope if h == 0 else pltpu.roll(nope, 64, 1)
            upper = pltpu.roll(fold, 64 - 32 * h, 1)
            lower = fold if h == 0 else pltpu.roll(fold, 96, 1)
            rotary = jnp.concatenate([upper, lower], axis=0)
            qbuf[member, h] = jnp.where(low, body, jnp.where(tag < 96, rotary, 0.0)).astype(bf)

    begin(0)
    begin(1)
    unpack(q_ref, mine)

    halo_copy.wait_recv()
    edge = halo[...].astype(f32)
    padded[0:32, :] = jnp.where(sp > 0, edge, jnp.zeros_like(edge))
    padded[pl.ds(32, ROWS), :] = gated_ref[...].astype(f32)
    total = jnp.zeros((ROWS, 128), f32)
    for tap in range(KERNEL):
        total = total + taps_ref[tap : tap + 1, :] * padded[pl.ds(tap + 2, ROWS), :]
    conv_out[...] = total
    sum_one = jnp.sum(total, axis=1, keepdims=True)
    sum_two = jnp.sum(total * total, axis=1, keepdims=True)
    mom_send[...] = jnp.transpose(jnp.where(tag == 0, sum_one, sum_two))[0:8, :]

    gathers[0].relay()
    begin(2)
    begin(3)

    def moment_copy(j):
        return remote(
            mom_send, mom_recv.at[tp], m_ssem.at[j], m_rsem.at[tp], (sp, (tp + j) % 8)
        )

    for j in range(1, 8):
        moment_copy(j).start()

    def assemble(p):
        slots = [4 * p + u for u in range(4)]
        at = pl.ds(pl.multiple_of(p * PIECE, PIECE), PIECE)
        first = jnp.concatenate([kbuf[:, s, 0:48, :].reshape(ROWS, 128) for s in slots], axis=0)
        second = jnp.concatenate([kbuf[:, s, 48:96, :].reshape(ROWS, 128) for s in slots], axis=0)
        product = jnp.dot(
            jnp.concatenate([first, second], axis=1), wkv[...], preferred_element_type=f32
        )
        pieces = []
        for s in slots:
            folded = kbuf[:, s, 96:112, :].astype(f32).reshape(128, 128)
            turned = [
                pltpu.roll(folded, (64 - 32 * j) % 128, 1).reshape(8, 1, 16, 128) for j in range(3)
            ]
            pieces.append(jnp.concatenate(turned, axis=1).reshape(ROWS, 128))
        rotary = jnp.concatenate(pieces, axis=0)
        front = lax.broadcasted_iota(jnp.int32, (PIECE, 128), 1) < 64
        for h in range(2):
            kk[h, at, :] = jnp.where(
                front, product[:, 128 * h : 128 * h + 128], rotary
            ).astype(bf)
            vv[h, at, :] = jnp.where(
                front, product[:, 256 + 128 * h : 384 + 128 * h], 1.0
            ).astype(bf)

    def step(member, p, masked):
        if masked:
            offset = lax.broadcasted_iota(jnp.int32, (ROWS, ROWS), 1) - lax.broadcasted_iota(
                jnp.int32, (ROWS, ROWS), 0
            )
            block = member_sp(member)
        for h in range(2):
            scores = lax.dot_general(
                qbuf[member, h],
                kk[h, pl.ds(p * PIECE, PIECE), :],
                (((1,), (1,)), ((), ())),
                preferred_element_type=f32,
            )
            if masked:
                columns = []
                for u in range(4):
                    key_block = (2 * p + u % 2) * 8 + 2 * ((residue + 4 - p) % 4) + u // 2
                    columns.append(
                        jnp.where(
                            offset <= (block - key_block) * ROWS,
                            scores[:, ROWS * u : ROWS * u + ROWS],
                            far_below,
                        )
                    )
                scores = jnp.concatenate(columns, axis=1)
            now = jnp.broadcast_to(jnp.max(scores, axis=1, keepdims=True), (ROWS, 128))
            if p > 0:
                before = top[member, h]
                now = jnp.maximum(before, now)
            top[member, h] = now
            likely = jnp.exp2(scores - jnp.concatenate([now] * (PIECE // 128), axis=1)).astype(bf)
            fresh = jnp.dot(likely, vv[h, pl.ds(p * PIECE, PIECE), :], preferred_element_type=f32)
            if p > 0:
                fresh = acc[member, h] * jnp.exp2(before - now) + fresh
            acc[member, h] = fresh

    def back_copies(member, source):
        to = (member_sp(member), tp)
        return (
            remote(o_send.at[member], o_recv.at[source], o_ssem.at[member], o_rsem.at[source], to),
            remote(l_send.at[member], l_recv.at[source], l_ssem.at[member], l_rsem.at[source], to),
        )

    def finalize(member):
        sums, tops = [], []
        for h in range(2):
            a = acc[member, h]
            part = jnp.where(low, pltpu.roll(a, 64, 1), a)
            sums.append(part)
            tops.append(top[member, h] + jnp.log2(part))
        value = jnp.where(low, acc[member, 0], pltpu.roll(acc[member, 1], 64, 1))
        value = value / jnp.where(low, sums[0], sums[1])
        o_send[member] = value.astype(bf)
        l_send[member] = jnp.transpose(jnp.where(tag < 4, tops[0], tops[1]))[0:8, :]

        @pl.when(mine == member)
        def _():
            own_out[...] = value
            own_lse[...] = jnp.where(low, tops[0], tops[1])

        @pl.when(mine != member)
        def _():
            for copy in back_copies(member, mine):
                copy.start()

    for copy in own_weights:
        copy.wait()
    for j in range(1, 8):
        source = (tp + j) % 8
        for n in range(2):
            rows = weights.at[n, source, slab]
            remote(rows, rows, w_ssem.at[n, j], w_rsem.at[n, source], (sp, source)).wait_recv()
        remote(gains, gain_all.at[source], g_ssem.at[j], g_rsem.at[source], (sp, source)).wait_recv()
    for d in range(1, 8):
        slab_copy(d).start()

    def arrive(i):
        query_copy(i).wait_recv()
        member = (mine + 4 - i) % 4
        unpack(qraw.at[i - 1], member)
        return member

    gathers[1].relay()
    gathers[0].relay_far()
    gathers[0].finish()
    assemble(0)
    gathers[2].relay()
    gathers[1].relay_far()
    step(mine, 0, True)
    gathers[3].relay()
    gathers[2].relay_far()

    mom_recv[tp] = mom_send[...]
    for j in range(1, 8):
        source = (tp + j) % 8
        remote(mom_send, mom_recv.at[source], m_ssem.at[j], m_rsem.at[source], (sp, source)).wait_recv()
    moments = mom_recv[0]
    for t in range(1, 8):
        moments = moments + mom_recv[t]
    columns = jnp.transpose(moments)
    mean_val = columns[:, 0:1] / CONV_CH
    spread = columns[:, 1:2] / CONV_CH - mean_val * mean_val
    normed = (conv_out[...] - mean_val) * lax.rsqrt(spread + norm_eps)
    swished = jax.nn.silu(normed * ln_gain_ref[...] + ln_bias_ref[...])
    cbuf[tp] = swished.astype(bf)

    conv_gather.begin()
    step(arrive(1), 0, True)
    gathers[3].relay_far()
    step(arrive(3), 0, True)
    conv_gather.relay()
    gathers[1].finish()
    assemble(1)
    step(arrive(2), 0, True)
    conv_gather.relay_far()
    finalize(0)
    step(1, 1, True)
    finalize(1)
    step(2, 1, False)
    step(3, 1, False)
    gathers[2].finish()
    assemble(2)
    step(2, 2, True)
    finalize(2)
    step(3, 2, False)
    gathers[3].finish()
    assemble(3)
    step(3, 3, True)
    finalize(3)

    gain_all[tp] = gains[...]
    conv_gather.finish()
    for d in range(1, 8):
        source = (y + d) % 8
        rows = weights.at[:, :, pl.ds(pl.multiple_of(16 * source, 16), 16)]
        remote(rows, rows, v_ssem.at[d], v_rsem.at[source], (z * 8 + source, tp)).wait_recv()

    def product(buf, n):
        wide = jnp.concatenate([buf[t] for t in range(8)], axis=1).astype(f32)
        gain = jnp.concatenate([gain_all[t, n : n + 1, :] for t in range(8)], axis=1)
        power = jnp.sum(wide * wide, axis=1, keepdims=True)
        mixed = (wide * lax.rsqrt(power / CONV_CH + norm_eps) * gain).astype(bf)
        return jnp.dot(mixed, weights[n].reshape(1024, 256), preferred_element_type=f32)

    branch[...] = product(cbuf, 1)

    logs, values = [own_lse[...]], [own_out[...]]
    for i in range(1, 4):
        source = (mine + i) % 4
        for copy in back_copies(source, source):
            copy.wait_recv()
        columns = jnp.transpose(l_recv[source])
        logs.append(jnp.where(low, columns[:, 0:1], columns[:, 4:5]))
        values.append(o_recv[source].astype(f32))
    peak = jnp.maximum(jnp.maximum(logs[0], logs[1]), jnp.maximum(logs[2], logs[3]))
    shares = [jnp.exp2(log - peak) for log in logs]
    merged = sum(s * v for s, v in zip(shares, values)) / sum(shares)
    abuf[tp] = merged.astype(bf)

    att_gather.begin()
    att_gather.relay()
    att_gather.relay_far()
    att_gather.finish()
    out_ref[...] = (branch[...] + product(abuf, 0)).astype(bf)

    tokens_gather.drain()
    halo_copy.wait_send()
    for i in range(1, 8):
        part_copy(i).wait_send()
        moment_copy(i).wait_send()
        for copy in weight_copies(i):
            copy.wait_send()
        slab_copy(i).wait_send()
    for j in range(4):
        key_copy(j).wait_send()
        for n in range(3):
            quad_copy(j, n).wait_send()
        gathers[j].drain()
    for i in range(1, 4):
        query_copy(i).wait_send()
        member = (mine + i) % 4
        for copy in back_copies(member, mine):
            copy.wait_send()
    conv_gather.drain()
    att_gather.drain()


def layer(*args):
    vmem, anywhere = pl.BlockSpec(memory_space=pltpu.VMEM), pl.BlockSpec(memory_space=pl.ANY)
    bf, f32 = jnp.bfloat16, jnp.float32
    dma = pltpu.SemaphoreType.DMA
    return pl.pallas_call(
        layer_kernel,
        out_shape=jax.ShapeDtypeStruct((ROWS, 256), bf),
        in_specs=[anywhere] * 13 + [vmem] * 9,
        out_specs=vmem,
        scratch_shapes=[
            pltpu.VMEM((8, ROWS, 256), bf),
            pltpu.VMEM((ROWS, D_MODEL), bf),
            pltpu.VMEM((D_MODEL, 384), bf),
            pltpu.VMEM((64, D_MODEL), bf),
            pltpu.VMEM((128, 256), bf),
            pltpu.VMEM((256, 256), bf),
            pltpu.VMEM((256, 128), bf),
            pltpu.VMEM((256, 128), bf),
            pltpu.VMEM((ROWS, 128), f32),
            pltpu.VMEM((ROWS, 128), f32),
            pltpu.VMEM((ROWS, 384), bf),
            pltpu.VMEM((8, 48, 384), bf),
            pltpu.VMEM((ROWS + ROWS // 2, 128), bf),
            pltpu.VMEM((SHARE, 128), bf),
            pltpu.VMEM((ROWS, 128), bf),
            pltpu.VMEM((3, ROWS + ROWS // 2, 128), bf),
            pltpu.VMEM((4, 2, ROWS, 128), bf),
            pltpu.VMEM((8, KSETS, SHARE, 128), bf),
            pltpu.VMEM((2, KSETS * ROWS, 128), bf),
            pltpu.VMEM((2, KSETS * ROWS, 128), bf),
            pltpu.VMEM((256, 512), bf),
            pltpu.VMEM((4, 2, ROWS, 128), f32),
            pltpu.VMEM((4, 2, ROWS, 128), f32),
            pltpu.VMEM((4, ROWS, 128), bf),
            pltpu.VMEM((4, 8, ROWS), f32),
            pltpu.VMEM((4, ROWS, 128), bf),
            pltpu.VMEM((4, 8, ROWS), f32),
            pltpu.VMEM((ROWS, 128), f32),
            pltpu.VMEM((ROWS, 128), f32),
            pltpu.VMEM((32, 128), bf),
            pltpu.VMEM((32 + ROWS, 128), f32),
            pltpu.VMEM((ROWS, 128), f32),
            pltpu.VMEM((8, ROWS), f32),
            pltpu.VMEM((8, 8, ROWS), f32),
            pltpu.VMEM((8, ROWS, 128), bf),
            pltpu.VMEM((8, ROWS, 128), bf),
            pltpu.VMEM((2, 8, 128, 256), bf),
            pltpu.VMEM((8, 128), f32),
            pltpu.VMEM((8, 8, 128), f32),
            pltpu.VMEM((ROWS, 256), f32),
            dma((3,)), dma((3,)), dma((4,)), dma((4,)), dma((4, 3)), dma((4, 3)), dma((4, 9)), dma((4, 9)),
            dma((4,)), dma((4,)), dma((4,)), dma((4,)), dma, dma, dma((8,)), dma((8,)),
            dma((9,)), dma((9,)), dma((9,)), dma((9,)), dma((2, 8)), dma((2, 8)), dma((8,)), dma((8,)),
            dma((2,)), dma((9,)), dma((9,)), dma((11,)), dma((8,)), dma((8,)), dma((8,)), dma((8,)),
        ],
        compiler_params=pltpu.CompilerParams(collective_id=1, has_side_effects=True),
        name="layer",
    )(*args)


def rotary_tables():
    lanes = np.arange(128)
    frequency = rope_base ** (-(lanes % 16) / 16.0)
    near = np.arange(ROWS)[:, None] * frequency[None, :]
    base = (np.arange(64) * ROWS)[:, None] * frequency[None, :]
    return tuple(np.asarray(f(a), np.float32) for a in (near, base) for f in (np.cos, np.sin))


def shards(
    tokens,
    input_gain,
    query_weight,
    query_rot_weight,
    kv_down,
    rot_down,
    kv_gain,
    key_up,
    value_up,
    conv_value_weight,
    conv_gate_weight,
    conv_taps,
    conv_ln_gain,
    conv_ln_bias,
    att_out_gain,
    conv_out_gain,
    att_out_weight,
    conv_out_weight,
):
    near_cos, near_sin, base_cos, base_sin = rotary_tables()
    return layer(
        tokens,
        query_weight,
        query_rot_weight.T,
        kv_down,
        rot_down.T,
        key_up,
        value_up,
        conv_value_weight,
        conv_gate_weight,
        att_out_weight,
        conv_out_weight,
        jnp.asarray(near_cos),
        jnp.asarray(near_sin),
        jnp.asarray(base_cos),
        jnp.asarray(base_sin),
        input_gain[None, :],
        kv_gain[None, :],
        conv_taps,
        conv_ln_gain[None, :],
        conv_ln_bias[None, :],
        att_out_gain[None, :],
        conv_out_gain[None, :],
    )


def solution(mesh):
    return jax.shard_map(
        shards,
        mesh=mesh,
        in_specs=(
            P("sp", "tp"),
            P(),
            P(None, "tp"),
            P(None, "tp"),
            P(),
            P(),
            P(),
            P(None, "tp"),
            P(None, "tp"),
            P(None, "tp"),
            P(None, "tp"),
            P(None, "tp"),
            P("tp"),
            P("tp"),
            P("tp"),
            P("tp"),
            P("tp", None),
            P("tp", None),
        ),
        out_specs=P("sp", "tp"),
        check_vma=False,
    )
```

```python
import math

import jax
import jax.numpy as jnp
import numpy as np
from jax import lax
from jax.experimental import pallas as pl
from jax.experimental.pallas import tpu as pltpu
from jax.sharding import PartitionSpec as P

D_MODEL = 2048
NOPE_DIM = 64
ROT_DIM = 32
CONV_CH = 1024
KERNEL = 31

norm_eps = 1e-06
far_below = -1e30
rope_base = 10000.0


MESH = pl.DeviceIdType.MESH
ROWS = 384
SHARE = 112
KSETS = 16
PIECE = 4 * ROWS
SCALE = 1.4426950408889634 / math.sqrt(NOPE_DIM + ROT_DIM)


def ring_peers(tp):
    x, c = tp // 2, tp % 2
    right = ((x + 1) % 4) * 2 + c
    left = ((x + 3) % 4) * 2 + c
    far = ((x + 2) % 4) * 2 + c
    partner = x * 2 + (1 - c)
    return right, left, far, partner


class RingGather:
    def __init__(self, buf, lo, size, send, recv, sp, tp):
        self.buf, self.lo, self.size = buf, lo, size
        self.send, self.recv, self.sp, self.tp = send, recv, sp, tp
        self.right, self.left, self.far, self.partner = ring_peers(tp)

    def piece(self, slot, part=None):
        size = self.size if part is None else self.size // 2
        start = self.lo + size if part == 1 else self.lo
        return self.buf.at[slot, pl.ds(start, size)]

    def copy(self, slot, part, sem, to):
        return pltpu.make_async_remote_copy(
            src_ref=self.piece(slot, part),
            dst_ref=self.piece(slot, part),
            send_sem=self.send.at[sem],
            recv_sem=self.recv.at[sem],
            device_id=(self.sp, to),
            device_id_type=MESH,
        )

    def begin(self):
        self.copy(self.tp, None, 0, self.right).start()
        self.copy(self.tp, None, 1, self.left).start()
        self.copy(self.tp, None, 2, self.partner).start()

    def relay(self):
        self.copy(self.left, None, 0, self.right).wait_recv()
        self.copy(self.left, 0, 5, self.right).start()
        self.copy(self.left, None, 3, self.partner).start()
        self.copy(self.right, None, 1, self.left).wait_recv()
        self.copy(self.right, 1, 6, self.left).start()
        self.copy(self.right, None, 4, self.partner).start()

    def relay_far(self):
        self.copy(self.far, 0, 5, self.right).wait_recv()
        self.copy(self.far, 0, 7, self.partner).start()
        self.copy(self.far, 1, 6, self.left).wait_recv()
        self.copy(self.far, 1, 8, self.partner).start()

    def finish(self):
        for sem, part in ((2, None), (3, None), (4, None), (7, 0), (8, 1)):
            self.copy(self.far, part, sem, self.partner).wait_recv()

    def drain(self):
        for sem, part in ((0, None), (1, None), (2, None), (3, None), (4, None), (5, 0), (6, 1), (7, 0), (8, 1)):
            self.copy(self.tp, part, sem, self.partner).wait_send()


def member_z(member, kind):
    return 2 * member + (kind + member) % 2


def layer_kernel(
    tokens_hbm, query_hbm, query_rot_hbm, kv_down_hbm, rot_down_hbm, key_up_hbm, value_up_hbm,
    conv_value_hbm, conv_gate_hbm, att_w_ref, conv_w_ref, near_cos_hbm, near_sin_hbm,
    base_cos_ref, base_sin_ref, input_gain_ref, kv_gain_ref,
    taps_ref, ln_gain_ref, ln_bias_ref, att_gain_ref, conv_gain_ref, out_ref,
    tbuf, scaled, wall, wqr, wrd, wkvd, kup, vup, near_cos, near_sin, p_send, p_recv,
    q_ref, share_ref, gated_ref,
    qraw, qbuf, kbuf, kk, vv, wkv, top, acc, o_send, l_send, o_recv, l_recv, own_out, own_lse,
    halo, padded, conv_out, mom_send, mom_recv, cbuf, abuf, weights, gains, gain_all, branch,
    q_ssem, q_rsem, k_ssem, k_rsem, f_ssem, f_rsem, ag_ssem, ag_rsem, o_ssem, o_rsem, l_ssem, l_rsem,
    h_ssem, h_rsem, m_ssem, m_rsem, c_ssem, c_rsem, a_ssem, a_rsem, w_ssem, w_rsem, g_ssem, g_rsem,
    own_sem, t_ssem, t_rsem, load_sem, p_ssem, p_rsem, v_ssem, v_rsem,
):
    sp, tp = lax.axis_index("sp"), lax.axis_index("tp")
    z, y = sp // 8, sp % 8
    kind, mine, parity = (z + z // 2) % 2, z // 2, y % 2
    residue = (y // 2 + mine + 2) % 4
    bf, f32 = jnp.bfloat16, jnp.float32

    def member_sp(member):
        return member_z(member, kind) * 8 + y

    place = 2 * parity + z % 2
    z_other, y_other = z + 1 - 2 * (z % 2), y + 1 - 2 * parity
    quad = (z_other * 8 + y, z * 8 + y_other, z_other * 8 + y_other)
    key_peers = []
    for d in range(4):
        m = (mine + d) % 4
        key_peers.append((2 * m + z % 2) * 8 + 2 * ((residue + 4 - m) % 4) + parity)
    after, before_sp = (sp + 1) % 64, (sp + 63) % 64

    own_rows = pl.ds(pl.multiple_of(256 * tp, 256), 256)
    wrd[32:128, :] = jnp.zeros((96, 256), bf)
    loads = [
        pltpu.make_async_copy(src, dst, load_sem.at[n])
        for n, (src, dst) in enumerate(
            (
                (tokens_hbm, tbuf.at[tp]),
                (kv_down_hbm.at[own_rows], wkvd),
                (rot_down_hbm.at[:, own_rows], wrd.at[pl.ds(0, 32)]),
                (key_up_hbm, kup),
                (value_up_hbm, vup),
                (query_hbm, wall.at[:, pl.ds(0, 128)]),
                (conv_value_hbm, wall.at[:, pl.ds(128, 128)]),
                (conv_gate_hbm, wall.at[:, pl.ds(256, 128)]),
                (query_rot_hbm, wqr),
                (near_cos_hbm, near_cos),
                (near_sin_hbm, near_sin),
            )
        )
    ]
    for load in loads:
        load.start()

    barrier = pltpu.get_barrier_semaphore()
    for i in range(1, 4):
        pl.semaphore_signal(
            barrier, inc=1, device_id=(member_sp((mine + i) % 4), tp), device_id_type=MESH
        )
        pl.semaphore_signal(barrier, inc=1, device_id=(quad[i - 1], tp), device_id_type=MESH)
    for peer in key_peers:
        pl.semaphore_signal(barrier, inc=1, device_id=(peer, tp), device_id_type=MESH)
    for i in range(1, 8):
        pl.semaphore_signal(barrier, inc=1, device_id=(sp, (tp + i) % 8), device_id_type=MESH)
        pl.semaphore_signal(barrier, inc=1, device_id=(z * 8 + (y + i) % 8, tp), device_id_type=MESH)
    pl.semaphore_signal(barrier, inc=1, device_id=(before_sp, tp), device_id_type=MESH)
    pl.semaphore_wait(barrier, 25)

    def remote(src, dst, ssem, rsem, to):
        return pltpu.make_async_remote_copy(
            src_ref=src, dst_ref=dst, send_sem=ssem, recv_sem=rsem, device_id=to, device_id_type=MESH
        )

    def scale_block(t):
        columns = pl.ds(pl.multiple_of(256 * t, 256), 256)
        x = tbuf[t].astype(f32)
        scaled[:, columns] = (x * input_gain_ref[:, columns]).astype(bf)
        return x * x

    tag = lax.broadcasted_iota(jnp.int32, (ROWS, 128), 1)
    low = tag < 64
    slab = pl.ds(pl.multiple_of(16 * y, 16), 16)

    def weight_copies(j):
        to = (sp, (tp + j) % 8)
        columns = pl.ds(pl.multiple_of(256 * ((tp + j) % 8), 256), 256)
        return (
            remote(
                att_w_ref.at[slab, columns], weights.at[0, tp, slab], w_ssem.at[0, j], w_rsem.at[0, tp], to
            ),
            remote(
                conv_w_ref.at[slab, columns], weights.at[1, tp, slab], w_ssem.at[1, j], w_rsem.at[1, tp], to
            ),
            remote(gains, gain_all.at[tp], g_ssem.at[j], g_rsem.at[tp], to),
        )

    own_weights = (
        pltpu.make_async_copy(att_w_ref.at[slab, own_rows], weights.at[0, tp, slab], own_sem.at[0]),
        pltpu.make_async_copy(conv_w_ref.at[slab, own_rows], weights.at[1, tp, slab], own_sem.at[1]),
    )

    def slab_copy(d):
        rows = weights.at[:, :, slab]
        return remote(rows, rows, v_ssem.at[d], v_rsem.at[y], (z * 8 + (y + d) % 8, tp))

    gains[...] = jnp.zeros(gains.shape, f32)
    gains[0:1, :] = att_gain_ref[...]
    gains[1:2, :] = conv_gain_ref[...]
    for copy in own_weights:
        copy.start()

    tokens_gather = RingGather(tbuf, 0, ROWS, t_ssem, t_rsem, sp, tp)
    for load in loads[0:3]:
        load.wait()
    squares = scale_block(tp)
    mine_scaled = scaled[:, own_rows]
    p_send[:, 0:256] = jnp.dot(mine_scaled, wkvd[...], preferred_element_type=f32).astype(bf)
    rot_part = lax.dot_general(
        mine_scaled, wrd[...], (((1,), (1,)), ((), ())), preferred_element_type=f32
    )
    p_send[:, 256:384] = jnp.where(
        tag == 32, jnp.sum(squares, axis=1, keepdims=True), rot_part
    ).astype(bf)

    def part_copy(j):
        peer = (tp + j) % 8
        return remote(
            p_send.at[pl.ds(pl.multiple_of(48 * peer, 16), 48)],
            p_recv.at[tp],
            p_ssem.at[j],
            p_rsem.at[tp],
            (sp, peer),
        )

    for j in range(1, 8):
        part_copy(j).start()
    tokens_gather.begin()

    for j in range(1, 8):
        for copy in weight_copies(j):
            copy.start()
    for load in loads[3:]:
        load.wait()
    lane = lax.broadcasted_iota(jnp.int32, (256, 128), 1)
    for n, ref in enumerate((kup, vup)):
        w = ref[...].astype(f32)
        wkv[:, pl.ds(256 * n, 128)] = jnp.where(lane < 64, w, 0.0).astype(bf)
        wkv[:, pl.ds(256 * n + 128, 128)] = jnp.where(lane < 64, pltpu.roll(w, 64, 1), 0.0).astype(bf)
    cos_base, sin_base = base_cos_ref[pl.ds(sp, 1), :], base_sin_ref[pl.ds(sp, 1), :]

    def turn(rows, near_c, near_s):
        cosine = near_c * cos_base - near_s * sin_base
        sine = near_s * cos_base + near_c * sin_base
        front = lax.broadcasted_iota(jnp.int32, rows.shape, 1) % 32 < 16
        other = jnp.where(front, pltpu.roll(rows, 112, 1), pltpu.roll(rows, 16, 1))
        return rows * cosine + other * jnp.where(front, -sine, sine)

    share_rows = pl.ds(pl.multiple_of(48 * tp, 16), 48)
    raw = p_send[share_rows, :].astype(f32)
    for j in range(1, 8):
        source = (tp + j) % 8
        remote(
            p_send.at[share_rows], p_recv.at[source], p_ssem.at[j], p_rsem.at[source], (sp, source)
        ).wait_recv()
        raw = raw + p_recv[source].astype(f32)
    power = jnp.sum(raw[:, 0:256] * raw[:, 0:256], axis=1, keepdims=True) / 256
    latent = (raw[:, 0:256] * lax.rsqrt(power + norm_eps) * kv_gain_ref[...]).astype(bf)
    share_ref[0:48, :] = latent[:, 0:128]
    share_ref[48:96, :] = latent[:, 128:256]
    key_rows = raw[:, 256:384]
    key_rows = key_rows * lax.rsqrt(key_rows[:, 32:33] / D_MODEL + norm_eps)
    key_rows = turn(key_rows, near_cos[share_rows, :], near_sin[share_rows, :])
    group = lax.broadcasted_iota(jnp.int32, (16, 128), 1) // 32
    fold = jnp.zeros((16, 128), f32)
    for j in range(3):
        fold = jnp.where(group == j, pltpu.roll(key_rows[16 * j : 16 * j + 16], 32 * j, 1), fold)
    share_ref[96:112, :] = fold.astype(bf)

    def block(p):
        return kbuf.at[tp, 4 * p + place]

    def key_copy(d):
        return remote(share_ref, block(mine), k_ssem.at[d], k_rsem.at[mine], (key_peers[d], tp))

    def quad_copy(p, n):
        return remote(block(p), block(p), f_ssem.at[p, n], f_rsem.at[p, n], (quad[n], tp))

    def spread(p):
        remote(share_ref, block(p), k_ssem.at[0], k_rsem.at[p], (key_peers[0], tp)).wait_recv()
        for n in range(3):
            quad_copy(p, n).start()

    def begin(p):
        for n in range(3):
            quad_copy(p, n).wait_recv()
        gathers[p].begin()

    for d in range(4):
        key_copy(d).start()

    gathers = [
        RingGather(kbuf, 4 * p, 4, ag_ssem.at[p], ag_rsem.at[p], sp, tp) for p in range(4)
    ]
    conv_gather = RingGather(cbuf, 0, ROWS, c_ssem, c_rsem, sp, tp)
    att_gather = RingGather(abuf, 0, ROWS, a_ssem, a_rsem, sp, tp)

    tokens_gather.relay()
    squares = squares + scale_block(tokens_gather.left)
    squares = squares + scale_block(tokens_gather.right)
    for p in range(4):
        spread(p)
    tokens_gather.relay_far()
    tokens_gather.finish()
    begin(0)
    begin(1)
    squares = squares + scale_block(tokens_gather.far)
    for t in (tp, tokens_gather.left, tokens_gather.right, tokens_gather.far):
        squares = squares + scale_block(t + 1 - 2 * (t % 2))
    row_scale = lax.rsqrt(jnp.sum(squares, axis=1, keepdims=True) / D_MODEL + norm_eps)
    flat = lax.dot_general(
        scaled[...], wqr[...], (((1,), (1,)), ((), ())), preferred_element_type=f32
    )
    flat = jnp.concatenate([flat * row_scale, jnp.zeros((ROWS, 64), f32)], axis=1)
    turned_rows = turn(flat, near_cos[...], near_sin[...])
    sums = jnp.dot(scaled[...], wall[...], preferred_element_type=f32)
    q_ref[0:ROWS, :] = (sums[:, 0:128] * (row_scale * SCALE)).astype(bf)
    half = ROWS // 2
    q_ref[ROWS : ROWS + half, :] = (
        jnp.where(low[0:half], turned_rows[0:half], pltpu.roll(turned_rows[half:ROWS], 64, 1)) * SCALE
    ).astype(bf)
    gated = (sums[:, 128:256] * row_scale * jax.nn.sigmoid(sums[:, 256:384] * row_scale)).astype(bf)
    gated_ref[...] = gated

    halo_copy = remote(gated_ref.at[pl.ds(ROWS - 32, 32)], halo, h_ssem, h_rsem, (after, tp))
    halo_copy.start()

    def query_copy(i):
        return remote(
            q_ref, qraw.at[i - 1], q_ssem.at[i - 1], q_rsem.at[i - 1], (member_sp((mine + i) % 4), tp)
        )

    for i in range(1, 4):
        query_copy(i).start()

    def unpack(ref, member):
        nope = ref[0:ROWS, :].astype(f32)
        fold = ref[ROWS : ROWS + ROWS // 2, :].astype(f32)
        for h in range(2):
            body = nope if h == 0 else pltpu.roll(nope, 64, 1)
            upper = pltpu.roll(fold, 64 - 32 * h, 1)
            lower = fold if h == 0 else pltpu.roll(fold, 96, 1)
            rotary = jnp.concatenate([upper, lower], axis=0)
            qbuf[member, h] = jnp.where(low, body, jnp.where(tag < 96, rotary, 0.0)).astype(bf)

    gathers[0].relay()
    begin(2)
    for copy in own_weights:
        copy.wait()
    for j in range(1, 8):
        source = (tp + j) % 8
        for n in range(2):
            rows = weights.at[n, source, slab]
            remote(rows, rows, w_ssem.at[n, j], w_rsem.at[n, source], (sp, source)).wait_recv()
        remote(gains, gain_all.at[source], g_ssem.at[j], g_rsem.at[source], (sp, source)).wait_recv()
    for d in range(1, 8):
        slab_copy(d).start()
    unpack(q_ref, mine)
    gathers[1].relay()
    begin(3)

    halo_copy.wait_recv()
    edge = halo[...].astype(f32)
    padded[0:32, :] = jnp.where(sp > 0, edge, jnp.zeros_like(edge))
    padded[pl.ds(32, ROWS), :] = gated_ref[...].astype(f32)
    total = jnp.zeros((ROWS, 128), f32)
    for tap in range(KERNEL):
        total = total + taps_ref[tap : tap + 1, :] * padded[pl.ds(tap + 2, ROWS), :]
    conv_out[...] = total
    sum_one = jnp.sum(total, axis=1, keepdims=True)
    sum_two = jnp.sum(total * total, axis=1, keepdims=True)
    mom_send[...] = jnp.transpose(jnp.where(tag == 0, sum_one, sum_two))[0:8, :]

    def moment_copy(j):
        return remote(
            mom_send, mom_recv.at[tp], m_ssem.at[j], m_rsem.at[tp], (sp, (tp + j) % 8)
        )

    for j in range(1, 8):
        moment_copy(j).start()

    def assemble(p):
        slots = [4 * p + u for u in range(4)]
        at = pl.ds(pl.multiple_of(p * PIECE, PIECE), PIECE)
        first = jnp.concatenate([kbuf[:, s, 0:48, :].reshape(ROWS, 128) for s in slots], axis=0)
        second = jnp.concatenate([kbuf[:, s, 48:96, :].reshape(ROWS, 128) for s in slots], axis=0)
        product = jnp.dot(
            jnp.concatenate([first, second], axis=1), wkv[...], preferred_element_type=f32
        )
        pieces = []
        for s in slots:
            folded = kbuf[:, s, 96:112, :].astype(f32).reshape(128, 128)
            turned = [
                pltpu.roll(folded, (64 - 32 * j) % 128, 1).reshape(8, 1, 16, 128) for j in range(3)
            ]
            pieces.append(jnp.concatenate(turned, axis=1).reshape(ROWS, 128))
        rotary = jnp.concatenate(pieces, axis=0)
        front = lax.broadcasted_iota(jnp.int32, (PIECE, 128), 1) < 64
        for h in range(2):
            kk[h, at, :] = jnp.where(
                front, product[:, 128 * h : 128 * h + 128], rotary
            ).astype(bf)
            vv[h, at, :] = jnp.where(
                front, product[:, 256 + 128 * h : 384 + 128 * h], 1.0
            ).astype(bf)

    def step(member, p, masked):
        if masked:
            offset = lax.broadcasted_iota(jnp.int32, (ROWS, ROWS), 1) - lax.broadcasted_iota(
                jnp.int32, (ROWS, ROWS), 0
            )
            block = member_sp(member)
        for h in range(2):
            scores = lax.dot_general(
                qbuf[member, h],
                kk[h, pl.ds(p * PIECE, PIECE), :],
                (((1,), (1,)), ((), ())),
                preferred_element_type=f32,
            )
            if masked:
                columns = []
                for u in range(4):
                    key_block = (2 * p + u % 2) * 8 + 2 * ((residue + 4 - p) % 4) + u // 2
                    columns.append(
                        jnp.where(
                            offset <= (block - key_block) * ROWS,
                            scores[:, ROWS * u : ROWS * u + ROWS],
                            far_below,
                        )
                    )
                scores = jnp.concatenate(columns, axis=1)
            now = jnp.broadcast_to(jnp.max(scores, axis=1, keepdims=True), (ROWS, 128))
            if p > 0:
                before = top[member, h]
                now = jnp.maximum(before, now)
            top[member, h] = now
            likely = jnp.exp2(scores - jnp.concatenate([now] * (PIECE // 128), axis=1)).astype(bf)
            fresh = jnp.dot(likely, vv[h, pl.ds(p * PIECE, PIECE), :], preferred_element_type=f32)
            if p > 0:
                fresh = acc[member, h] * jnp.exp2(before - now) + fresh
            acc[member, h] = fresh

    def back_copies(member, source):
        to = (member_sp(member), tp)
        return (
            remote(o_send.at[member], o_recv.at[source], o_ssem.at[member], o_rsem.at[source], to),
            remote(l_send.at[member], l_recv.at[source], l_ssem.at[member], l_rsem.at[source], to),
        )

    def finalize(member):
        sums, tops = [], []
        for h in range(2):
            a = acc[member, h]
            part = jnp.where(low, pltpu.roll(a, 64, 1), a)
            sums.append(part)
            tops.append(top[member, h] + jnp.log2(part))
        value = jnp.where(low, acc[member, 0], pltpu.roll(acc[member, 1], 64, 1))
        value = value / jnp.where(low, sums[0], sums[1])
        o_send[member] = value.astype(bf)
        l_send[member] = jnp.transpose(jnp.where(tag < 4, tops[0], tops[1]))[0:8, :]

        @pl.when(mine == member)
        def _():
            own_out[...] = value
            own_lse[...] = jnp.where(low, tops[0], tops[1])

        @pl.when(mine != member)
        def _():
            for copy in back_copies(member, mine):
                copy.start()

    def arrive(i):
        query_copy(i).wait_recv()
        member = (mine + 4 - i) % 4
        unpack(qraw.at[i - 1], member)
        return member

    gathers[0].relay_far()
    gathers[2].relay()
    gathers[0].finish()
    assemble(0)
    gathers[1].relay_far()
    gathers[3].relay()
    step(mine, 0, True)
    gathers[2].relay_far()

    mom_recv[tp] = mom_send[...]
    for j in range(1, 8):
        source = (tp + j) % 8
        remote(mom_send, mom_recv.at[source], m_ssem.at[j], m_rsem.at[source], (sp, source)).wait_recv()
    moments = mom_recv[0]
    for t in range(1, 8):
        moments = moments + mom_recv[t]
    columns = jnp.transpose(moments)
    mean_val = columns[:, 0:1] / CONV_CH
    spread = columns[:, 1:2] / CONV_CH - mean_val * mean_val
    normed = (conv_out[...] - mean_val) * lax.rsqrt(spread + norm_eps)
    swished = jax.nn.silu(normed * ln_gain_ref[...] + ln_bias_ref[...])
    cbuf[tp] = swished.astype(bf)

    gathers[3].relay_far()
    conv_gather.begin()
    step(arrive(1), 0, True)
    gathers[1].finish()
    assemble(1)
    step(arrive(3), 0, True)
    for p in (2, 3):
        gathers[p].finish()
        assemble(p)
    conv_gather.relay()
    step(arrive(2), 0, True)
    finalize(0)
    conv_gather.relay_far()
    step(1, 1, True)
    finalize(1)
    step(2, 1, False)
    step(2, 2, True)
    finalize(2)
    step(3, 1, False)
    step(3, 2, False)
    step(3, 3, True)
    finalize(3)

    gain_all[tp] = gains[...]
    conv_gather.finish()
    for d in range(1, 8):
        source = (y + d) % 8
        rows = weights.at[:, :, pl.ds(pl.multiple_of(16 * source, 16), 16)]
        remote(rows, rows, v_ssem.at[d], v_rsem.at[source], (z * 8 + source, tp)).wait_recv()

    def product(buf, n):
        wide = jnp.concatenate([buf[t] for t in range(8)], axis=1).astype(f32)
        gain = jnp.concatenate([gain_all[t, n : n + 1, :] for t in range(8)], axis=1)
        power = jnp.sum(wide * wide, axis=1, keepdims=True)
        mixed = (wide * lax.rsqrt(power / CONV_CH + norm_eps) * gain).astype(bf)
        return jnp.dot(mixed, weights[n].reshape(1024, 256), preferred_element_type=f32)

    branch[...] = product(cbuf, 1)

    logs, values = [own_lse[...]], [own_out[...]]
    for i in range(1, 4):
        source = (mine + i) % 4
        for copy in back_copies(source, source):
            copy.wait_recv()
        columns = jnp.transpose(l_recv[source])
        logs.append(jnp.where(low, columns[:, 0:1], columns[:, 4:5]))
        values.append(o_recv[source].astype(f32))
    peak = jnp.maximum(jnp.maximum(logs[0], logs[1]), jnp.maximum(logs[2], logs[3]))
    shares = [jnp.exp2(log - peak) for log in logs]
    merged = sum(s * v for s, v in zip(shares, values)) / sum(shares)
    abuf[tp] = merged.astype(bf)

    att_gather.begin()
    att_gather.relay()
    att_gather.relay_far()
    att_gather.finish()
    out_ref[...] = (branch[...] + product(abuf, 0)).astype(bf)

    tokens_gather.drain()
    halo_copy.wait_send()
    for i in range(1, 8):
        part_copy(i).wait_send()
        moment_copy(i).wait_send()
        for copy in weight_copies(i):
            copy.wait_send()
        slab_copy(i).wait_send()
    for j in range(4):
        key_copy(j).wait_send()
        for n in range(3):
            quad_copy(j, n).wait_send()
        gathers[j].drain()
    for i in range(1, 4):
        query_copy(i).wait_send()
        member = (mine + i) % 4
        for copy in back_copies(member, mine):
            copy.wait_send()
    conv_gather.drain()
    att_gather.drain()


def layer(*args):
    vmem, anywhere = pl.BlockSpec(memory_space=pltpu.VMEM), pl.BlockSpec(memory_space=pl.ANY)
    bf, f32 = jnp.bfloat16, jnp.float32
    dma = pltpu.SemaphoreType.DMA
    return pl.pallas_call(
        layer_kernel,
        out_shape=jax.ShapeDtypeStruct((ROWS, 256), bf),
        in_specs=[anywhere] * 13 + [vmem] * 9,
        out_specs=vmem,
        scratch_shapes=[
            pltpu.VMEM((8, ROWS, 256), bf),
            pltpu.VMEM((ROWS, D_MODEL), bf),
            pltpu.VMEM((D_MODEL, 384), bf),
            pltpu.VMEM((64, D_MODEL), bf),
            pltpu.VMEM((128, 256), bf),
            pltpu.VMEM((256, 256), bf),
            pltpu.VMEM((256, 128), bf),
            pltpu.VMEM((256, 128), bf),
            pltpu.VMEM((ROWS, 128), f32),
            pltpu.VMEM((ROWS, 128), f32),
            pltpu.VMEM((ROWS, 384), bf),
            pltpu.VMEM((8, 48, 384), bf),
            pltpu.VMEM((ROWS + ROWS // 2, 128), bf),
            pltpu.VMEM((SHARE, 128), bf),
            pltpu.VMEM((ROWS, 128), bf),
            pltpu.VMEM((3, ROWS + ROWS // 2, 128), bf),
            pltpu.VMEM((4, 2, ROWS, 128), bf),
            pltpu.VMEM((8, KSETS, SHARE, 128), bf),
            pltpu.VMEM((2, KSETS * ROWS, 128), bf),
            pltpu.VMEM((2, KSETS * ROWS, 128), bf),
            pltpu.VMEM((256, 512), bf),
            pltpu.VMEM((4, 2, ROWS, 128), f32),
            pltpu.VMEM((4, 2, ROWS, 128), f32),
            pltpu.VMEM((4, ROWS, 128), bf),
            pltpu.VMEM((4, 8, ROWS), f32),
            pltpu.VMEM((4, ROWS, 128), bf),
            pltpu.VMEM((4, 8, ROWS), f32),
            pltpu.VMEM((ROWS, 128), f32),
            pltpu.VMEM((ROWS, 128), f32),
            pltpu.VMEM((32, 128), bf),
            pltpu.VMEM((32 + ROWS, 128), f32),
            pltpu.VMEM((ROWS, 128), f32),
            pltpu.VMEM((8, ROWS), f32),
            pltpu.VMEM((8, 8, ROWS), f32),
            pltpu.VMEM((8, ROWS, 128), bf),
            pltpu.VMEM((8, ROWS, 128), bf),
            pltpu.VMEM((2, 8, 128, 256), bf),
            pltpu.VMEM((8, 128), f32),
            pltpu.VMEM((8, 8, 128), f32),
            pltpu.VMEM((ROWS, 256), f32),
            dma((3,)), dma((3,)), dma((4,)), dma((4,)), dma((4, 3)), dma((4, 3)), dma((4, 9)), dma((4, 9)),
            dma((4,)), dma((4,)), dma((4,)), dma((4,)), dma, dma, dma((8,)), dma((8,)),
            dma((9,)), dma((9,)), dma((9,)), dma((9,)), dma((2, 8)), dma((2, 8)), dma((8,)), dma((8,)),
            dma((2,)), dma((9,)), dma((9,)), dma((11,)), dma((8,)), dma((8,)), dma((8,)), dma((8,)),
        ],
        compiler_params=pltpu.CompilerParams(collective_id=1, has_side_effects=True),
        name="layer",
    )(*args)


def rotary_tables():
    lanes = np.arange(128)
    frequency = rope_base ** (-(lanes % 16) / 16.0)
    near = np.arange(ROWS)[:, None] * frequency[None, :]
    base = (np.arange(64) * ROWS)[:, None] * frequency[None, :]
    return tuple(np.asarray(f(a), np.float32) for a in (near, base) for f in (np.cos, np.sin))


def shards(
    tokens,
    input_gain,
    query_weight,
    query_rot_weight,
    kv_down,
    rot_down,
    kv_gain,
    key_up,
    value_up,
    conv_value_weight,
    conv_gate_weight,
    conv_taps,
    conv_ln_gain,
    conv_ln_bias,
    att_out_gain,
    conv_out_gain,
    att_out_weight,
    conv_out_weight,
):
    near_cos, near_sin, base_cos, base_sin = rotary_tables()
    return layer(
        tokens,
        query_weight,
        query_rot_weight.T,
        kv_down,
        rot_down.T,
        key_up,
        value_up,
        conv_value_weight,
        conv_gate_weight,
        att_out_weight,
        conv_out_weight,
        jnp.asarray(near_cos),
        jnp.asarray(near_sin),
        jnp.asarray(base_cos),
        jnp.asarray(base_sin),
        input_gain[None, :],
        kv_gain[None, :],
        conv_taps,
        conv_ln_gain[None, :],
        conv_ln_bias[None, :],
        att_out_gain[None, :],
        conv_out_gain[None, :],
    )


def solution(mesh):
    return jax.shard_map(
        shards,
        mesh=mesh,
        in_specs=(
            P("sp", "tp"),
            P(),
            P(None, "tp"),
            P(None, "tp"),
            P(),
            P(),
            P(),
            P(None, "tp"),
            P(None, "tp"),
            P(None, "tp"),
            P(None, "tp"),
            P(None, "tp"),
            P("tp"),
            P("tp"),
            P("tp"),
            P("tp"),
            P("tp", None),
            P("tp", None),
        ),
        out_specs=P("sp", "tp"),
        check_vma=False,
    )
```

```python
import math

import jax
import jax.numpy as jnp
import numpy as np
from jax import lax
from jax.experimental import pallas as pl
from jax.experimental.pallas import tpu as pltpu
from jax.sharding import PartitionSpec as P

D_MODEL = 2048
NOPE_DIM = 64
ROT_DIM = 32
CONV_CH = 1024
KERNEL = 31

norm_eps = 1e-06
far_below = -1e30
rope_base = 10000.0


MESH = pl.DeviceIdType.MESH
ROWS = 384
SHARE = 112
KSETS = 16
PIECE = 4 * ROWS
SCALE = 1.4426950408889634 / math.sqrt(NOPE_DIM + ROT_DIM)


def ring_peers(tp):
    x, c = tp // 2, tp % 2
    right = ((x + 1) % 4) * 2 + c
    left = ((x + 3) % 4) * 2 + c
    far = ((x + 2) % 4) * 2 + c
    partner = x * 2 + (1 - c)
    return right, left, far, partner


class RingGather:
    def __init__(self, buf, lo, size, send, recv, sp, tp):
        self.buf, self.lo, self.size = buf, lo, size
        self.send, self.recv, self.sp, self.tp = send, recv, sp, tp
        self.right, self.left, self.far, self.partner = ring_peers(tp)

    def piece(self, slot, part=None):
        size = self.size if part is None else self.size // 2
        start = self.lo + size if part == 1 else self.lo
        return self.buf.at[slot, pl.ds(start, size)]

    def copy(self, slot, part, sem, to):
        return pltpu.make_async_remote_copy(
            src_ref=self.piece(slot, part),
            dst_ref=self.piece(slot, part),
            send_sem=self.send.at[sem],
            recv_sem=self.recv.at[sem],
            device_id=(self.sp, to),
            device_id_type=MESH,
        )

    def begin(self):
        self.copy(self.tp, None, 0, self.right).start()
        self.copy(self.tp, None, 1, self.left).start()
        self.copy(self.tp, None, 2, self.partner).start()

    def relay(self):
        self.copy(self.left, None, 0, self.right).wait_recv()
        self.copy(self.left, 0, 5, self.right).start()
        self.copy(self.left, None, 3, self.partner).start()
        self.copy(self.right, None, 1, self.left).wait_recv()
        self.copy(self.right, 1, 6, self.left).start()
        self.copy(self.right, None, 4, self.partner).start()

    def relay_far(self):
        self.copy(self.far, 0, 5, self.right).wait_recv()
        self.copy(self.far, 0, 7, self.partner).start()
        self.copy(self.far, 1, 6, self.left).wait_recv()
        self.copy(self.far, 1, 8, self.partner).start()

    def finish(self):
        for sem, part in ((2, None), (3, None), (4, None), (7, 0), (8, 1)):
            self.copy(self.far, part, sem, self.partner).wait_recv()

    def drain(self):
        for sem, part in ((0, None), (1, None), (2, None), (3, None), (4, None), (5, 0), (6, 1), (7, 0), (8, 1)):
            self.copy(self.tp, part, sem, self.partner).wait_send()


def member_z(member, kind):
    return 2 * member + (kind + member) % 2


def layer_kernel(
    tokens_hbm, query_hbm, query_rot_hbm, kv_down_hbm, rot_down_hbm, key_up_hbm, value_up_hbm,
    conv_value_hbm, conv_gate_hbm, att_w_ref, conv_w_ref, near_cos_hbm, near_sin_hbm,
    base_cos_ref, base_sin_ref, input_gain_ref, kv_gain_ref,
    taps_ref, ln_gain_ref, ln_bias_ref, att_gain_ref, conv_gain_ref, out_ref,
    tbuf, scaled, wall, wqr, wrd, wkvd, kup, vup, near_cos, near_sin, p_send, p_recv,
    q_ref, share_ref, gated_ref,
    qraw, qbuf, kbuf, kk, vv, wkv, top, acc, o_send, l_send, o_recv, l_recv, own_out, own_lse,
    halo, padded, conv_out, mom_send, mom_recv, cbuf, abuf, weights, gains, gain_all, branch,
    q_ssem, q_rsem, k_ssem, k_rsem, f_ssem, f_rsem, ag_ssem, ag_rsem, o_ssem, o_rsem, l_ssem, l_rsem,
    h_ssem, h_rsem, m_ssem, m_rsem, c_ssem, c_rsem, a_ssem, a_rsem, w_ssem, w_rsem, g_ssem, g_rsem,
    own_sem, t_ssem, t_rsem, load_sem, p_ssem, p_rsem, v_ssem, v_rsem,
):
    sp, tp = lax.axis_index("sp"), lax.axis_index("tp")
    z, y = sp // 8, sp % 8
    kind, mine, parity = (z + z // 2) % 2, z // 2, y % 2
    residue = (y // 2 + mine + 2) % 4
    bf, f32 = jnp.bfloat16, jnp.float32

    def member_sp(member):
        return member_z(member, kind) * 8 + y

    place = 2 * parity + z % 2
    z_other, y_other = z + 1 - 2 * (z % 2), y + 1 - 2 * parity
    quad = (z_other * 8 + y, z * 8 + y_other, z_other * 8 + y_other)
    key_peers = []
    for d in range(4):
        m = (mine + d) % 4
        key_peers.append((2 * m + z % 2) * 8 + 2 * ((residue + 4 - m) % 4) + parity)
    after, before_sp = (sp + 1) % 64, (sp + 63) % 64

    barrier = pltpu.get_barrier_semaphore()
    for i in range(1, 4):
        pl.semaphore_signal(
            barrier, inc=1, device_id=(member_sp((mine + i) % 4), tp), device_id_type=MESH
        )
        pl.semaphore_signal(barrier, inc=1, device_id=(quad[i - 1], tp), device_id_type=MESH)
    for peer in key_peers:
        pl.semaphore_signal(barrier, inc=1, device_id=(peer, tp), device_id_type=MESH)
    for i in range(1, 8):
        pl.semaphore_signal(barrier, inc=1, device_id=(sp, (tp + i) % 8), device_id_type=MESH)
        pl.semaphore_signal(barrier, inc=1, device_id=(z * 8 + (y + i) % 8, tp), device_id_type=MESH)
    pl.semaphore_signal(barrier, inc=1, device_id=(before_sp, tp), device_id_type=MESH)

    own_rows = pl.ds(pl.multiple_of(256 * tp, 256), 256)
    wrd[32:128, :] = jnp.zeros((96, 256), bf)
    loads = [
        pltpu.make_async_copy(src, dst, load_sem.at[n])
        for n, (src, dst) in enumerate(
            (
                (tokens_hbm, tbuf.at[tp]),
                (kv_down_hbm.at[own_rows], wkvd),
                (rot_down_hbm.at[:, own_rows], wrd.at[pl.ds(0, 32)]),
                (key_up_hbm, kup),
                (value_up_hbm, vup),
                (query_hbm, wall.at[:, pl.ds(0, 128)]),
                (conv_value_hbm, wall.at[:, pl.ds(128, 128)]),
                (conv_gate_hbm, wall.at[:, pl.ds(256, 128)]),
                (query_rot_hbm, wqr),
                (near_cos_hbm, near_cos),
                (near_sin_hbm, near_sin),
            )
        )
    ]
    for load in loads:
        load.start()

    def remote(src, dst, ssem, rsem, to):
        return pltpu.make_async_remote_copy(
            src_ref=src, dst_ref=dst, send_sem=ssem, recv_sem=rsem, device_id=to, device_id_type=MESH
        )

    def scale_block(t):
        columns = pl.ds(pl.multiple_of(256 * t, 256), 256)
        x = tbuf[t].astype(f32)
        scaled[:, columns] = (x * input_gain_ref[:, columns]).astype(bf)
        return x * x

    tag = lax.broadcasted_iota(jnp.int32, (ROWS, 128), 1)
    low = tag < 64
    slab = pl.ds(pl.multiple_of(16 * y, 16), 16)

    def weight_copies(j):
        to = (sp, (tp + j) % 8)
        columns = pl.ds(pl.multiple_of(256 * ((tp + j) % 8), 256), 256)
        return (
            remote(
                att_w_ref.at[slab, columns], weights.at[0, tp, slab], w_ssem.at[0, j], w_rsem.at[0, tp], to
            ),
            remote(
                conv_w_ref.at[slab, columns], weights.at[1, tp, slab], w_ssem.at[1, j], w_rsem.at[1, tp], to
            ),
            remote(gains, gain_all.at[tp], g_ssem.at[j], g_rsem.at[tp], to),
        )

    own_weights = (
        pltpu.make_async_copy(att_w_ref.at[slab, own_rows], weights.at[0, tp, slab], own_sem.at[0]),
        pltpu.make_async_copy(conv_w_ref.at[slab, own_rows], weights.at[1, tp, slab], own_sem.at[1]),
    )

    def slab_copy(d):
        rows = weights.at[:, :, slab]
        return remote(rows, rows, v_ssem.at[d], v_rsem.at[y], (z * 8 + (y + d) % 8, tp))

    gains[...] = jnp.zeros(gains.shape, f32)
    gains[0:1, :] = att_gain_ref[...]
    gains[1:2, :] = conv_gain_ref[...]
    for copy in own_weights:
        copy.start()

    tokens_gather = RingGather(tbuf, 0, ROWS, t_ssem, t_rsem, sp, tp)
    for load in loads[0:3]:
        load.wait()
    squares = scale_block(tp)
    mine_scaled = scaled[:, own_rows]
    p_send[:, 0:256] = jnp.dot(mine_scaled, wkvd[...], preferred_element_type=f32).astype(bf)
    rot_part = lax.dot_general(
        mine_scaled, wrd[...], (((1,), (1,)), ((), ())), preferred_element_type=f32
    )
    p_send[:, 256:384] = jnp.where(
        tag == 32, jnp.sum(squares, axis=1, keepdims=True), rot_part
    ).astype(bf)

    def part_copy(j):
        peer = (tp + j) % 8
        return remote(
            p_send.at[pl.ds(pl.multiple_of(48 * peer, 16), 48)],
            p_recv.at[tp],
            p_ssem.at[j],
            p_rsem.at[tp],
            (sp, peer),
        )

    pl.semaphore_wait(barrier, 25)
    for j in range(1, 8):
        part_copy(j).start()
    tokens_gather.begin()

    for j in range(1, 8):
        for copy in weight_copies(j):
            copy.start()
    for load in loads[3:]:
        load.wait()
    lane = lax.broadcasted_iota(jnp.int32, (256, 128), 1)
    for n, ref in enumerate((kup, vup)):
        w = ref[...].astype(f32)
        wkv[:, pl.ds(256 * n, 128)] = jnp.where(lane < 64, w, 0.0).astype(bf)
        wkv[:, pl.ds(256 * n + 128, 128)] = jnp.where(lane < 64, pltpu.roll(w, 64, 1), 0.0).astype(bf)
    cos_base, sin_base = base_cos_ref[pl.ds(sp, 1), :], base_sin_ref[pl.ds(sp, 1), :]

    def turn(rows, near_c, near_s):
        cosine = near_c * cos_base - near_s * sin_base
        sine = near_s * cos_base + near_c * sin_base
        front = lax.broadcasted_iota(jnp.int32, rows.shape, 1) % 32 < 16
        other = jnp.where(front, pltpu.roll(rows, 112, 1), pltpu.roll(rows, 16, 1))
        return rows * cosine + other * jnp.where(front, -sine, sine)

    share_rows = pl.ds(pl.multiple_of(48 * tp, 16), 48)
    raw = p_send[share_rows, :].astype(f32)
    for j in range(1, 8):
        source = (tp + j) % 8
        remote(
            p_send.at[share_rows], p_recv.at[source], p_ssem.at[j], p_rsem.at[source], (sp, source)
        ).wait_recv()
        raw = raw + p_recv[source].astype(f32)
    power = jnp.sum(raw[:, 0:256] * raw[:, 0:256], axis=1, keepdims=True) / 256
    latent = (raw[:, 0:256] * lax.rsqrt(power + norm_eps) * kv_gain_ref[...]).astype(bf)
    share_ref[0:48, :] = latent[:, 0:128]
    share_ref[48:96, :] = latent[:, 128:256]
    key_rows = raw[:, 256:384]
    key_rows = key_rows * lax.rsqrt(key_rows[:, 32:33] / D_MODEL + norm_eps)
    key_rows = turn(key_rows, near_cos[share_rows, :], near_sin[share_rows, :])
    group = lax.broadcasted_iota(jnp.int32, (16, 128), 1) // 32
    fold = jnp.zeros((16, 128), f32)
    for j in range(3):
        fold = jnp.where(group == j, pltpu.roll(key_rows[16 * j : 16 * j + 16], 32 * j, 1), fold)
    share_ref[96:112, :] = fold.astype(bf)

    def block(p):
        return kbuf.at[tp, 4 * p + place]

    def key_copy(d):
        return remote(share_ref, block(mine), k_ssem.at[d], k_rsem.at[mine], (key_peers[d], tp))

    def quad_copy(p, n):
        return remote(block(p), block(p), f_ssem.at[p, n], f_rsem.at[p, n], (quad[n], tp))

    def spread(p):
        remote(share_ref, block(p), k_ssem.at[0], k_rsem.at[p], (key_peers[0], tp)).wait_recv()
        for n in range(3):
            quad_copy(p, n).start()

    def begin(p):
        for n in range(3):
            quad_copy(p, n).wait_recv()
        gathers[p].begin()

    for d in range(4):
        key_copy(d).start()

    gathers = [
        RingGather(kbuf, 4 * p, 4, ag_ssem.at[p], ag_rsem.at[p], sp, tp) for p in range(4)
    ]
    conv_gather = RingGather(cbuf, 0, ROWS, c_ssem, c_rsem, sp, tp)
    att_gather = RingGather(abuf, 0, ROWS, a_ssem, a_rsem, sp, tp)

    tokens_gather.relay()
    squares = squares + scale_block(tokens_gather.left)
    squares = squares + scale_block(tokens_gather.right)
    for p in range(4):
        spread(p)
    tokens_gather.relay_far()
    tokens_gather.finish()
    begin(0)
    begin(1)
    squares = squares + scale_block(tokens_gather.far)
    for t in (tp, tokens_gather.left, tokens_gather.right, tokens_gather.far):
        squares = squares + scale_block(t + 1 - 2 * (t % 2))
    row_scale = lax.rsqrt(jnp.sum(squares, axis=1, keepdims=True) / D_MODEL + norm_eps)
    flat = lax.dot_general(
        scaled[...], wqr[...], (((1,), (1,)), ((), ())), preferred_element_type=f32
    )
    flat = jnp.concatenate([flat * row_scale, jnp.zeros((ROWS, 64), f32)], axis=1)
    turned_rows = turn(flat, near_cos[...], near_sin[...])
    sums = jnp.dot(scaled[...], wall[...], preferred_element_type=f32)
    q_ref[0:ROWS, :] = (sums[:, 0:128] * (row_scale * SCALE)).astype(bf)
    half = ROWS // 2
    q_ref[ROWS : ROWS + half, :] = (
        jnp.where(low[0:half], turned_rows[0:half], pltpu.roll(turned_rows[half:ROWS], 64, 1)) * SCALE
    ).astype(bf)
    gated = (sums[:, 128:256] * row_scale * jax.nn.sigmoid(sums[:, 256:384] * row_scale)).astype(bf)
    gated_ref[...] = gated

    halo_copy = remote(gated_ref.at[pl.ds(ROWS - 32, 32)], halo, h_ssem, h_rsem, (after, tp))
    halo_copy.start()

    def query_copy(i):
        return remote(
            q_ref, qraw.at[i - 1], q_ssem.at[i - 1], q_rsem.at[i - 1], (member_sp((mine + i) % 4), tp)
        )

    for i in range(1, 4):
        query_copy(i).start()

    def unpack(ref, member):
        nope = ref[0:ROWS, :].astype(f32)
        fold = ref[ROWS : ROWS + ROWS // 2, :].astype(f32)
        for h in range(2):
            body = nope if h == 0 else pltpu.roll(nope, 64, 1)
            upper = pltpu.roll(fold, 64 - 32 * h, 1)
            lower = fold if h == 0 else pltpu.roll(fold, 96, 1)
            rotary = jnp.concatenate([upper, lower], axis=0)
            qbuf[member, h] = jnp.where(low, body, jnp.where(tag < 96, rotary, 0.0)).astype(bf)

    gathers[0].relay()
    begin(2)
    for copy in own_weights:
        copy.wait()
    for j in range(1, 8):
        source = (tp + j) % 8
        for n in range(2):
            rows = weights.at[n, source, slab]
            remote(rows, rows, w_ssem.at[n, j], w_rsem.at[n, source], (sp, source)).wait_recv()
        remote(gains, gain_all.at[source], g_ssem.at[j], g_rsem.at[source], (sp, source)).wait_recv()
    for d in range(1, 8):
        slab_copy(d).start()
    unpack(q_ref, mine)
    gathers[1].relay()
    begin(3)

    halo_copy.wait_recv()
    edge = halo[...].astype(f32)
    padded[0:32, :] = jnp.where(sp > 0, edge, jnp.zeros_like(edge))
    padded[pl.ds(32, ROWS), :] = gated_ref[...].astype(f32)
    total = jnp.zeros((ROWS, 128), f32)
    for tap in range(KERNEL):
        total = total + taps_ref[tap : tap + 1, :] * padded[pl.ds(tap + 2, ROWS), :]
    conv_out[...] = total
    sum_one = jnp.sum(total, axis=1, keepdims=True)
    sum_two = jnp.sum(total * total, axis=1, keepdims=True)
    mom_send[...] = jnp.transpose(jnp.where(tag == 0, sum_one, sum_two))[0:8, :]

    def moment_copy(j):
        return remote(
            mom_send, mom_recv.at[tp], m_ssem.at[j], m_rsem.at[tp], (sp, (tp + j) % 8)
        )

    for j in range(1, 8):
        moment_copy(j).start()

    def assemble(p):
        slots = [4 * p + u for u in range(4)]
        at = pl.ds(pl.multiple_of(p * PIECE, PIECE), PIECE)
        first = jnp.concatenate([kbuf[:, s, 0:48, :].reshape(ROWS, 128) for s in slots], axis=0)
        second = jnp.concatenate([kbuf[:, s, 48:96, :].reshape(ROWS, 128) for s in slots], axis=0)
        product = jnp.dot(
            jnp.concatenate([first, second], axis=1), wkv[...], preferred_element_type=f32
        )
        pieces = []
        for s in slots:
            folded = kbuf[:, s, 96:112, :].astype(f32).reshape(128, 128)
            turned = [
                pltpu.roll(folded, (64 - 32 * j) % 128, 1).reshape(8, 1, 16, 128) for j in range(3)
            ]
            pieces.append(jnp.concatenate(turned, axis=1).reshape(ROWS, 128))
        rotary = jnp.concatenate(pieces, axis=0)
        front = lax.broadcasted_iota(jnp.int32, (PIECE, 128), 1) < 64
        for h in range(2):
            kk[h, at, :] = jnp.where(
                front, product[:, 128 * h : 128 * h + 128], rotary
            ).astype(bf)
            vv[h, at, :] = jnp.where(
                front, product[:, 256 + 128 * h : 384 + 128 * h], 1.0
            ).astype(bf)

    def step(member, p, masked):
        if masked:
            offset = lax.broadcasted_iota(jnp.int32, (ROWS, ROWS), 1) - lax.broadcasted_iota(
                jnp.int32, (ROWS, ROWS), 0
            )
            block = member_sp(member)
        for h in range(2):
            scores = lax.dot_general(
                qbuf[member, h],
                kk[h, pl.ds(p * PIECE, PIECE), :],
                (((1,), (1,)), ((), ())),
                preferred_element_type=f32,
            )
            if masked:
                columns = []
                for u in range(4):
                    key_block = (2 * p + u % 2) * 8 + 2 * ((residue + 4 - p) % 4) + u // 2
                    columns.append(
                        jnp.where(
                            offset <= (block - key_block) * ROWS,
                            scores[:, ROWS * u : ROWS * u + ROWS],
                            far_below,
                        )
                    )
                scores = jnp.concatenate(columns, axis=1)
            now = jnp.broadcast_to(jnp.max(scores, axis=1, keepdims=True), (ROWS, 128))
            if p > 0:
                before = top[member, h]
                now = jnp.maximum(before, now)
            top[member, h] = now
            likely = jnp.exp2(scores - jnp.concatenate([now] * (PIECE // 128), axis=1)).astype(bf)
            fresh = jnp.dot(likely, vv[h, pl.ds(p * PIECE, PIECE), :], preferred_element_type=f32)
            if p > 0:
                fresh = acc[member, h] * jnp.exp2(before - now) + fresh
            acc[member, h] = fresh

    def back_copies(member, source):
        to = (member_sp(member), tp)
        return (
            remote(o_send.at[member], o_recv.at[source], o_ssem.at[member], o_rsem.at[source], to),
            remote(l_send.at[member], l_recv.at[source], l_ssem.at[member], l_rsem.at[source], to),
        )

    def finalize(member):
        sums, tops = [], []
        for h in range(2):
            a = acc[member, h]
            part = jnp.where(low, pltpu.roll(a, 64, 1), a)
            sums.append(part)
            tops.append(top[member, h] + jnp.log2(part))
        value = jnp.where(low, acc[member, 0], pltpu.roll(acc[member, 1], 64, 1))
        value = value / jnp.where(low, sums[0], sums[1])
        o_send[member] = value.astype(bf)
        l_send[member] = jnp.transpose(jnp.where(tag < 4, tops[0], tops[1]))[0:8, :]

        @pl.when(mine == member)
        def _():
            own_out[...] = value
            own_lse[...] = jnp.where(low, tops[0], tops[1])

        @pl.when(mine != member)
        def _():
            for copy in back_copies(member, mine):
                copy.start()

    def arrive(i):
        query_copy(i).wait_recv()
        member = (mine + 4 - i) % 4
        unpack(qraw.at[i - 1], member)
        return member

    gathers[0].relay_far()
    gathers[2].relay()
    gathers[0].finish()
    assemble(0)
    gathers[1].relay_far()
    gathers[3].relay()
    step(mine, 0, True)
    gathers[2].relay_far()

    gathers[3].relay_far()
    step(arrive(1), 0, True)
    gathers[1].finish()
    assemble(1)
    step(arrive(3), 0, True)
    for p in (2, 3):
        gathers[p].finish()
        assemble(p)
    mom_recv[tp] = mom_send[...]
    for j in range(1, 8):
        source = (tp + j) % 8
        remote(mom_send, mom_recv.at[source], m_ssem.at[j], m_rsem.at[source], (sp, source)).wait_recv()
    moments = mom_recv[0]
    for t in range(1, 8):
        moments = moments + mom_recv[t]
    columns = jnp.transpose(moments)
    mean_val = columns[:, 0:1] / CONV_CH
    spread = columns[:, 1:2] / CONV_CH - mean_val * mean_val
    normed = (conv_out[...] - mean_val) * lax.rsqrt(spread + norm_eps)
    swished = jax.nn.silu(normed * ln_gain_ref[...] + ln_bias_ref[...])
    cbuf[tp] = swished.astype(bf)

    conv_gather.begin()
    step(arrive(2), 0, True)
    finalize(0)
    step(1, 1, True)
    finalize(1)
    step(2, 1, False)
    conv_gather.relay()
    step(2, 2, True)
    finalize(2)
    conv_gather.relay_far()
    step(3, 1, False)
    step(3, 2, False)
    step(3, 3, True)
    finalize(3)

    gain_all[tp] = gains[...]
    conv_gather.finish()
    for d in range(1, 8):
        source = (y + d) % 8
        rows = weights.at[:, :, pl.ds(pl.multiple_of(16 * source, 16), 16)]
        remote(rows, rows, v_ssem.at[d], v_rsem.at[source], (z * 8 + source, tp)).wait_recv()

    def product(buf, n):
        wide = jnp.concatenate([buf[t] for t in range(8)], axis=1).astype(f32)
        gain = jnp.concatenate([gain_all[t, n : n + 1, :] for t in range(8)], axis=1)
        power = jnp.sum(wide * wide, axis=1, keepdims=True)
        mixed = (wide * lax.rsqrt(power / CONV_CH + norm_eps) * gain).astype(bf)
        return jnp.dot(mixed, weights[n].reshape(1024, 256), preferred_element_type=f32)

    branch[...] = product(cbuf, 1)

    logs, values = [own_lse[...]], [own_out[...]]
    for i in range(1, 4):
        source = (mine + i) % 4
        for copy in back_copies(source, source):
            copy.wait_recv()
        columns = jnp.transpose(l_recv[source])
        logs.append(jnp.where(low, columns[:, 0:1], columns[:, 4:5]))
        values.append(o_recv[source].astype(f32))
    peak = jnp.maximum(jnp.maximum(logs[0], logs[1]), jnp.maximum(logs[2], logs[3]))
    shares = [jnp.exp2(log - peak) for log in logs]
    merged = sum(s * v for s, v in zip(shares, values)) / sum(shares)
    abuf[tp] = merged.astype(bf)

    att_gather.begin()
    att_gather.relay()
    att_gather.relay_far()
    att_gather.finish()
    out_ref[...] = (branch[...] + product(abuf, 0)).astype(bf)

    tokens_gather.drain()
    halo_copy.wait_send()
    for i in range(1, 8):
        part_copy(i).wait_send()
        moment_copy(i).wait_send()
        for copy in weight_copies(i):
            copy.wait_send()
        slab_copy(i).wait_send()
    for j in range(4):
        key_copy(j).wait_send()
        for n in range(3):
            quad_copy(j, n).wait_send()
        gathers[j].drain()
    for i in range(1, 4):
        query_copy(i).wait_send()
        member = (mine + i) % 4
        for copy in back_copies(member, mine):
            copy.wait_send()
    conv_gather.drain()
    att_gather.drain()


def layer(*args):
    vmem, anywhere = pl.BlockSpec(memory_space=pltpu.VMEM), pl.BlockSpec(memory_space=pl.ANY)
    bf, f32 = jnp.bfloat16, jnp.float32
    dma = pltpu.SemaphoreType.DMA
    return pl.pallas_call(
        layer_kernel,
        out_shape=jax.ShapeDtypeStruct((ROWS, 256), bf),
        in_specs=[anywhere] * 13 + [vmem] * 9,
        out_specs=vmem,
        scratch_shapes=[
            pltpu.VMEM((8, ROWS, 256), bf),
            pltpu.VMEM((ROWS, D_MODEL), bf),
            pltpu.VMEM((D_MODEL, 384), bf),
            pltpu.VMEM((64, D_MODEL), bf),
            pltpu.VMEM((128, 256), bf),
            pltpu.VMEM((256, 256), bf),
            pltpu.VMEM((256, 128), bf),
            pltpu.VMEM((256, 128), bf),
            pltpu.VMEM((ROWS, 128), f32),
            pltpu.VMEM((ROWS, 128), f32),
            pltpu.VMEM((ROWS, 384), bf),
            pltpu.VMEM((8, 48, 384), bf),
            pltpu.VMEM((ROWS + ROWS // 2, 128), bf),
            pltpu.VMEM((SHARE, 128), bf),
            pltpu.VMEM((ROWS, 128), bf),
            pltpu.VMEM((3, ROWS + ROWS // 2, 128), bf),
            pltpu.VMEM((4, 2, ROWS, 128), bf),
            pltpu.VMEM((8, KSETS, SHARE, 128), bf),
            pltpu.VMEM((2, KSETS * ROWS, 128), bf),
            pltpu.VMEM((2, KSETS * ROWS, 128), bf),
            pltpu.VMEM((256, 512), bf),
            pltpu.VMEM((4, 2, ROWS, 128), f32),
            pltpu.VMEM((4, 2, ROWS, 128), f32),
            pltpu.VMEM((4, ROWS, 128), bf),
            pltpu.VMEM((4, 8, ROWS), f32),
            pltpu.VMEM((4, ROWS, 128), bf),
            pltpu.VMEM((4, 8, ROWS), f32),
            pltpu.VMEM((ROWS, 128), f32),
            pltpu.VMEM((ROWS, 128), f32),
            pltpu.VMEM((32, 128), bf),
            pltpu.VMEM((32 + ROWS, 128), f32),
            pltpu.VMEM((ROWS, 128), f32),
            pltpu.VMEM((8, ROWS), f32),
            pltpu.VMEM((8, 8, ROWS), f32),
            pltpu.VMEM((8, ROWS, 128), bf),
            pltpu.VMEM((8, ROWS, 128), bf),
            pltpu.VMEM((2, 8, 128, 256), bf),
            pltpu.VMEM((8, 128), f32),
            pltpu.VMEM((8, 8, 128), f32),
            pltpu.VMEM((ROWS, 256), f32),
            dma((3,)), dma((3,)), dma((4,)), dma((4,)), dma((4, 3)), dma((4, 3)), dma((4, 9)), dma((4, 9)),
            dma((4,)), dma((4,)), dma((4,)), dma((4,)), dma, dma, dma((8,)), dma((8,)),
            dma((9,)), dma((9,)), dma((9,)), dma((9,)), dma((2, 8)), dma((2, 8)), dma((8,)), dma((8,)),
            dma((2,)), dma((9,)), dma((9,)), dma((11,)), dma((8,)), dma((8,)), dma((8,)), dma((8,)),
        ],
        compiler_params=pltpu.CompilerParams(collective_id=1, has_side_effects=True),
        name="layer",
    )(*args)


def rotary_tables():
    lanes = np.arange(128)
    frequency = rope_base ** (-(lanes % 16) / 16.0)
    near = np.arange(ROWS)[:, None] * frequency[None, :]
    base = (np.arange(64) * ROWS)[:, None] * frequency[None, :]
    return tuple(np.asarray(f(a), np.float32) for a in (near, base) for f in (np.cos, np.sin))


def shards(
    tokens,
    input_gain,
    query_weight,
    query_rot_weight,
    kv_down,
    rot_down,
    kv_gain,
    key_up,
    value_up,
    conv_value_weight,
    conv_gate_weight,
    conv_taps,
    conv_ln_gain,
    conv_ln_bias,
    att_out_gain,
    conv_out_gain,
    att_out_weight,
    conv_out_weight,
):
    near_cos, near_sin, base_cos, base_sin = rotary_tables()
    return layer(
        tokens,
        query_weight,
        query_rot_weight.T,
        kv_down,
        rot_down.T,
        key_up,
        value_up,
        conv_value_weight,
        conv_gate_weight,
        att_out_weight,
        conv_out_weight,
        jnp.asarray(near_cos),
        jnp.asarray(near_sin),
        jnp.asarray(base_cos),
        jnp.asarray(base_sin),
        input_gain[None, :],
        kv_gain[None, :],
        conv_taps,
        conv_ln_gain[None, :],
        conv_ln_bias[None, :],
        att_out_gain[None, :],
        conv_out_gain[None, :],
    )


def solution(mesh):
    return jax.shard_map(
        shards,
        mesh=mesh,
        in_specs=(
            P("sp", "tp"),
            P(),
            P(None, "tp"),
            P(None, "tp"),
            P(),
            P(),
            P(),
            P(None, "tp"),
            P(None, "tp"),
            P(None, "tp"),
            P(None, "tp"),
            P(None, "tp"),
            P("tp"),
            P("tp"),
            P("tp"),
            P("tp"),
            P("tp", None),
            P("tp", None),
        ),
        out_specs=P("sp", "tp"),
        check_vma=False,
    )
```

```python
import math

import jax
import jax.numpy as jnp
import numpy as np
from jax import lax
from jax.experimental import pallas as pl
from jax.experimental.pallas import tpu as pltpu
from jax.sharding import PartitionSpec as P

D_MODEL = 2048
NOPE_DIM = 64
ROT_DIM = 32
CONV_CH = 1024
KERNEL = 31

norm_eps = 1e-06
far_below = -1e30
rope_base = 10000.0


MESH = pl.DeviceIdType.MESH
ROWS = 384
SHARE = 112
KSETS = 16
PIECE = 4 * ROWS
SCALE = 1.4426950408889634 / math.sqrt(NOPE_DIM + ROT_DIM)


def ring_peers(tp):
    x, c = tp // 2, tp % 2
    right = ((x + 1) % 4) * 2 + c
    left = ((x + 3) % 4) * 2 + c
    far = ((x + 2) % 4) * 2 + c
    partner = x * 2 + (1 - c)
    return right, left, far, partner


class RingGather:
    def __init__(self, buf, lo, size, send, recv, sp, tp):
        self.buf, self.lo, self.size = buf, lo, size
        self.send, self.recv, self.sp, self.tp = send, recv, sp, tp
        self.right, self.left, self.far, self.partner = ring_peers(tp)

    def piece(self, slot, part=None):
        size = self.size if part is None else self.size // 2
        start = self.lo + size if part == 1 else self.lo
        return self.buf.at[slot, pl.ds(start, size)]

    def copy(self, slot, part, sem, to):
        return pltpu.make_async_remote_copy(
            src_ref=self.piece(slot, part),
            dst_ref=self.piece(slot, part),
            send_sem=self.send.at[sem],
            recv_sem=self.recv.at[sem],
            device_id=(self.sp, to),
            device_id_type=MESH,
        )

    def begin(self):
        self.copy(self.tp, None, 0, self.right).start()
        self.copy(self.tp, None, 1, self.left).start()
        self.copy(self.tp, None, 2, self.partner).start()

    def relay(self):
        self.copy(self.left, None, 0, self.right).wait_recv()
        self.copy(self.left, 0, 5, self.right).start()
        self.copy(self.left, None, 3, self.partner).start()
        self.copy(self.right, None, 1, self.left).wait_recv()
        self.copy(self.right, 1, 6, self.left).start()
        self.copy(self.right, None, 4, self.partner).start()

    def relay_far(self):
        self.copy(self.far, 0, 5, self.right).wait_recv()
        self.copy(self.far, 0, 7, self.partner).start()
        self.copy(self.far, 1, 6, self.left).wait_recv()
        self.copy(self.far, 1, 8, self.partner).start()

    def finish(self):
        for sem, part in ((2, None), (3, None), (4, None), (7, 0), (8, 1)):
            self.copy(self.far, part, sem, self.partner).wait_recv()

    def drain(self):
        for sem, part in ((0, None), (1, None), (2, None), (3, None), (4, None), (5, 0), (6, 1), (7, 0), (8, 1)):
            self.copy(self.tp, part, sem, self.partner).wait_send()


def member_z(member, kind):
    return 2 * member + (kind + member) % 2


def layer_kernel(
    tokens_hbm, query_hbm, query_rot_hbm, kv_down_hbm, rot_down_hbm, key_up_hbm, value_up_hbm,
    conv_value_hbm, conv_gate_hbm, att_w_ref, conv_w_ref, near_cos_hbm, near_sin_hbm,
    base_cos_ref, base_sin_ref, input_gain_ref, kv_gain_ref,
    taps_ref, ln_gain_ref, ln_bias_ref, att_gain_ref, conv_gain_ref, out_ref,
    tbuf, scaled, wall, wqr, wrd, wkvd, kup, vup, near_cos, near_sin, p_send, p_recv,
    q_ref, share_ref, gated_ref,
    qraw, qbuf, kbuf, kk, vv, wkv, top, acc, o_send, l_send, o_recv, l_recv, own_out, own_lse,
    halo, padded, conv_out, mom_send, mom_recv, cbuf, abuf, weights, gains, gain_all, branch,
    q_ssem, q_rsem, k_ssem, k_rsem, f_ssem, f_rsem, ag_ssem, ag_rsem, o_ssem, o_rsem, l_ssem, l_rsem,
    h_ssem, h_rsem, m_ssem, m_rsem, c_ssem, c_rsem, a_ssem, a_rsem, w_ssem, w_rsem, g_ssem, g_rsem,
    own_sem, t_ssem, t_rsem, load_sem, p_ssem, p_rsem, v_ssem, v_rsem,
):
    sp, tp = lax.axis_index("sp"), lax.axis_index("tp")
    z, y = sp // 8, sp % 8
    kind, mine, parity = (z + z // 2) % 2, z // 2, y % 2
    residue = (y // 2 + mine + 2) % 4
    bf, f32 = jnp.bfloat16, jnp.float32

    def member_sp(member):
        return member_z(member, kind) * 8 + y

    place = 2 * parity + z % 2
    z_other, y_other = z + 1 - 2 * (z % 2), y + 1 - 2 * parity
    quad = (z_other * 8 + y, z * 8 + y_other, z_other * 8 + y_other)
    key_peers = []
    for d in range(4):
        m = (mine + d) % 4
        key_peers.append((2 * m + z % 2) * 8 + 2 * ((residue + 4 - m) % 4) + parity)
    after, before_sp = (sp + 1) % 64, (sp + 63) % 64

    own_rows = pl.ds(pl.multiple_of(256 * tp, 256), 256)
    wrd[32:128, :] = jnp.zeros((96, 256), bf)
    loads = [
        pltpu.make_async_copy(src, dst, load_sem.at[n])
        for n, (src, dst) in enumerate(
            (
                (tokens_hbm, tbuf.at[tp]),
                (kv_down_hbm.at[own_rows], wkvd),
                (rot_down_hbm.at[:, own_rows], wrd.at[pl.ds(0, 32)]),
                (key_up_hbm, kup),
                (value_up_hbm, vup),
                (query_hbm, wall.at[:, pl.ds(0, 128)]),
                (conv_value_hbm, wall.at[:, pl.ds(128, 128)]),
                (conv_gate_hbm, wall.at[:, pl.ds(256, 128)]),
                (query_rot_hbm, wqr),
                (near_cos_hbm, near_cos),
                (near_sin_hbm, near_sin),
            )
        )
    ]
    for load in loads:
        load.start()

    barrier = pltpu.get_barrier_semaphore()
    for i in range(1, 4):
        pl.semaphore_signal(
            barrier, inc=1, device_id=(member_sp((mine + i) % 4), tp), device_id_type=MESH
        )
        pl.semaphore_signal(barrier, inc=1, device_id=(quad[i - 1], tp), device_id_type=MESH)
    for peer in key_peers:
        pl.semaphore_signal(barrier, inc=1, device_id=(peer, tp), device_id_type=MESH)
    for i in range(1, 8):
        pl.semaphore_signal(barrier, inc=1, device_id=(sp, (tp + i) % 8), device_id_type=MESH)
        pl.semaphore_signal(barrier, inc=1, device_id=(z * 8 + (y + i) % 8, tp), device_id_type=MESH)
    pl.semaphore_signal(barrier, inc=1, device_id=(before_sp, tp), device_id_type=MESH)
    pl.semaphore_wait(barrier, 25)

    def remote(src, dst, ssem, rsem, to):
        return pltpu.make_async_remote_copy(
            src_ref=src, dst_ref=dst, send_sem=ssem, recv_sem=rsem, device_id=to, device_id_type=MESH
        )

    def scale_block(t):
        columns = pl.ds(pl.multiple_of(256 * t, 256), 256)
        x = tbuf[t].astype(f32)
        scaled[:, columns] = (x * input_gain_ref[:, columns]).astype(bf)
        return x * x

    tag = lax.broadcasted_iota(jnp.int32, (ROWS, 128), 1)
    low = tag < 64
    slab = pl.ds(pl.multiple_of(16 * y, 16), 16)

    def weight_copies(j):
        to = (sp, (tp + j) % 8)
        columns = pl.ds(pl.multiple_of(256 * ((tp + j) % 8), 256), 256)
        return (
            remote(
                att_w_ref.at[slab, columns], weights.at[0, tp, slab], w_ssem.at[0, j], w_rsem.at[0, tp], to
            ),
            remote(
                conv_w_ref.at[slab, columns], weights.at[1, tp, slab], w_ssem.at[1, j], w_rsem.at[1, tp], to
            ),
            remote(gains, gain_all.at[tp], g_ssem.at[j], g_rsem.at[tp], to),
        )

    own_weights = (
        pltpu.make_async_copy(att_w_ref.at[slab, own_rows], weights.at[0, tp, slab], own_sem.at[0]),
        pltpu.make_async_copy(conv_w_ref.at[slab, own_rows], weights.at[1, tp, slab], own_sem.at[1]),
    )

    def slab_copy(d):
        rows = weights.at[:, :, slab]
        return remote(rows, rows, v_ssem.at[d], v_rsem.at[y], (z * 8 + (y + d) % 8, tp))

    gains[...] = jnp.zeros(gains.shape, f32)
    gains[0:1, :] = att_gain_ref[...]
    gains[1:2, :] = conv_gain_ref[...]
    for copy in own_weights:
        copy.start()

    tokens_gather = RingGather(tbuf, 0, ROWS, t_ssem, t_rsem, sp, tp)
    for load in loads[0:3]:
        load.wait()
    squares = scale_block(tp)
    mine_scaled = scaled[:, own_rows]
    p_send[:, 0:256] = jnp.dot(mine_scaled, wkvd[...], preferred_element_type=f32).astype(bf)
    rot_part = lax.dot_general(
        mine_scaled, wrd[...], (((1,), (1,)), ((), ())), preferred_element_type=f32
    )
    p_send[:, 256:384] = jnp.where(
        tag == 32, jnp.sum(squares, axis=1, keepdims=True), rot_part
    ).astype(bf)

    def part_copy(j):
        peer = (tp + j) % 8
        return remote(
            p_send.at[pl.ds(pl.multiple_of(48 * peer, 16), 48)],
            p_recv.at[tp],
            p_ssem.at[j],
            p_rsem.at[tp],
            (sp, peer),
        )

    for j in range(1, 8):
        part_copy(j).start()
    tokens_gather.begin()

    for j in range(1, 8):
        for copy in weight_copies(j):
            copy.start()
    for load in loads[3:]:
        load.wait()
    lane = lax.broadcasted_iota(jnp.int32, (256, 128), 1)
    for n, ref in enumerate((kup, vup)):
        w = ref[...].astype(f32)
        wkv[:, pl.ds(256 * n, 128)] = jnp.where(lane < 64, w, 0.0).astype(bf)
        wkv[:, pl.ds(256 * n + 128, 128)] = jnp.where(lane < 64, pltpu.roll(w, 64, 1), 0.0).astype(bf)
    cos_base, sin_base = base_cos_ref[pl.ds(sp, 1), :], base_sin_ref[pl.ds(sp, 1), :]

    def turn(rows, near_c, near_s):
        cosine = near_c * cos_base - near_s * sin_base
        sine = near_s * cos_base + near_c * sin_base
        front = lax.broadcasted_iota(jnp.int32, rows.shape, 1) % 32 < 16
        other = jnp.where(front, pltpu.roll(rows, 112, 1), pltpu.roll(rows, 16, 1))
        return rows * cosine + other * jnp.where(front, -sine, sine)

    share_rows = pl.ds(pl.multiple_of(48 * tp, 16), 48)
    raw = p_send[share_rows, :].astype(f32)
    for j in range(1, 8):
        source = (tp + j) % 8
        remote(
            p_send.at[share_rows], p_recv.at[source], p_ssem.at[j], p_rsem.at[source], (sp, source)
        ).wait_recv()
        raw = raw + p_recv[source].astype(f32)
    power = jnp.sum(raw[:, 0:256] * raw[:, 0:256], axis=1, keepdims=True) / 256
    latent = (raw[:, 0:256] * lax.rsqrt(power + norm_eps) * kv_gain_ref[...]).astype(bf)
    share_ref[0:48, :] = latent[:, 0:128]
    share_ref[48:96, :] = latent[:, 128:256]
    key_rows = raw[:, 256:384]
    key_rows = key_rows * lax.rsqrt(key_rows[:, 32:33] / D_MODEL + norm_eps)
    key_rows = turn(key_rows, near_cos[share_rows, :], near_sin[share_rows, :])
    group = lax.broadcasted_iota(jnp.int32, (16, 128), 1) // 32
    fold = jnp.zeros((16, 128), f32)
    for j in range(3):
        fold = jnp.where(group == j, pltpu.roll(key_rows[16 * j : 16 * j + 16], 32 * j, 1), fold)
    share_ref[96:112, :] = fold.astype(bf)

    def block(p):
        return kbuf.at[tp, 4 * p + place]

    def key_copy(d):
        return remote(share_ref, block(mine), k_ssem.at[d], k_rsem.at[mine], (key_peers[d], tp))

    def quad_copy(p, n):
        return remote(block(p), block(p), f_ssem.at[p, n], f_rsem.at[p, n], (quad[n], tp))

    def spread(p):
        remote(share_ref, block(p), k_ssem.at[0], k_rsem.at[p], (key_peers[0], tp)).wait_recv()
        for n in range(3):
            quad_copy(p, n).start()

    def begin(p):
        for n in range(3):
            quad_copy(p, n).wait_recv()
        gathers[p].begin()

    for d in range(4):
        key_copy(d).start()

    gathers = [
        RingGather(kbuf, 4 * p, 4, ag_ssem.at[p], ag_rsem.at[p], sp, tp) for p in range(4)
    ]
    conv_gather = RingGather(cbuf, 0, ROWS, c_ssem, c_rsem, sp, tp)
    att_gathers = [
        RingGather(abuf, 192 * n, 192, a_ssem.at[n], a_rsem.at[n], sp, tp) for n in range(2)
    ]

    tokens_gather.relay()
    squares = squares + scale_block(tokens_gather.left)
    squares = squares + scale_block(tokens_gather.right)
    for p in range(4):
        spread(p)
    tokens_gather.relay_far()
    tokens_gather.finish()
    begin(0)
    begin(1)
    squares = squares + scale_block(tokens_gather.far)
    for t in (tp, tokens_gather.left, tokens_gather.right, tokens_gather.far):
        squares = squares + scale_block(t + 1 - 2 * (t % 2))
    row_scale = lax.rsqrt(jnp.sum(squares, axis=1, keepdims=True) / D_MODEL + norm_eps)
    flat = lax.dot_general(
        scaled[...], wqr[...], (((1,), (1,)), ((), ())), preferred_element_type=f32
    )
    flat = jnp.concatenate([flat * row_scale, jnp.zeros((ROWS, 64), f32)], axis=1)
    turned_rows = turn(flat, near_cos[...], near_sin[...])
    sums = jnp.dot(scaled[...], wall[...], preferred_element_type=f32)
    q_ref[0:ROWS, :] = (sums[:, 0:128] * (row_scale * SCALE)).astype(bf)
    half = ROWS // 2
    q_ref[ROWS : ROWS + half, :] = (
        jnp.where(low[0:half], turned_rows[0:half], pltpu.roll(turned_rows[half:ROWS], 64, 1)) * SCALE
    ).astype(bf)
    gated = (sums[:, 128:256] * row_scale * jax.nn.sigmoid(sums[:, 256:384] * row_scale)).astype(bf)
    gated_ref[...] = gated

    halo_copy = remote(gated_ref.at[pl.ds(ROWS - 32, 32)], halo, h_ssem, h_rsem, (after, tp))
    halo_copy.start()

    def query_copy(i):
        return remote(
            q_ref, qraw.at[i - 1], q_ssem.at[i - 1], q_rsem.at[i - 1], (member_sp((mine + i) % 4), tp)
        )

    for i in range(1, 4):
        query_copy(i).start()

    def unpack(ref, member):
        nope = ref[0:ROWS, :].astype(f32)
        fold = ref[ROWS : ROWS + ROWS // 2, :].astype(f32)
        for h in range(2):
            body = nope if h == 0 else pltpu.roll(nope, 64, 1)
            upper = pltpu.roll(fold, 64 - 32 * h, 1)
            lower = fold if h == 0 else pltpu.roll(fold, 96, 1)
            rotary = jnp.concatenate([upper, lower], axis=0)
            qbuf[member, h] = jnp.where(low, body, jnp.where(tag < 96, rotary, 0.0)).astype(bf)

    gathers[0].relay()
    begin(2)
    for copy in own_weights:
        copy.wait()
    for j in range(1, 8):
        source = (tp + j) % 8
        for n in range(2):
            rows = weights.at[n, source, slab]
            remote(rows, rows, w_ssem.at[n, j], w_rsem.at[n, source], (sp, source)).wait_recv()
        remote(gains, gain_all.at[source], g_ssem.at[j], g_rsem.at[source], (sp, source)).wait_recv()
    for d in range(1, 8):
        slab_copy(d).start()
    unpack(q_ref, mine)
    gathers[1].relay()
    begin(3)

    halo_copy.wait_recv()
    edge = halo[...].astype(f32)
    padded[0:32, :] = jnp.where(sp > 0, edge, jnp.zeros_like(edge))
    padded[pl.ds(32, ROWS), :] = gated_ref[...].astype(f32)
    total = jnp.zeros((ROWS, 128), f32)
    for tap in range(KERNEL):
        total = total + taps_ref[tap : tap + 1, :] * padded[pl.ds(tap + 2, ROWS), :]
    conv_out[...] = total
    sum_one = jnp.sum(total, axis=1, keepdims=True)
    sum_two = jnp.sum(total * total, axis=1, keepdims=True)
    mom_send[...] = jnp.transpose(jnp.where(tag == 0, sum_one, sum_two))[0:8, :]

    def moment_copy(j):
        return remote(
            mom_send, mom_recv.at[tp], m_ssem.at[j], m_rsem.at[tp], (sp, (tp + j) % 8)
        )

    for j in range(1, 8):
        moment_copy(j).start()

    def assemble(p):
        slots = [4 * p + u for u in range(4)]
        at = pl.ds(pl.multiple_of(p * PIECE, PIECE), PIECE)
        first = jnp.concatenate([kbuf[:, s, 0:48, :].reshape(ROWS, 128) for s in slots], axis=0)
        second = jnp.concatenate([kbuf[:, s, 48:96, :].reshape(ROWS, 128) for s in slots], axis=0)
        product = jnp.dot(
            jnp.concatenate([first, second], axis=1), wkv[...], preferred_element_type=f32
        )
        pieces = []
        for s in slots:
            folded = kbuf[:, s, 96:112, :].astype(f32).reshape(128, 128)
            turned = [
                pltpu.roll(folded, (64 - 32 * j) % 128, 1).reshape(8, 1, 16, 128) for j in range(3)
            ]
            pieces.append(jnp.concatenate(turned, axis=1).reshape(ROWS, 128))
        rotary = jnp.concatenate(pieces, axis=0)
        front = lax.broadcasted_iota(jnp.int32, (PIECE, 128), 1) < 64
        for h in range(2):
            kk[h, at, :] = jnp.where(
                front, product[:, 128 * h : 128 * h + 128], rotary
            ).astype(bf)
            vv[h, at, :] = jnp.where(
                front, product[:, 256 + 128 * h : 384 + 128 * h], 1.0
            ).astype(bf)

    def step(member, p, masked):
        if masked:
            offset = lax.broadcasted_iota(jnp.int32, (ROWS, ROWS), 1) - lax.broadcasted_iota(
                jnp.int32, (ROWS, ROWS), 0
            )
            block = member_sp(member)
        for h in range(2):
            scores = lax.dot_general(
                qbuf[member, h],
                kk[h, pl.ds(p * PIECE, PIECE), :],
                (((1,), (1,)), ((), ())),
                preferred_element_type=f32,
            )
            if masked:
                columns = []
                for u in range(4):
                    key_block = (2 * p + u % 2) * 8 + 2 * ((residue + 4 - p) % 4) + u // 2
                    columns.append(
                        jnp.where(
                            offset <= (block - key_block) * ROWS,
                            scores[:, ROWS * u : ROWS * u + ROWS],
                            far_below,
                        )
                    )
                scores = jnp.concatenate(columns, axis=1)
            now = jnp.broadcast_to(jnp.max(scores, axis=1, keepdims=True), (ROWS, 128))
            if p > 0:
                before = top[member, h]
                now = jnp.maximum(before, now)
            top[member, h] = now
            likely = jnp.exp2(scores - jnp.concatenate([now] * (PIECE // 128), axis=1)).astype(bf)
            fresh = jnp.dot(likely, vv[h, pl.ds(p * PIECE, PIECE), :], preferred_element_type=f32)
            if p > 0:
                fresh = acc[member, h] * jnp.exp2(before - now) + fresh
            acc[member, h] = fresh

    def back_copies(member, source):
        to = (member_sp(member), tp)
        copies = [remote(l_send.at[member], l_recv.at[source], l_ssem.at[member], l_rsem.at[source], to)]
        for n in range(2):
            rows = pl.ds(192 * n, 192)
            copies.append(
                remote(
                    o_send.at[member, rows],
                    o_recv.at[source, rows],
                    o_ssem.at[n, member],
                    o_rsem.at[n, source],
                    to,
                )
            )
        return copies

    def finalize(member):
        sums, tops = [], []
        for h in range(2):
            a = acc[member, h]
            part = jnp.where(low, pltpu.roll(a, 64, 1), a)
            sums.append(part)
            tops.append(top[member, h] + jnp.log2(part))
        value = jnp.where(low, acc[member, 0], pltpu.roll(acc[member, 1], 64, 1))
        value = value / jnp.where(low, sums[0], sums[1])
        o_send[member] = value.astype(bf)
        l_send[member] = jnp.transpose(jnp.where(tag < 4, tops[0], tops[1]))[0:8, :]

        @pl.when(mine == member)
        def _():
            own_out[...] = value
            own_lse[...] = jnp.where(low, tops[0], tops[1])

        @pl.when(mine != member)
        def _():
            for copy in back_copies(member, mine):
                copy.start()

    def arrive(i):
        query_copy(i).wait_recv()
        member = (mine + 4 - i) % 4
        unpack(qraw.at[i - 1], member)
        return member

    gathers[0].relay_far()
    gathers[2].relay()
    gathers[0].finish()
    assemble(0)
    gathers[1].relay_far()
    gathers[3].relay()
    step(mine, 0, True)
    gathers[2].relay_far()

    mom_recv[tp] = mom_send[...]
    for j in range(1, 8):
        source = (tp + j) % 8
        remote(mom_send, mom_recv.at[source], m_ssem.at[j], m_rsem.at[source], (sp, source)).wait_recv()
    moments = mom_recv[0]
    for t in range(1, 8):
        moments = moments + mom_recv[t]
    columns = jnp.transpose(moments)
    mean_val = columns[:, 0:1] / CONV_CH
    spread = columns[:, 1:2] / CONV_CH - mean_val * mean_val
    normed = (conv_out[...] - mean_val) * lax.rsqrt(spread + norm_eps)
    swished = jax.nn.silu(normed * ln_gain_ref[...] + ln_bias_ref[...])
    cbuf[tp] = swished.astype(bf)

    gathers[3].relay_far()
    conv_gather.begin()
    step(arrive(1), 0, True)
    gathers[1].finish()
    assemble(1)
    step(arrive(3), 0, True)
    for p in (2, 3):
        gathers[p].finish()
        assemble(p)
    conv_gather.relay()
    step(arrive(2), 0, True)
    finalize(0)
    conv_gather.relay_far()
    step(1, 1, True)
    finalize(1)
    step(2, 1, False)
    step(2, 2, True)
    finalize(2)
    step(3, 1, False)
    step(3, 2, False)
    step(3, 3, True)
    finalize(3)

    gain_all[tp] = gains[...]
    conv_gather.finish()
    for d in range(1, 8):
        source = (y + d) % 8
        rows = weights.at[:, :, pl.ds(pl.multiple_of(16 * source, 16), 16)]
        remote(rows, rows, v_ssem.at[d], v_rsem.at[source], (z * 8 + source, tp)).wait_recv()

    def product(buf, n):
        wide = jnp.concatenate([buf[t] for t in range(8)], axis=1).astype(f32)
        gain = jnp.concatenate([gain_all[t, n : n + 1, :] for t in range(8)], axis=1)
        power = jnp.sum(wide * wide, axis=1, keepdims=True)
        mixed = (wide * lax.rsqrt(power / CONV_CH + norm_eps) * gain).astype(bf)
        return jnp.dot(mixed, weights[n].reshape(1024, 256), preferred_element_type=f32)

    branch[...] = product(cbuf, 1)

    logs = [own_lse[...]]
    for i in range(1, 4):
        source = (mine + i) % 4
        back_copies(source, source)[0].wait_recv()
        columns = jnp.transpose(l_recv[source])
        logs.append(jnp.where(low, columns[:, 0:1], columns[:, 4:5]))
    peak = jnp.maximum(jnp.maximum(logs[0], logs[1]), jnp.maximum(logs[2], logs[3]))
    shares = [jnp.exp2(log - peak) for log in logs]
    whole = sum(shares)
    for n in range(2):
        rows = slice(192 * n, 192 * n + 192)
        merged = shares[0][rows] * own_out[rows, :]
        for i in range(1, 4):
            source = (mine + i) % 4
            back_copies(source, source)[1 + n].wait_recv()
            merged = merged + shares[i][rows] * o_recv[source, rows, :].astype(f32)
        abuf[tp, rows, :] = (merged / whole[rows]).astype(bf)
        att_gathers[n].begin()

    for gather in att_gathers:
        gather.relay()
    for gather in att_gathers:
        gather.relay_far()
    for gather in att_gathers:
        gather.finish()
    out_ref[...] = branch[...] + product(abuf, 0)

    tokens_gather.drain()
    halo_copy.wait_send()
    for i in range(1, 8):
        part_copy(i).wait_send()
        moment_copy(i).wait_send()
        for copy in weight_copies(i):
            copy.wait_send()
        slab_copy(i).wait_send()
    for j in range(4):
        key_copy(j).wait_send()
        for n in range(3):
            quad_copy(j, n).wait_send()
        gathers[j].drain()
    for i in range(1, 4):
        query_copy(i).wait_send()
        member = (mine + i) % 4
        for copy in back_copies(member, mine):
            copy.wait_send()
    conv_gather.drain()
    for gather in att_gathers:
        gather.drain()


def layer(*args):
    vmem, anywhere = pl.BlockSpec(memory_space=pltpu.VMEM), pl.BlockSpec(memory_space=pl.ANY)
    bf, f32 = jnp.bfloat16, jnp.float32
    dma = pltpu.SemaphoreType.DMA
    return pl.pallas_call(
        layer_kernel,
        out_shape=jax.ShapeDtypeStruct((ROWS, 256), f32),
        in_specs=[anywhere] * 13 + [vmem] * 9,
        out_specs=vmem,
        scratch_shapes=[
            pltpu.VMEM((8, ROWS, 256), bf),
            pltpu.VMEM((ROWS, D_MODEL), bf),
            pltpu.VMEM((D_MODEL, 384), bf),
            pltpu.VMEM((64, D_MODEL), bf),
            pltpu.VMEM((128, 256), bf),
            pltpu.VMEM((256, 256), bf),
            pltpu.VMEM((256, 128), bf),
            pltpu.VMEM((256, 128), bf),
            pltpu.VMEM((ROWS, 128), f32),
            pltpu.VMEM((ROWS, 128), f32),
            pltpu.VMEM((ROWS, 384), bf),
            pltpu.VMEM((8, 48, 384), bf),
            pltpu.VMEM((ROWS + ROWS // 2, 128), bf),
            pltpu.VMEM((SHARE, 128), bf),
            pltpu.VMEM((ROWS, 128), bf),
            pltpu.VMEM((3, ROWS + ROWS // 2, 128), bf),
            pltpu.VMEM((4, 2, ROWS, 128), bf),
            pltpu.VMEM((8, KSETS, SHARE, 128), bf),
            pltpu.VMEM((2, KSETS * ROWS, 128), bf),
            pltpu.VMEM((2, KSETS * ROWS, 128), bf),
            pltpu.VMEM((256, 512), bf),
            pltpu.VMEM((4, 2, ROWS, 128), f32),
            pltpu.VMEM((4, 2, ROWS, 128), f32),
            pltpu.VMEM((4, ROWS, 128), bf),
            pltpu.VMEM((4, 8, ROWS), f32),
            pltpu.VMEM((4, ROWS, 128), bf),
            pltpu.VMEM((4, 8, ROWS), f32),
            pltpu.VMEM((ROWS, 128), f32),
            pltpu.VMEM((ROWS, 128), f32),
            pltpu.VMEM((32, 128), bf),
            pltpu.VMEM((32 + ROWS, 128), f32),
            pltpu.VMEM((ROWS, 128), f32),
            pltpu.VMEM((8, ROWS), f32),
            pltpu.VMEM((8, 8, ROWS), f32),
            pltpu.VMEM((8, ROWS, 128), bf),
            pltpu.VMEM((8, ROWS, 128), bf),
            pltpu.VMEM((2, 8, 128, 256), bf),
            pltpu.VMEM((8, 128), f32),
            pltpu.VMEM((8, 8, 128), f32),
            pltpu.VMEM((ROWS, 256), f32),
            dma((3,)), dma((3,)), dma((4,)), dma((4,)), dma((4, 3)), dma((4, 3)), dma((4, 9)), dma((4, 9)),
            dma((2, 4)), dma((2, 4)), dma((4,)), dma((4,)), dma, dma, dma((8,)), dma((8,)),
            dma((9,)), dma((9,)), dma((2, 9)), dma((2, 9)), dma((2, 8)), dma((2, 8)), dma((8,)), dma((8,)),
            dma((2,)), dma((9,)), dma((9,)), dma((11,)), dma((8,)), dma((8,)), dma((8,)), dma((8,)),
        ],
        compiler_params=pltpu.CompilerParams(collective_id=1, has_side_effects=True),
        name="layer",
    )(*args)


def rotary_tables():
    lanes = np.arange(128)
    frequency = rope_base ** (-(lanes % 16) / 16.0)
    near = np.arange(ROWS)[:, None] * frequency[None, :]
    base = (np.arange(64) * ROWS)[:, None] * frequency[None, :]
    return tuple(np.asarray(f(a), np.float32) for a in (near, base) for f in (np.cos, np.sin))


def shards(
    tokens,
    input_gain,
    query_weight,
    query_rot_weight,
    kv_down,
    rot_down,
    kv_gain,
    key_up,
    value_up,
    conv_value_weight,
    conv_gate_weight,
    conv_taps,
    conv_ln_gain,
    conv_ln_bias,
    att_out_gain,
    conv_out_gain,
    att_out_weight,
    conv_out_weight,
):
    near_cos, near_sin, base_cos, base_sin = rotary_tables()
    return layer(
        tokens,
        query_weight,
        query_rot_weight.T,
        kv_down,
        rot_down.T,
        key_up,
        value_up,
        conv_value_weight,
        conv_gate_weight,
        att_out_weight,
        conv_out_weight,
        jnp.asarray(near_cos),
        jnp.asarray(near_sin),
        jnp.asarray(base_cos),
        jnp.asarray(base_sin),
        input_gain[None, :],
        kv_gain[None, :],
        conv_taps,
        conv_ln_gain[None, :],
        conv_ln_bias[None, :],
        att_out_gain[None, :],
        conv_out_gain[None, :],
    ).astype(jnp.bfloat16)


def solution(mesh):
    return jax.shard_map(
        shards,
        mesh=mesh,
        in_specs=(
            P("sp", "tp"),
            P(),
            P(None, "tp"),
            P(None, "tp"),
            P(),
            P(),
            P(),
            P(None, "tp"),
            P(None, "tp"),
            P(None, "tp"),
            P(None, "tp"),
            P(None, "tp"),
            P("tp"),
            P("tp"),
            P("tp"),
            P("tp"),
            P("tp", None),
            P("tp", None),
        ),
        out_specs=P("sp", "tp"),
        check_vma=False,
    )
```

```python
import math

import jax
import jax.numpy as jnp
import numpy as np
from jax import lax
from jax.experimental import pallas as pl
from jax.experimental.pallas import tpu as pltpu
from jax.sharding import PartitionSpec as P

D_MODEL = 2048
NOPE_DIM = 64
ROT_DIM = 32
CONV_CH = 1024
KERNEL = 31

norm_eps = 1e-06
far_below = -1e30
rope_base = 10000.0


MESH = pl.DeviceIdType.MESH
ROWS = 384
SHARE = 112
KSETS = 16
PIECE = 4 * ROWS
SCALE = 1.4426950408889634 / math.sqrt(NOPE_DIM + ROT_DIM)


def ring_peers(tp):
    x, c = tp // 2, tp % 2
    right = ((x + 1) % 4) * 2 + c
    left = ((x + 3) % 4) * 2 + c
    far = ((x + 2) % 4) * 2 + c
    partner = x * 2 + (1 - c)
    return right, left, far, partner


class RingGather:
    def __init__(self, buf, lo, size, send, recv, sp, tp):
        self.buf, self.lo, self.size = buf, lo, size
        self.send, self.recv, self.sp, self.tp = send, recv, sp, tp
        self.right, self.left, self.far, self.partner = ring_peers(tp)

    def piece(self, slot, part=None):
        size = self.size if part is None else self.size // 2
        start = self.lo + size if part == 1 else self.lo
        return self.buf.at[slot, pl.ds(start, size)]

    def copy(self, slot, part, sem, to):
        return pltpu.make_async_remote_copy(
            src_ref=self.piece(slot, part),
            dst_ref=self.piece(slot, part),
            send_sem=self.send.at[sem],
            recv_sem=self.recv.at[sem],
            device_id=(self.sp, to),
            device_id_type=MESH,
        )

    def begin(self):
        self.copy(self.tp, None, 0, self.right).start()
        self.copy(self.tp, None, 1, self.left).start()
        self.copy(self.tp, None, 2, self.partner).start()

    def relay(self):
        self.copy(self.left, None, 0, self.right).wait_recv()
        self.copy(self.left, 0, 5, self.right).start()
        self.copy(self.left, None, 3, self.partner).start()
        self.copy(self.right, None, 1, self.left).wait_recv()
        self.copy(self.right, 1, 6, self.left).start()
        self.copy(self.right, None, 4, self.partner).start()

    def relay_far(self):
        self.copy(self.far, 0, 5, self.right).wait_recv()
        self.copy(self.far, 0, 7, self.partner).start()
        self.copy(self.far, 1, 6, self.left).wait_recv()
        self.copy(self.far, 1, 8, self.partner).start()

    def finish(self):
        for sem, part in ((2, None), (3, None), (4, None), (7, 0), (8, 1)):
            self.copy(self.far, part, sem, self.partner).wait_recv()

    def drain(self):
        for sem, part in ((0, None), (1, None), (2, None), (3, None), (4, None), (5, 0), (6, 1), (7, 0), (8, 1)):
            self.copy(self.tp, part, sem, self.partner).wait_send()


def member_z(member, kind):
    return 2 * member + (kind + member) % 2


def layer_kernel(
    tokens_hbm, query_hbm, query_rot_hbm, kv_down_hbm, rot_down_hbm, key_up_hbm, value_up_hbm,
    conv_value_hbm, conv_gate_hbm, att_w_ref, conv_w_ref, near_cos_hbm, near_sin_hbm,
    base_cos_ref, base_sin_ref, input_gain_ref, kv_gain_ref,
    taps_ref, ln_gain_ref, ln_bias_ref, att_gain_ref, conv_gain_ref, out_ref,
    tbuf, scaled, wall, wqr, wrd, wkvd, kup, vup, near_cos, near_sin, p_send, p_recv,
    q_ref, share_ref, gated_ref,
    qraw, qbuf, kbuf, kk, vv, wkv, top, acc, o_send, l_send, o_recv, l_recv, own_out, own_lse,
    halo, padded, conv_out, mom_send, mom_recv, cbuf, abuf, weights, gains, gain_all, branch,
    q_ssem, q_rsem, k_ssem, k_rsem, f_ssem, f_rsem, ag_ssem, ag_rsem, o_ssem, o_rsem, l_ssem, l_rsem,
    h_ssem, h_rsem, m_ssem, m_rsem, c_ssem, c_rsem, a_ssem, a_rsem, w_ssem, w_rsem, g_ssem, g_rsem,
    own_sem, t_ssem, t_rsem, load_sem, p_ssem, p_rsem, v_ssem, v_rsem,
):
    sp, tp = lax.axis_index("sp"), lax.axis_index("tp")
    z, y = sp // 8, sp % 8
    kind, mine, parity = (z + z // 2) % 2, z // 2, y % 2
    residue = (y // 2 + mine + 2) % 4
    bf, f32 = jnp.bfloat16, jnp.float32

    def member_sp(member):
        return member_z(member, kind) * 8 + y

    place = 2 * parity + z % 2
    z_other, y_other = z + 1 - 2 * (z % 2), y + 1 - 2 * parity
    quad = (z_other * 8 + y, z * 8 + y_other, z_other * 8 + y_other)
    key_peers = []
    for d in range(4):
        m = (mine + d) % 4
        key_peers.append((2 * m + z % 2) * 8 + 2 * ((residue + 4 - m) % 4) + parity)
    after, before_sp = (sp + 1) % 64, (sp + 63) % 64

    own_rows = pl.ds(pl.multiple_of(256 * tp, 256), 256)
    wrd[32:128, :] = jnp.zeros((96, 256), bf)
    loads = [
        pltpu.make_async_copy(src, dst, load_sem.at[n])
        for n, (src, dst) in enumerate(
            (
                (tokens_hbm, tbuf.at[tp]),
                (kv_down_hbm.at[own_rows], wkvd),
                (rot_down_hbm.at[:, own_rows], wrd.at[pl.ds(0, 32)]),
                (key_up_hbm, kup),
                (value_up_hbm, vup),
                (query_hbm, wall.at[:, pl.ds(0, 128)]),
                (conv_value_hbm, wall.at[:, pl.ds(128, 128)]),
                (conv_gate_hbm, wall.at[:, pl.ds(256, 128)]),
                (query_rot_hbm, wqr),
                (near_cos_hbm, near_cos),
                (near_sin_hbm, near_sin),
            )
        )
    ]
    for load in loads:
        load.start()

    barrier = pltpu.get_barrier_semaphore()
    for i in range(1, 4):
        pl.semaphore_signal(
            barrier, inc=1, device_id=(member_sp((mine + i) % 4), tp), device_id_type=MESH
        )
        pl.semaphore_signal(barrier, inc=1, device_id=(quad[i - 1], tp), device_id_type=MESH)
    for peer in key_peers:
        pl.semaphore_signal(barrier, inc=1, device_id=(peer, tp), device_id_type=MESH)
    for i in range(1, 8):
        pl.semaphore_signal(barrier, inc=1, device_id=(sp, (tp + i) % 8), device_id_type=MESH)
        pl.semaphore_signal(barrier, inc=1, device_id=(z * 8 + (y + i) % 8, tp), device_id_type=MESH)
    pl.semaphore_signal(barrier, inc=1, device_id=(before_sp, tp), device_id_type=MESH)
    pl.semaphore_wait(barrier, 25)

    def remote(src, dst, ssem, rsem, to):
        return pltpu.make_async_remote_copy(
            src_ref=src, dst_ref=dst, send_sem=ssem, recv_sem=rsem, device_id=to, device_id_type=MESH
        )

    def scale_block(t):
        columns = pl.ds(pl.multiple_of(256 * t, 256), 256)
        x = tbuf[t].astype(f32)
        scaled[:, columns] = (x * input_gain_ref[:, columns]).astype(bf)
        return x * x

    tag = lax.broadcasted_iota(jnp.int32, (ROWS, 128), 1)
    low = tag < 64
    slab = pl.ds(pl.multiple_of(16 * y, 16), 16)

    def weight_copies(j):
        to = (sp, (tp + j) % 8)
        columns = pl.ds(pl.multiple_of(256 * ((tp + j) % 8), 256), 256)
        return (
            remote(
                att_w_ref.at[slab, columns], weights.at[0, tp, slab], w_ssem.at[0, j], w_rsem.at[0, tp], to
            ),
            remote(
                conv_w_ref.at[slab, columns], weights.at[1, tp, slab], w_ssem.at[1, j], w_rsem.at[1, tp], to
            ),
            remote(gains, gain_all.at[tp], g_ssem.at[j], g_rsem.at[tp], to),
        )

    own_weights = (
        pltpu.make_async_copy(att_w_ref.at[slab, own_rows], weights.at[0, tp, slab], own_sem.at[0]),
        pltpu.make_async_copy(conv_w_ref.at[slab, own_rows], weights.at[1, tp, slab], own_sem.at[1]),
    )

    def slab_copy(d):
        rows = weights.at[:, :, slab]
        return remote(rows, rows, v_ssem.at[d], v_rsem.at[y], (z * 8 + (y + d) % 8, tp))

    gains[...] = jnp.zeros(gains.shape, f32)
    gains[0:1, :] = att_gain_ref[...]
    gains[1:2, :] = conv_gain_ref[...]
    for copy in own_weights:
        copy.start()

    tokens_gather = RingGather(tbuf, 0, ROWS, t_ssem, t_rsem, sp, tp)
    for load in loads[0:3]:
        load.wait()
    squares = scale_block(tp)
    mine_scaled = scaled[:, own_rows]
    p_send[:, 0:256] = jnp.dot(mine_scaled, wkvd[...], preferred_element_type=f32).astype(bf)
    rot_part = lax.dot_general(
        mine_scaled, wrd[...], (((1,), (1,)), ((), ())), preferred_element_type=f32
    )
    p_send[:, 256:384] = jnp.where(
        tag == 32, jnp.sum(squares, axis=1, keepdims=True), rot_part
    ).astype(bf)

    def part_copy(j):
        peer = (tp + j) % 8
        return remote(
            p_send.at[pl.ds(pl.multiple_of(48 * peer, 16), 48)],
            p_recv.at[tp],
            p_ssem.at[j],
            p_rsem.at[tp],
            (sp, peer),
        )

    for j in range(1, 8):
        part_copy(j).start()
    tokens_gather.begin()

    for j in range(1, 8):
        for copy in weight_copies(j):
            copy.start()
    for load in loads[3:]:
        load.wait()
    lane = lax.broadcasted_iota(jnp.int32, (256, 128), 1)
    for n, ref in enumerate((kup, vup)):
        w = ref[...].astype(f32)
        wkv[:, pl.ds(256 * n, 128)] = jnp.where(lane < 64, w, 0.0).astype(bf)
        wkv[:, pl.ds(256 * n + 128, 128)] = jnp.where(lane < 64, pltpu.roll(w, 64, 1), 0.0).astype(bf)
    cos_base, sin_base = base_cos_ref[pl.ds(sp, 1), :], base_sin_ref[pl.ds(sp, 1), :]

    def turn(rows, near_c, near_s):
        cosine = near_c * cos_base - near_s * sin_base
        sine = near_s * cos_base + near_c * sin_base
        front = lax.broadcasted_iota(jnp.int32, rows.shape, 1) % 32 < 16
        other = jnp.where(front, pltpu.roll(rows, 112, 1), pltpu.roll(rows, 16, 1))
        return rows * cosine + other * jnp.where(front, -sine, sine)

    share_rows = pl.ds(pl.multiple_of(48 * tp, 16), 48)
    raw = p_send[share_rows, :].astype(f32)
    for j in range(1, 8):
        source = (tp + j) % 8
        remote(
            p_send.at[share_rows], p_recv.at[source], p_ssem.at[j], p_rsem.at[source], (sp, source)
        ).wait_recv()
        raw = raw + p_recv[source].astype(f32)
    power = jnp.sum(raw[:, 0:256] * raw[:, 0:256], axis=1, keepdims=True) / 256
    latent = (raw[:, 0:256] * lax.rsqrt(power + norm_eps) * kv_gain_ref[...]).astype(bf)
    share_ref[0:48, :] = latent[:, 0:128]
    share_ref[48:96, :] = latent[:, 128:256]
    key_rows = raw[:, 256:384]
    key_rows = key_rows * lax.rsqrt(key_rows[:, 32:33] / D_MODEL + norm_eps)
    key_rows = turn(key_rows, near_cos[share_rows, :], near_sin[share_rows, :])
    group = lax.broadcasted_iota(jnp.int32, (16, 128), 1) // 32
    fold = jnp.zeros((16, 128), f32)
    for j in range(3):
        fold = jnp.where(group == j, pltpu.roll(key_rows[16 * j : 16 * j + 16], 32 * j, 1), fold)
    share_ref[96:112, :] = fold.astype(bf)

    def block(p):
        return kbuf.at[tp, 4 * p + place]

    def key_copy(d):
        return remote(share_ref, block(mine), k_ssem.at[d], k_rsem.at[mine], (key_peers[d], tp))

    def quad_copy(p, n):
        return remote(block(p), block(p), f_ssem.at[p, n], f_rsem.at[p, n], (quad[n], tp))

    def spread(p):
        remote(share_ref, block(p), k_ssem.at[0], k_rsem.at[p], (key_peers[0], tp)).wait_recv()
        for n in range(3):
            quad_copy(p, n).start()

    def begin(p):
        for n in range(3):
            quad_copy(p, n).wait_recv()
        gathers[p].begin()

    for d in range(4):
        key_copy(d).start()

    gathers = [
        RingGather(kbuf, 4 * p, 4, ag_ssem.at[p], ag_rsem.at[p], sp, tp) for p in range(4)
    ]
    conv_gather = RingGather(cbuf, 0, ROWS, c_ssem, c_rsem, sp, tp)
    att_gather = RingGather(abuf, 0, ROWS, a_ssem, a_rsem, sp, tp)

    tokens_gather.relay()
    squares = squares + scale_block(tokens_gather.left)
    squares = squares + scale_block(tokens_gather.right)
    for p in range(4):
        spread(p)
    tokens_gather.relay_far()
    tokens_gather.finish()
    begin(0)
    begin(1)
    squares = squares + scale_block(tokens_gather.far)
    for t in (tp, tokens_gather.left, tokens_gather.right, tokens_gather.far):
        squares = squares + scale_block(t + 1 - 2 * (t % 2))
    row_scale = lax.rsqrt(jnp.sum(squares, axis=1, keepdims=True) / D_MODEL + norm_eps)
    flat = lax.dot_general(
        scaled[...], wqr[...], (((1,), (1,)), ((), ())), preferred_element_type=f32
    )
    flat = jnp.concatenate([flat * row_scale, jnp.zeros((ROWS, 64), f32)], axis=1)
    turned_rows = turn(flat, near_cos[...], near_sin[...])
    sums = jnp.dot(scaled[...], wall[...], preferred_element_type=f32)
    q_ref[0:ROWS, :] = (sums[:, 0:128] * (row_scale * SCALE)).astype(bf)
    half = ROWS // 2
    q_ref[ROWS : ROWS + half, :] = (
        jnp.where(low[0:half], turned_rows[0:half], pltpu.roll(turned_rows[half:ROWS], 64, 1)) * SCALE
    ).astype(bf)
    gated = (sums[:, 128:256] * row_scale * jax.nn.sigmoid(sums[:, 256:384] * row_scale)).astype(bf)
    gated_ref[...] = gated

    halo_copy = remote(gated_ref.at[pl.ds(ROWS - 32, 32)], halo, h_ssem, h_rsem, (after, tp))
    halo_copy.start()

    def query_copy(i):
        return remote(
            q_ref, qraw.at[i - 1], q_ssem.at[i - 1], q_rsem.at[i - 1], (member_sp((mine + i) % 4), tp)
        )

    for i in range(1, 4):
        query_copy(i).start()

    def unpack(ref, member):
        nope = ref[0:ROWS, :].astype(f32)
        fold = ref[ROWS : ROWS + ROWS // 2, :].astype(f32)
        for h in range(2):
            body = nope if h == 0 else pltpu.roll(nope, 64, 1)
            upper = pltpu.roll(fold, 64 - 32 * h, 1)
            lower = fold if h == 0 else pltpu.roll(fold, 96, 1)
            rotary = jnp.concatenate([upper, lower], axis=0)
            qbuf[member, h] = jnp.where(low, body, jnp.where(tag < 96, rotary, 0.0)).astype(bf)

    gathers[0].relay()
    begin(2)
    for copy in own_weights:
        copy.wait()
    for j in range(1, 8):
        source = (tp + j) % 8
        for n in range(2):
            rows = weights.at[n, source, slab]
            remote(rows, rows, w_ssem.at[n, j], w_rsem.at[n, source], (sp, source)).wait_recv()
        remote(gains, gain_all.at[source], g_ssem.at[j], g_rsem.at[source], (sp, source)).wait_recv()
    for d in range(1, 8):
        slab_copy(d).start()
    unpack(q_ref, mine)
    gathers[1].relay()
    begin(3)

    halo_copy.wait_recv()
    edge = halo[...].astype(f32)
    padded[0:32, :] = jnp.where(sp > 0, edge, jnp.zeros_like(edge))
    padded[pl.ds(32, ROWS), :] = gated_ref[...].astype(f32)
    total = jnp.zeros((ROWS, 128), f32)
    for tap in range(KERNEL):
        total = total + taps_ref[tap : tap + 1, :] * padded[pl.ds(tap + 2, ROWS), :]
    conv_out[...] = total
    sum_one = jnp.sum(total, axis=1, keepdims=True)
    sum_two = jnp.sum(total * total, axis=1, keepdims=True)
    mom_send[...] = jnp.transpose(jnp.where(tag == 0, sum_one, sum_two))[0:8, :]

    def moment_copy(j):
        return remote(
            mom_send, mom_recv.at[tp], m_ssem.at[j], m_rsem.at[tp], (sp, (tp + j) % 8)
        )

    for j in range(1, 8):
        moment_copy(j).start()

    def assemble(p):
        slots = [4 * p + u for u in range(4)]
        at = pl.ds(pl.multiple_of(p * PIECE, PIECE), PIECE)
        first = jnp.concatenate([kbuf[:, s, 0:48, :].reshape(ROWS, 128) for s in slots], axis=0)
        second = jnp.concatenate([kbuf[:, s, 48:96, :].reshape(ROWS, 128) for s in slots], axis=0)
        product = jnp.dot(
            jnp.concatenate([first, second], axis=1), wkv[...], preferred_element_type=f32
        )
        pieces = []
        for s in slots:
            folded = kbuf[:, s, 96:112, :].astype(f32).reshape(128, 128)
            turned = [
                pltpu.roll(folded, (64 - 32 * j) % 128, 1).reshape(8, 1, 16, 128) for j in range(3)
            ]
            pieces.append(jnp.concatenate(turned, axis=1).reshape(ROWS, 128))
        rotary = jnp.concatenate(pieces, axis=0)
        front = lax.broadcasted_iota(jnp.int32, (PIECE, 128), 1) < 64
        for h in range(2):
            kk[h, at, :] = jnp.where(
                front, product[:, 128 * h : 128 * h + 128], rotary
            ).astype(bf)
            vv[h, at, :] = jnp.where(
                front, product[:, 256 + 128 * h : 384 + 128 * h], 1.0
            ).astype(bf)

    def step(member, p, masked):
        if masked:
            offset = lax.broadcasted_iota(jnp.int32, (ROWS, ROWS), 1) - lax.broadcasted_iota(
                jnp.int32, (ROWS, ROWS), 0
            )
            block = member_sp(member)
        for h in range(2):
            scores = lax.dot_general(
                qbuf[member, h],
                kk[h, pl.ds(p * PIECE, PIECE), :],
                (((1,), (1,)), ((), ())),
                preferred_element_type=f32,
            )
            if masked:
                columns = []
                for u in range(4):
                    key_block = (2 * p + u % 2) * 8 + 2 * ((residue + 4 - p) % 4) + u // 2
                    columns.append(
                        jnp.where(
                            offset <= (block - key_block) * ROWS,
                            scores[:, ROWS * u : ROWS * u + ROWS],
                            far_below,
                        )
                    )
                scores = jnp.concatenate(columns, axis=1)
            now = jnp.broadcast_to(jnp.max(scores, axis=1, keepdims=True), (ROWS, 128))
            if p > 0:
                before = top[member, h]
                now = jnp.maximum(before, now)
            top[member, h] = now
            likely = jnp.exp2(scores - jnp.concatenate([now] * (PIECE // 128), axis=1)).astype(bf)
            fresh = jnp.dot(likely, vv[h, pl.ds(p * PIECE, PIECE), :], preferred_element_type=f32)
            if p > 0:
                fresh = acc[member, h] * jnp.exp2(before - now) + fresh
            acc[member, h] = fresh

    def back_copies(member, source):
        to = (member_sp(member), tp)
        return (
            remote(o_send.at[member], o_recv.at[source], o_ssem.at[member], o_rsem.at[source], to),
            remote(l_send.at[member], l_recv.at[source], l_ssem.at[member], l_rsem.at[source], to),
        )

    def finalize(member):
        sums, tops = [], []
        for h in range(2):
            a = acc[member, h]
            part = jnp.where(low, pltpu.roll(a, 64, 1), a)
            sums.append(part)
            tops.append(top[member, h] + jnp.log2(part))
        value = jnp.where(low, acc[member, 0], pltpu.roll(acc[member, 1], 64, 1))
        value = value / jnp.where(low, sums[0], sums[1])
        o_send[member] = value.astype(bf)
        l_send[member] = jnp.transpose(jnp.where(tag < 4, tops[0], tops[1]))[0:8, :]

        @pl.when(mine == member)
        def _():
            own_out[...] = value
            own_lse[...] = jnp.where(low, tops[0], tops[1])

        @pl.when(mine != member)
        def _():
            for copy in back_copies(member, mine):
                copy.start()

    def arrive(i):
        query_copy(i).wait_recv()
        member = (mine + 4 - i) % 4
        unpack(qraw.at[i - 1], member)
        return member

    gathers[0].relay_far()
    gathers[2].relay()
    gathers[0].finish()
    assemble(0)
    gathers[1].relay_far()
    step(mine, 0, True)
    gathers[3].relay()
    gathers[1].finish()
    assemble(1)
    gathers[2].relay_far()
    step(arrive(1), 0, True)
    gathers[3].relay_far()
    step(arrive(3), 0, True)

    mom_recv[tp] = mom_send[...]
    for j in range(1, 8):
        source = (tp + j) % 8
        remote(mom_send, mom_recv.at[source], m_ssem.at[j], m_rsem.at[source], (sp, source)).wait_recv()
    moments = mom_recv[0]
    for t in range(1, 8):
        moments = moments + mom_recv[t]
    columns = jnp.transpose(moments)
    mean_val = columns[:, 0:1] / CONV_CH
    spread = columns[:, 1:2] / CONV_CH - mean_val * mean_val
    normed = (conv_out[...] - mean_val) * lax.rsqrt(spread + norm_eps)
    swished = jax.nn.silu(normed * ln_gain_ref[...] + ln_bias_ref[...])
    cbuf[tp] = swished.astype(bf)

    conv_gather.begin()
    gathers[2].finish()
    assemble(2)
    step(arrive(2), 0, True)
    finalize(0)
    step(1, 1, True)
    finalize(1)
    step(2, 1, False)
    conv_gather.relay()
    step(2, 2, True)
    finalize(2)
    step(3, 1, False)
    conv_gather.relay_far()
    step(3, 2, False)
    gathers[3].finish()
    assemble(3)
    step(3, 3, True)
    finalize(3)

    gain_all[tp] = gains[...]
    conv_gather.finish()
    for d in range(1, 8):
        source = (y + d) % 8
        rows = weights.at[:, :, pl.ds(pl.multiple_of(16 * source, 16), 16)]
        remote(rows, rows, v_ssem.at[d], v_rsem.at[source], (z * 8 + source, tp)).wait_recv()

    def product(buf, n):
        wide = jnp.concatenate([buf[t] for t in range(8)], axis=1).astype(f32)
        gain = jnp.concatenate([gain_all[t, n : n + 1, :] for t in range(8)], axis=1)
        power = jnp.sum(wide * wide, axis=1, keepdims=True)
        mixed = (wide * lax.rsqrt(power / CONV_CH + norm_eps) * gain).astype(bf)
        return jnp.dot(mixed, weights[n].reshape(1024, 256), preferred_element_type=f32)

    branch[...] = product(cbuf, 1)

    logs, values = [own_lse[...]], [own_out[...]]
    for i in range(1, 4):
        source = (mine + i) % 4
        for copy in back_copies(source, source):
            copy.wait_recv()
        columns = jnp.transpose(l_recv[source])
        logs.append(jnp.where(low, columns[:, 0:1], columns[:, 4:5]))
        values.append(o_recv[source].astype(f32))
    peak = jnp.maximum(jnp.maximum(logs[0], logs[1]), jnp.maximum(logs[2], logs[3]))
    shares = [jnp.exp2(log - peak) for log in logs]
    merged = sum(s * v for s, v in zip(shares, values)) / sum(shares)
    abuf[tp] = merged.astype(bf)

    att_gather.begin()
    att_gather.relay()
    att_gather.relay_far()
    att_gather.finish()
    out_ref[...] = (branch[...] + product(abuf, 0)).astype(bf)

    tokens_gather.drain()
    halo_copy.wait_send()
    for i in range(1, 8):
        part_copy(i).wait_send()
        moment_copy(i).wait_send()
        for copy in weight_copies(i):
            copy.wait_send()
        slab_copy(i).wait_send()
    for j in range(4):
        key_copy(j).wait_send()
        for n in range(3):
            quad_copy(j, n).wait_send()
        gathers[j].drain()
    for i in range(1, 4):
        query_copy(i).wait_send()
        member = (mine + i) % 4
        for copy in back_copies(member, mine):
            copy.wait_send()
    conv_gather.drain()
    att_gather.drain()


def layer(*args):
    vmem, anywhere = pl.BlockSpec(memory_space=pltpu.VMEM), pl.BlockSpec(memory_space=pl.ANY)
    bf, f32 = jnp.bfloat16, jnp.float32
    dma = pltpu.SemaphoreType.DMA
    return pl.pallas_call(
        layer_kernel,
        out_shape=jax.ShapeDtypeStruct((ROWS, 256), bf),
        in_specs=[anywhere] * 13 + [vmem] * 9,
        out_specs=vmem,
        scratch_shapes=[
            pltpu.VMEM((8, ROWS, 256), bf),
            pltpu.VMEM((ROWS, D_MODEL), bf),
            pltpu.VMEM((D_MODEL, 384), bf),
            pltpu.VMEM((64, D_MODEL), bf),
            pltpu.VMEM((128, 256), bf),
            pltpu.VMEM((256, 256), bf),
            pltpu.VMEM((256, 128), bf),
            pltpu.VMEM((256, 128), bf),
            pltpu.VMEM((ROWS, 128), f32),
            pltpu.VMEM((ROWS, 128), f32),
            pltpu.VMEM((ROWS, 384), bf),
            pltpu.VMEM((8, 48, 384), bf),
            pltpu.VMEM((ROWS + ROWS // 2, 128), bf),
            pltpu.VMEM((SHARE, 128), bf),
            pltpu.VMEM((ROWS, 128), bf),
            pltpu.VMEM((3, ROWS + ROWS // 2, 128), bf),
            pltpu.VMEM((4, 2, ROWS, 128), bf),
            pltpu.VMEM((8, KSETS, SHARE, 128), bf),
            pltpu.VMEM((2, KSETS * ROWS, 128), bf),
            pltpu.VMEM((2, KSETS * ROWS, 128), bf),
            pltpu.VMEM((256, 512), bf),
            pltpu.VMEM((4, 2, ROWS, 128), f32),
            pltpu.VMEM((4, 2, ROWS, 128), f32),
            pltpu.VMEM((4, ROWS, 128), bf),
            pltpu.VMEM((4, 8, ROWS), f32),
            pltpu.VMEM((4, ROWS, 128), bf),
            pltpu.VMEM((4, 8, ROWS), f32),
            pltpu.VMEM((ROWS, 128), f32),
            pltpu.VMEM((ROWS, 128), f32),
            pltpu.VMEM((32, 128), bf),
            pltpu.VMEM((32 + ROWS, 128), f32),
            pltpu.VMEM((ROWS, 128), f32),
            pltpu.VMEM((8, ROWS), f32),
            pltpu.VMEM((8, 8, ROWS), f32),
            pltpu.VMEM((8, ROWS, 128), bf),
            pltpu.VMEM((8, ROWS, 128), bf),
            pltpu.VMEM((2, 8, 128, 256), bf),
            pltpu.VMEM((8, 128), f32),
            pltpu.VMEM((8, 8, 128), f32),
            pltpu.VMEM((ROWS, 256), f32),
            dma((3,)), dma((3,)), dma((4,)), dma((4,)), dma((4, 3)), dma((4, 3)), dma((4, 9)), dma((4, 9)),
            dma((4,)), dma((4,)), dma((4,)), dma((4,)), dma, dma, dma((8,)), dma((8,)),
            dma((9,)), dma((9,)), dma((9,)), dma((9,)), dma((2, 8)), dma((2, 8)), dma((8,)), dma((8,)),
            dma((2,)), dma((9,)), dma((9,)), dma((11,)), dma((8,)), dma((8,)), dma((8,)), dma((8,)),
        ],
        compiler_params=pltpu.CompilerParams(collective_id=1, has_side_effects=True),
        name="layer",
    )(*args)


def rotary_tables():
    lanes = np.arange(128)
    frequency = rope_base ** (-(lanes % 16) / 16.0)
    near = np.arange(ROWS)[:, None] * frequency[None, :]
    base = (np.arange(64) * ROWS)[:, None] * frequency[None, :]
    return tuple(np.asarray(f(a), np.float32) for a in (near, base) for f in (np.cos, np.sin))


def shards(
    tokens,
    input_gain,
    query_weight,
    query_rot_weight,
    kv_down,
    rot_down,
    kv_gain,
    key_up,
    value_up,
    conv_value_weight,
    conv_gate_weight,
    conv_taps,
    conv_ln_gain,
    conv_ln_bias,
    att_out_gain,
    conv_out_gain,
    att_out_weight,
    conv_out_weight,
):
    near_cos, near_sin, base_cos, base_sin = rotary_tables()
    return layer(
        tokens,
        query_weight,
        query_rot_weight.T,
        kv_down,
        rot_down.T,
        key_up,
        value_up,
        conv_value_weight,
        conv_gate_weight,
        att_out_weight,
        conv_out_weight,
        jnp.asarray(near_cos),
        jnp.asarray(near_sin),
        jnp.asarray(base_cos),
        jnp.asarray(base_sin),
        input_gain[None, :],
        kv_gain[None, :],
        conv_taps,
        conv_ln_gain[None, :],
        conv_ln_bias[None, :],
        att_out_gain[None, :],
        conv_out_gain[None, :],
    )


def solution(mesh):
    return jax.shard_map(
        shards,
        mesh=mesh,
        in_specs=(
            P("sp", "tp"),
            P(),
            P(None, "tp"),
            P(None, "tp"),
            P(),
            P(),
            P(),
            P(None, "tp"),
            P(None, "tp"),
            P(None, "tp"),
            P(None, "tp"),
            P(None, "tp"),
            P("tp"),
            P("tp"),
            P("tp"),
            P("tp"),
            P("tp", None),
            P("tp", None),
        ),
        out_specs=P("sp", "tp"),
        check_vma=False,
    )
```
